128 devices in a mesh: fs: 16 (over z, y), tp: 8 (over x, core).
Axes of the slice: x: 4, y: 4, z: 4, core: 2. Of those that a mesh axis runs over, the one named last changes fastest.
Arguments:
- mixed: bfloat16 [49152, 2048], P(('fs', 'tp')), may hold values from -6 to 6
- residual: bfloat16 [49152, 2048], P(('fs', 'tp')), may hold values from -6 to 6
- mix_weight: bfloat16 [2048, 2048], P(('fs', 'tp')), may hold values from -0.125 to 0.125
- norm_gain: float32 [2048], replicated, may hold values from 0.1 to 1.9
- up_weight: bfloat16 [2048, 5504], P('fs', 'tp'), may hold values from -0.125 to 0.125
- gate_weight: bfloat16 [2048, 5504], P('fs', 'tp'), may hold values from -0.125 to 0.125
- conv_weight: float32 [3, 5504], P(None, 'tp'), may hold values from -3 to 3
- conv_bias: float32 [5504], P('tp'), may hold values from -3 to 3
- down_weight: bfloat16 [5504, 2048], P('tp', 'fs'), may hold values from -0.078125 to 0.078125
Outputs:
- output: bfloat16 [49152, 2048], P(('fs', 'tp'))
The draws below stay inside these ranges and needn't reach their ends.
All inputs are finite; a program needn't handle non-finite values.
Results may differ from the reference program's by a relative error of at most 0.012.
Values may be sent and summed in bfloat16 or wider, within the bound.
A program may use at most 128 MiB of HBM per device.

```python
import jax
import jax.numpy as jnp
from jax import lax

D = 2048
DM = 2048
FF = 5504
TOK_DEV = 384
TOKENS = 49152
N_FS = 16
N_TP = 8


def block_levels(stream_key, dims, shards, smallest, top_value):
    factor_of = 1.0
    for axis_at, parts in shards:
        steps = jax.random.uniform(jax.random.fold_in(jax.random.fold_in(stream_key, 6), axis_at), (parts,), jnp.float32, smallest / len(shards), top_value / len(shards))
        factor_of = factor_of * jnp.repeat(jnp.exp(steps), dims[axis_at] // parts).reshape((-1,) + (1,) * (len(dims) - 1 - axis_at))
    return factor_of


def scatter_about(own_key, shape, width, bound, pieces=(), kind=jnp.bfloat16):
    loudness = block_levels(own_key, shape, pieces, -0.22, 0.18) if pieces else 1.0
    entries = jax.random.normal(own_key, shape, jnp.float32) * width * loudness
    return jnp.minimum(jnp.maximum(entries, -bound), bound).astype(kind)


def setup_inputs(seed: int = 0) -> dict:
    streams_of = jax.random.split(jax.random.key(seed), 10)
    return {
        "mixed": scatter_about(streams_of[0], (TOKENS, DM), 1.0, 6.0, ((0, 128),)),
        "residual": scatter_about(streams_of[1], (TOKENS, D), 1.0, 6.0, ((0, 128),)),
        "mix_weight": scatter_about(streams_of[2], (DM, D), DM ** -0.5, 0.125, ((0, 128),)),
        "norm_gain": jnp.clip(1.0 + 0.18 * jax.random.normal(streams_of[3], (D,), jnp.float32), 0.1, 1.9),
        "up_weight": scatter_about(streams_of[4], (D, FF), D ** -0.5, 0.125, ((0, 16), (1, 8))),
        "gate_weight": scatter_about(streams_of[5], (D, FF), D ** -0.5, 0.125, ((0, 16), (1, 8))),
        "conv_weight": scatter_about(streams_of[6], (3, FF), 0.577, 3.0, ((1, 8),), jnp.float32),
        "conv_bias": scatter_about(streams_of[7], (FF,), 0.5, 3.0, ((0, 8),), jnp.float32),
        "down_weight": scatter_about(streams_of[8], (FF, D), FF ** -0.5, 0.078125, ((0, 8), (1, 16))),
    }


norm_eps = 1e-06

def reference(mixed, residual, mix_weight, norm_gain, up_weight, gate_weight, conv_weight, conv_bias, down_weight):
    unit_block = FF // N_TP
    length = TOK_DEV * N_TP
    stream = (residual.astype(jnp.float32) + jnp.dot(mixed, mix_weight, preferred_element_type=jnp.float32)).astype(jnp.bfloat16)
    x_float = stream.astype(jnp.float32)
    normed = (x_float * lax.rsqrt(lax.optimization_barrier(jnp.mean(x_float * x_float, axis=-1, keepdims=True)) + norm_eps) * norm_gain).astype(jnp.bfloat16)

    def one_seq(pair):
        normed_seq, stream_seq = pair
        up_part = jnp.dot(normed_seq, up_weight, preferred_element_type=jnp.float32).astype(jnp.bfloat16)
        gate_part = jnp.dot(normed_seq, gate_weight, preferred_element_type=jnp.float32).astype(jnp.bfloat16)
        up_float = lax.optimization_barrier(up_part).astype(jnp.float32)
        padded = jnp.pad(up_float, ((2, 0), (0, 0)))
        smoothed = conv_bias + conv_weight[0] * padded[:-2] + conv_weight[1] * padded[1:-1] + conv_weight[2] * padded[2:]
        hidden = (jax.nn.gelu(smoothed) * gate_part.astype(jnp.float32)).astype(jnp.bfloat16)
        accum_sum = stream_seq.astype(jnp.float32)
        for index in range(N_TP):
            partial_value = jnp.dot(hidden[:, index * unit_block:(index + 1) * unit_block], down_weight[index * unit_block:(index + 1) * unit_block], preferred_element_type=jnp.float32).astype(jnp.bfloat16)
            accum_sum = accum_sum + lax.optimization_barrier(partial_value).astype(jnp.float32)
        return accum_sum.astype(jnp.bfloat16)
    result = lax.map(one_seq, (normed.reshape(N_FS, length, D), stream.reshape(N_FS, length, D)))
    return result.reshape(N_FS * length, D)
```

```python
import functools

import jax
import jax.numpy as jnp
from jax import lax
from jax.experimental import pallas as pl
from jax.experimental.pallas import tpu as pltpu
from jax.sharding import PartitionSpec as P

MESH = pl.DeviceIdType.MESH
F32 = jnp.float32
BF16 = jnp.bfloat16
NORM_EPS = 1e-06
GELU_C = 0.7978845608028654

D = 2048
TOK = 384
PIECE = 96
HALF = 192
UG = 1408
HID = 768


def gelu_tanh(v):
    return 0.5 * v * (1.0 + jnp.tanh(GELU_C * (v + 0.044715 * (v * v * v))))


class Gather:
    def __init__(self, ref, lo, rows, split, flip, fs, tp, send_sem, recv_sem):
        self.ref, self.lo, self.rows, self.split, self.flip = ref, lo, rows, split, flip
        self.tp, self.ss, self.rs = tp, send_sem, recv_sem
        z, y = fs // 4, fs % 4
        self.p = y * (1 - flip) + z * flip
        self.s = z * (1 - flip) + y * flip
        self.n = 0
        self.sends = []

    def zy(self, dp, ds):
        p, s = (self.p + dp + 4) % 4, (self.s + ds + 4) % 4
        return s * (1 - self.flip) + p * self.flip, p * (1 - self.flip) + s * self.flip

    def view(self, dp, ds, a=0, n=None):
        z, y = self.zy(dp, ds)
        n = self.rows if n is None else n
        return self.ref.at[z, y, pl.ds(self.lo + a, n)]

    def copy(self, k, blk, to):
        z, y = self.zy(*to)
        return pltpu.make_async_remote_copy(
            src_ref=blk, dst_ref=blk, send_sem=self.ss.at[self.n % 16], recv_sem=self.rs.at[k],
            device_id={"fs": z * 4 + y, "tp": self.tp}, device_id_type=MESH)

    def send(self, k, blk, to):
        c = self.copy(k, blk, to)
        c.start()
        self.sends.append(c)
        self.n += 1

    def wait(self, k, blk):
        self.copy(k, blk, (1, 0)).wait_recv()

    REL = (0, -1, 1, 2)

    def both(self, i):
        blk = self.view(self.REL[i], 0)
        self.send(4 + i, blk, (0, 1))
        self.send(8 + i, blk, (0, -1))

    def start(self):
        own = self.view(0, 0)
        self.send(0, own, (1, 0))
        self.send(1, own, (-1, 0))
        self.both(0)

    def near(self):
        s = self.split
        self.wait(0, self.view(-1, 0))
        self.send(2, self.view(-1, 0, 0, s), (1, 0))
        self.both(1)
        self.wait(1, self.view(1, 0))
        self.send(3, self.view(1, 0, s, self.rows - s), (-1, 0))
        self.both(2)

    def far(self):
        s = self.split
        self.wait(2, self.view(2, 0, 0, s))
        self.wait(3, self.view(2, 0, s, self.rows - s))
        self.both(3)

    def cross(self, i):
        below, above = self.view(self.REL[i], -1), self.view(self.REL[i], 1)
        self.wait(4 + i, below)
        if i < 2:
            self.send(12 + i, below, (0, 1))
        self.wait(8 + i, above)
        if i >= 2:
            self.send(12 + i, above, (0, -1))

    def last(self, i):
        self.wait(12 + i, self.view(self.REL[i], 2))

    def drain(self):
        for c in self.sends:
            c.wait_send()


def kernel(mixed, resid, wm_in, gain, ug_in, cw, dw_in, out,
           wm, ug, dwn, tok, mx, rs, stream, hal, xexp, hu, hid, pbuf, precv, xfwd, xfin,
           lsem, wx_s, wx_r, g_s, g_r, d_s, d_r, t_s, t_r, td_s, td_r, h_s, h_r, p_s, p_r,
           x_s, x_r):
    fs, tp = lax.axis_index("fs"), lax.axis_index("tp")
    z, y, x, c = fs // 4, fs % 4, tp // 2, tp % 2
    xr, xl, xo = (x + 1) % 4, (x + 3) % 4, (x + 2) % 4
    mate = x * 2 + (1 - c)
    drains = []

    def rcopy(src, dst, ss, rsem, tp_to, fs_to=None):
        return pltpu.make_async_remote_copy(
            src_ref=src, dst_ref=dst, send_sem=ss, recv_sem=rsem,
            device_id={"fs": fs if fs_to is None else fs_to, "tp": tp_to}, device_id_type=MESH)

    ld_ug = pltpu.make_async_copy(ug_in, ug.at[z, y], lsem.at[0])
    ld_dw = pltpu.make_async_copy(dw_in, dwn.at[z, y, pl.ds(0, 688)], lsem.at[1])
    ld_mx = pltpu.make_async_copy(mixed, mx, lsem.at[2])
    ld_rs = pltpu.make_async_copy(resid, rs, lsem.at[3])
    ld_mx.start()
    ld_rs.start()
    ld_ug.start()
    ld_dw.start()

    bar = pltpu.get_barrier_semaphore()
    peers = [(fs, (tp + k) % 8) for k in range(1, 8)]
    peers += [(z * 4 + (y + 1) % 4, tp), (z * 4 + (y + 3) % 4, tp)]
    peers += [(((z + 1) % 4) * 4 + y, tp), (((z + 3) % 4) * 4 + y, tp)]
    for f, t in peers:
        pl.semaphore_signal(bar, inc=1, device_id={"fs": f, "tp": t}, device_id_type=MESH)
    pl.semaphore_wait(bar, len(peers))

    half = tp // 4
    row16 = pl.multiple_of(tp * 16, 16)
    wm_dst = wm.at[z, y, pl.ds(row16, 16)]
    slot = tp % 4
    for k in range(1, 4):
        cp = rcopy(wm_in, wm_dst, wx_s.at[k], wx_r.at[slot], ((x + k) % 4) * 2 + half)
        cp.start()
        drains.append(cp)
    stay = pltpu.make_async_copy(wm_in, wm_dst, wx_r.at[slot])
    over = rcopy(wm_in, wm_dst, wx_s.at[0], wx_r.at[slot], mate)

    @pl.when(c == half)
    def _():
        stay.start()

    @pl.when(c != half)
    def _():
        over.start()

    zero_rows = jnp.zeros((HID - 688, 128), BF16)

    @pl.loop(0, 16)
    def _(f):
        dwn[f // 4, f % 4, pl.ds(688, HID - 688)] = zero_rows

    lo = pl.multiple_of(c * 64, 64)
    for k in range(4):
        row = pl.multiple_of(lo + k * 16, 16)
        blk = wm.at[z, y, pl.ds(row, 16)]
        rcopy(blk, blk, wx_s.at[0], wx_r.at[k], mate).wait_recv()

    gw = Gather(wm, lo, 64, 32, c, fs, tp, g_s.at[0], g_r.at[0])
    gu = Gather(ug, 0, 128, 64, c, fs, tp, g_s.at[1], g_r.at[1])
    gd = Gather(dwn, 0, 688, 352, 1 - c, fs, tp, g_s.at[2], g_r.at[2])

    def share(k, dp, ds):
        blk = gw.view(dp, ds)
        cp = rcopy(blk, blk, d_s.at[k], d_r.at[k], mate)
        cp.start()
        drains.append(cp)

    gw.start()
    share(0, 0, 0)
    gw.near()
    share(1, -1, 0)
    share(2, 1, 0)
    gw.cross(0)
    share(4, 0, -1)
    share(5, 0, 1)
    gw.far()
    share(3, 2, 0)
    gw.cross(1)
    share(6, -1, -1)
    share(7, -1, 1)
    gw.cross(2)
    share(8, 1, -1)
    share(9, 1, 1)
    gw.cross(3)
    share(10, 2, -1)
    share(11, 2, 1)
    ld_ug.wait()
    gu.start()
    for i in range(4):
        gw.last(i)
        share(12 + i, gw.REL[i], 2)
    other = pl.multiple_of(64 - lo, 64)
    for k in range(16):
        blk = wm.at[k // 4, k % 4, pl.ds(other, 64)]
        rcopy(blk, blk, d_s.at[k], d_r.at[k], mate).wait_recv()

    ld_mx.wait()
    ld_rs.wait()

    @pl.loop(0, 8)
    def _(n):
        cols = pl.ds(pl.multiple_of(n * 256, 256), 256)
        w = wm[:, :, :, cols].reshape(D, 256)
        s = jnp.dot(mx[...], w, preferred_element_type=F32)
        stream[:, cols] = (rs[:, cols].astype(F32) + s).astype(BF16)

    def send_tok(k, piece, xsrc, to_right, sidx):
        blk = tok.at[xsrc, c, piece]
        side = 0 if to_right else 1
        cp = rcopy(blk, blk, t_s.at[side, sidx], t_r.at[side, sidx],
                   (xr if to_right else xl) * 2 + c)
        cp.start()
        drains.append(cp)

    def norm_piece(k):
        @pl.loop(0, PIECE // 16)
        def _(r):
            rows = pl.ds(pl.multiple_of(k * PIECE + r * 16, 16), 16)
            v = stream[rows, :].astype(F32)
            m = jnp.mean(v * v, axis=-1, keepdims=True)
            v = v * lax.rsqrt(m + NORM_EPS) * gain[...]
            tok[x, c, k, pl.ds(pl.multiple_of(r * 16, 16), 16), :] = v.astype(BF16)

    norm_piece(0)
    send_tok(0, 0, x, True, 0)
    norm_piece(2)
    send_tok(2, 2, x, False, 0)
    norm_piece(1)
    send_tok(1, 1, x, True, 1)
    norm_piece(3)
    send_tok(3, 3, x, False, 1)

    tails = []
    for k in (1, 3):
        v = tok[x, c, k, pl.ds(PIECE - 16, 16), :].astype(F32)
        for r in (14, 15):
            for q in range(8):
                tails.append(v[r:r + 1, q * 256:(q + 1) * 256])
    hal[tp] = jnp.concatenate(tails, axis=0).astype(BF16)
    for k in range(1, 8):
        cp = rcopy(hal.at[tp], hal.at[tp], h_s.at[k], h_r.at[8 - k], (tp + k) % 8)
        cp.start()
        drains.append(cp)

    def mate_tok(k, xsrc, first, n):
        blk = tok.at[xsrc, c, pl.ds(first, n)]
        cp = rcopy(blk, blk, td_s.at[k], td_r.at[k], mate)
        cp.start()
        drains.append(cp)

    def mate_wait(k, xsrc, first, n):
        blk = tok.at[xsrc, 1 - c, pl.ds(first, n)]
        rcopy(blk, blk, td_s.at[k], td_r.at[k], mate).wait_recv()

    def tok_wait(from_left, idx, xsrc, piece):
        blk = tok.at[xsrc, c, piece]
        side = 0 if from_left else 1
        rcopy(blk, blk, t_s.at[side, idx], t_r.at[side, idx], mate).wait_recv()

    mate_tok(0, x, 0, 4)
    gu.near()
    gu.cross(0)
    gu.far()

    tok_wait(True, 0, xl, 0)
    send_tok(0, 0, xl, True, 2)
    tok_wait(False, 0, xr, 2)
    send_tok(2, 2, xr, False, 2)
    gu.cross(1)
    gu.cross(2)
    tok_wait(True, 1, xl, 1)
    send_tok(1, 1, xl, True, 3)
    send_tok(2, 2, x, True, 4)
    send_tok(3, 3, x, True, 5)
    tok_wait(False, 1, xr, 3)
    send_tok(3, 3, xr, False, 3)
    send_tok(0, 0, x, False, 4)
    send_tok(1, 1, x, False, 5)
    mate_tok(1, xl, 0, 2)
    mate_tok(2, xr, 2, 2)
    gu.cross(3)
    ld_dw.wait()
    gd.start()
    for i in range(4):
        gu.last(i)

    for k in range(1, 8):
        src = (tp + k) % 8
        rcopy(hal.at[src], hal.at[src], h_s.at[k], h_r.at[k], mate).wait_recv()
    hv = hal[...].reshape(256, 256).astype(F32)
    rid = lax.broadcasted_iota(jnp.int32, (256, 256), 0) % 8
    for q in range(8):
        xexp[:, q * 256:(q + 1) * 256] = jnp.where(rid == q, hv, 0.0).astype(BF16)

    gd.near()
    gd.cross(0)
    gd.far()

    @pl.loop(0, 6)
    def _(i):
        w = ug[:, :, :, pl.ds(pl.multiple_of(i * 256, 256), 128)].reshape(D, 128)
        r = jnp.dot(xexp[...], w, preferred_element_type=F32)
        r = jnp.sum(r.reshape(32, 8, 128), axis=1).astype(BF16).astype(F32)
        cols = pl.ds(pl.multiple_of(i * 128, 128), 128)
        hu[0, 0:2, cols] = jnp.zeros((2, 128), F32)
        for q in range(15):
            hu[q + 1, 0:2, cols] = r[2 * q:2 * q + 2]

    gd.cross(1)
    gd.cross(2)
    gd.cross(3)

    tok_wait(True, 2, xo, 0)
    tok_wait(True, 3, xo, 1)
    mate_tok(3, xo, 0, 2)
    tok_wait(False, 2, xo, 2)
    tok_wait(False, 3, xo, 3)
    mate_tok(4, xo, 2, 2)
    for i in range(4):
        gd.last(i)
    mate_wait(1, xl, 0, 2)
    mate_wait(2, xr, 2, 2)
    mate_wait(3, xo, 0, 2)
    mate_wait(4, xo, 2, 2)

    rowid = lax.broadcasted_iota(jnp.int32, (HALF, 128), 0)

    def unit(xx, cc, h, cls):
        j = xx * 2 + cc

        def act(i, u, g):
            cols = pl.ds(pl.multiple_of(i * 128, 128), 128)
            u = u.astype(BF16).astype(F32)
            g = g.astype(BF16).astype(F32)
            before = hu[j * 2 + h, :, cols]
            h0, h1 = before[0:1], before[1:2]
            u1 = jnp.where(rowid == 0, h1, pltpu.roll(u, 1, 0))
            u2 = jnp.where(rowid == 0, h0, jnp.where(rowid == 1, h1, pltpu.roll(u, 2, 0)))
            s = (cw[pl.ds(3, 1), cols] + cw[pl.ds(0, 1), cols] * u2
                 + cw[pl.ds(1, 1), cols] * u1 + cw[pl.ds(2, 1), cols] * u)
            hid[:, cols] = (gelu_tanh(s) * g).astype(BF16)

        def rows():
            return tok[xx, cc, pl.ds(h * 2, 2)].reshape(HALF, D)

        @pl.loop(0, 5)
        def _(i):
            w = ug[:, :, :, pl.ds(pl.multiple_of(i * 256, 256), 256)].reshape(D, 256)
            r = jnp.dot(rows(), w, preferred_element_type=F32)
            act(i, r[:, :128], r[:, 128:])

        w = ug[:, :, :, pl.ds(1280, 128)].reshape(D, 128)
        r = jnp.dot(rows(), w, preferred_element_type=F32)
        act(5, r, pltpu.roll(r, 64, 1))

        @pl.loop(0, 8)
        def _(n):
            zz, y0 = n // 2, (n % 2) * 2
            w = jnp.concatenate([dwn[zz, y0], dwn[zz, y0 + 1]], axis=1)
            r = jnp.dot(hid[...], w, preferred_element_type=F32)
            pbuf[cls, xx, h, :, pl.ds(pl.multiple_of(n * 256, 256), 256)] = r.astype(BF16)

    def group(xs, hs):
        @pl.loop(0, 4)
        def _(i):
            cls, kind = i // 2, i % 2
            cc = (1 - c) * (1 - cls) + c * cls
            xx = xs[0] * (1 - kind) + xs[1] * kind
            h = hs[0] * (1 - kind) + hs[1] * kind
            unit(xx, cc, h, cls)

            @pl.when(cls == 0)
            def _():
                rcopy(pbuf.at[0, xx, h], precv.at[xx, h], p_s.at[xx, h], p_r.at[xx, h],
                      mate).start()

    def joined(xx, h, extra=None):
        rcopy(pbuf.at[0, xx, h], precv.at[xx, h], p_s.at[xx, h], p_r.at[xx, h], mate).wait_recv()

        @pl.loop(0, HALF // 16)
        def _(r):
            rr = pl.ds(pl.multiple_of(r * 16, 16), 16)
            v = pbuf[1, xx, h, rr, :].astype(F32) + precv[xx, h, rr, :].astype(F32)
            if extra is not None:
                v = v + extra[rr, :].astype(F32)
            pbuf[1, xx, h, rr, :] = v.astype(BF16)

    def send_sum(xx, h, to_right, dst, k):
        side = 0 if to_right else 1
        cp = rcopy(pbuf.at[1, xx, h], dst, x_s.at[side, k], x_r.at[side, k],
                   (xr if to_right else xl) * 2 + c)
        cp.start()
        drains.append(cp)

    def wait_sum(from_left, dst, k):
        side = 0 if from_left else 1
        rcopy(dst, dst, x_s.at[side, k], x_r.at[side, k], mate).wait_recv()

    group((xo, xo), (0, 1))
    joined(xo, 0)
    send_sum(xo, 0, True, xfwd.at[0], 0)
    joined(xo, 1)
    send_sum(xo, 1, False, xfwd.at[1], 0)
    group((xr, xl), (1, 0))
    joined(xr, 1)
    send_sum(xr, 1, True, xfin.at[0, 1], 1)
    joined(xl, 0)
    send_sum(xl, 0, False, xfin.at[1, 0], 1)

    tok_wait(True, 4, xl, 2)
    tok_wait(True, 5, xl, 3)
    mate_tok(5, xl, 2, 2)
    tok_wait(False, 4, xr, 0)
    tok_wait(False, 5, xr, 1)
    mate_tok(6, xr, 0, 2)
    mate_wait(5, xl, 2, 2)
    mate_wait(6, xr, 0, 2)
    group((xr, xl), (0, 1))
    wait_sum(True, xfwd.at[0], 0)
    joined(xr, 0, xfwd.at[0])
    send_sum(xr, 0, True, xfin.at[0, 0], 2)
    wait_sum(False, xfwd.at[1], 0)
    joined(xl, 1, xfwd.at[1])
    send_sum(xl, 1, False, xfin.at[1, 1], 2)

    mate_wait(0, x, 0, 4)
    group((x, x), (0, 1))
    joined(x, 0)
    joined(x, 1)

    wait_sum(True, xfin.at[0, 1], 1)
    wait_sum(False, xfin.at[1, 0], 1)
    wait_sum(True, xfin.at[0, 0], 2)
    wait_sum(False, xfin.at[1, 1], 2)
    for h in range(2):
        @pl.loop(0, HALF // 16)
        def _(r):
            rr = pl.ds(pl.multiple_of(r * 16, 16), 16)
            oo = pl.ds(pl.multiple_of(h * HALF + r * 16, 16), 16)
            v = stream[oo, :].astype(F32) + pbuf[1, x, h, rr, :].astype(F32)
            v = v + xfin[0, h, rr, :].astype(F32) + xfin[1, h, rr, :].astype(F32)
            out[oo, :] = v.astype(BF16)

    @pl.when(c == half)
    def _():
        pass

    @pl.when(c != half)
    def _():
        over.wait_send()

    for cp in drains:
        cp.wait_send()
    gw.drain()
    gu.drain()
    gd.drain()
    for xx in range(4):
        for h in range(2):
            rcopy(pbuf.at[0, xx, h], precv.at[xx, h], p_s.at[xx, h], p_r.at[xx, h],
                  mate).wait_send()


def body(mixed, residual, mix_weight, norm_gain, up_weight, gate_weight, conv_weight, conv_bias,
         down_weight):
    parts = []
    for i in range(5):
        parts += [up_weight[:, i * 128:(i + 1) * 128], gate_weight[:, i * 128:(i + 1) * 128]]
    gap = jnp.zeros((128, 16), BF16)
    parts += [up_weight[:, 640:], gap, gate_weight[:, 640:], gap]
    ug_own = jnp.concatenate(parts, axis=1)
    taps = jnp.concatenate([conv_weight, conv_bias[None], jnp.zeros((4, 688), F32)], axis=0)
    taps = jnp.pad(taps, ((0, 0), (0, HID - 688)))

    any_ = pl.BlockSpec(memory_space=pl.ANY)
    vm = pl.BlockSpec(memory_space=pltpu.VMEM)
    dma = pltpu.SemaphoreType.DMA
    return pl.pallas_call(
        kernel,
        out_shape=jax.ShapeDtypeStruct((TOK, D), BF16),
        in_specs=[any_, any_, any_, vm, any_, vm, any_],
        out_specs=vm,
        scratch_shapes=[
            pltpu.VMEM((4, 4, 128, D), BF16),
            pltpu.VMEM((4, 4, 128, UG), BF16),
            pltpu.VMEM((4, 4, HID, 128), BF16),
            pltpu.VMEM((4, 2, 4, PIECE, D), BF16),
            pltpu.VMEM((TOK, D), BF16),
            pltpu.VMEM((TOK, D), BF16),
            pltpu.VMEM((TOK, D), BF16),
            pltpu.VMEM((8, 32, 256), BF16),
            pltpu.VMEM((256, D), BF16),
            pltpu.VMEM((16, 8, HID), F32),
            pltpu.VMEM((HALF, HID), BF16),
            pltpu.VMEM((2, 4, 2, HALF, D), BF16),
            pltpu.VMEM((4, 2, HALF, D), BF16),
            pltpu.VMEM((2, HALF, D), BF16),
            pltpu.VMEM((2, 2, HALF, D), BF16),
            dma((4,)), dma((4,)), dma((4,)),
            dma((3, 16)), dma((3, 16)),
            dma((16,)), dma((16,)),
            dma((2, 6)), dma((2, 6)),
            dma((7,)), dma((7,)),
            dma((8,)), dma((8,)),
            dma((4, 2)), dma((4, 2)),
            dma((2, 3)), dma((2, 3)),
        ],
        compiler_params=pltpu.CompilerParams(
            collective_id=0, has_side_effects=True, vmem_limit_bytes=67_043_328),
    )(mixed, residual, mix_weight, norm_gain[None], ug_own, taps, down_weight)


def solution(mesh):
    rows = P(("fs", "tp"), None)
    in_specs = (rows, rows, rows, P(), P("fs", "tp"), P("fs", "tp"), P(None, "tp"), P("tp"),
                P("tp", "fs"))
    return jax.shard_map(body, mesh=mesh, in_specs=in_specs, out_specs=rows, check_vma=False)
```

```python
import functools

import jax
import jax.numpy as jnp
from jax import lax
from jax.experimental import pallas as pl
from jax.experimental.pallas import tpu as pltpu
from jax.sharding import PartitionSpec as P

MESH = pl.DeviceIdType.MESH
F32 = jnp.float32
BF16 = jnp.bfloat16
NORM_EPS = 1e-06
GELU_C = 0.7978845608028654

D = 2048
TOK = 384
CH = 1024
HALF = 192
UG = 1408
HID = 768


def gated_gelu(v, gate):
    t = jnp.tanh(v * (GELU_C + (GELU_C * 0.044715) * (v * v)))
    v = 0.5 * v
    return (v + v * t) * gate


class Phases:
    def __init__(self):
        self.scope = None

    def __call__(self, name):
        if self.scope is not None:
            self.scope.__exit__(None, None, None)
        self.scope = jax.named_scope(name) if name else None
        if name:
            self.scope.__enter__()


class Gather:
    def __init__(self, ref, lo, rows, split, flip, fs, tp, send_sem, recv_sem):
        self.ref, self.lo, self.rows, self.split, self.flip = ref, lo, rows, split, flip
        self.tp, self.ss, self.rs = tp, send_sem, recv_sem
        z, y = fs // 4, fs % 4
        self.p = y * (1 - flip) + z * flip
        self.s = z * (1 - flip) + y * flip
        self.n = 0
        self.sends = []

    def zy(self, dp, ds):
        p, s = (self.p + dp + 4) % 4, (self.s + ds + 4) % 4
        return s * (1 - self.flip) + p * self.flip, p * (1 - self.flip) + s * self.flip

    def view(self, dp, ds, a=0, n=None):
        z, y = self.zy(dp, ds)
        n = self.rows if n is None else n
        return self.ref.at[z, y, pl.ds(self.lo + a, n)]

    def copy(self, k, blk, to):
        z, y = self.zy(*to)
        return pltpu.make_async_remote_copy(
            src_ref=blk, dst_ref=blk, send_sem=self.ss.at[self.n % 16], recv_sem=self.rs.at[k],
            device_id={"fs": z * 4 + y, "tp": self.tp}, device_id_type=MESH)

    def send(self, k, blk, to):
        c = self.copy(k, blk, to)
        c.start()
        self.sends.append(c)
        self.n += 1

    def wait(self, k, blk):
        self.copy(k, blk, (1, 0)).wait_recv()

    REL = (0, -1, 1, 2)

    def both(self, i):
        blk = self.view(self.REL[i], 0)
        self.send(4 + i, blk, (0, 1))
        self.send(8 + i, blk, (0, -1))

    def start(self):
        own = self.view(0, 0)
        self.send(0, own, (1, 0))
        self.send(1, own, (-1, 0))
        self.both(0)

    def near(self):
        s = self.split
        self.wait(0, self.view(-1, 0))
        self.send(2, self.view(-1, 0, 0, s), (1, 0))
        self.both(1)
        self.wait(1, self.view(1, 0))
        self.send(3, self.view(1, 0, s, self.rows - s), (-1, 0))
        self.both(2)

    def far(self):
        s = self.split
        self.wait(2, self.view(2, 0, 0, s))
        self.wait(3, self.view(2, 0, s, self.rows - s))
        self.both(3)

    def cross(self, i):
        below, above = self.view(self.REL[i], -1), self.view(self.REL[i], 1)
        self.wait(4 + i, below)
        if i < 2:
            self.send(12 + i, below, (0, 1))
        self.wait(8 + i, above)
        if i >= 2:
            self.send(12 + i, above, (0, -1))

    def last(self, i):
        self.wait(12 + i, self.view(self.REL[i], 2))

    def drain(self):
        for c in self.sends:
            c.wait_send()


def kernel(mixed, resid, wm_in, gain, up_in, gate_in, cw_in, cb_in, dw_in, out, xfin,
           wm, ug, dwn, upt, cw, tok, rr, mx, rs, hal, xexp, hu, hid, pbuf, precv, xfwd, base,
           lsem, wx_s, wx_r, g_s, g_r, d_s, d_r, t_s, t_r, td_s, td_r, rd_s, rd_r, h_s, h_r,
           p_s, p_r, x_s, x_r):
    fs, tp = lax.axis_index("fs"), lax.axis_index("tp")
    z, y, x, c = fs // 4, fs % 4, tp // 2, tp % 2
    xr, xl, xo = (x + 1) % 4, (x + 3) % 4, (x + 2) % 4
    mate = x * 2 + (1 - c)
    drains = []

    def rcopy(src, dst, ss, rsem, tp_to, fs_to=None):
        return pltpu.make_async_remote_copy(
            src_ref=src, dst_ref=dst, send_sem=ss, recv_sem=rsem,
            device_id={"fs": fs if fs_to is None else fs_to, "tp": tp_to}, device_id_type=MESH)

    ph = Phases()
    ph("load")
    ld_up = pltpu.make_async_copy(up_in, upt.at[0], lsem.at[0])
    ld_gate = pltpu.make_async_copy(gate_in, upt.at[1], lsem.at[4])
    ld_dw = pltpu.make_async_copy(dw_in, dwn.at[z, y, pl.ds(0, 688)], lsem.at[1])
    ld_mx = pltpu.make_async_copy(mixed, mx, lsem.at[2])
    ld_rs = pltpu.make_async_copy(resid, rs, lsem.at[3])
    ld_up.start()
    ld_gate.start()
    ld_mx.start()
    ld_rs.start()
    ld_dw.start()

    ph("barrier")
    bar = pltpu.get_barrier_semaphore()
    peers = [(fs, (tp + k) % 8) for k in range(1, 8)]
    peers += [(z * 4 + (y + 1) % 4, tp), (z * 4 + (y + 3) % 4, tp)]
    peers += [(((z + 1) % 4) * 4 + y, tp), (((z + 3) % 4) * 4 + y, tp)]
    for f, t in peers:
        pl.semaphore_signal(bar, inc=1, device_id={"fs": f, "tp": t}, device_id_type=MESH)
    pl.semaphore_wait(bar, len(peers))

    ph("wx")
    half = tp // 4
    row16 = pl.multiple_of(tp * 16, 16)
    slot = tp % 4
    stays, overs = [], []
    for ch in range(2):
        src = wm_in.at[:, pl.ds(ch * CH, CH)]
        dst = wm.at[ch, z, y, pl.ds(row16, 16)]
        for k in range(1, 4):
            cp = rcopy(src, dst, wx_s.at[ch, k], wx_r.at[ch, slot], ((x + k) % 4) * 2 + half)
            cp.start()
            drains.append(cp)
        stays.append(pltpu.make_async_copy(src, dst, wx_r.at[ch, slot]))
        overs.append(rcopy(src, dst, wx_s.at[ch, 0], wx_r.at[ch, slot], mate))

    @pl.when(c == half)
    def _():
        for cp in stays:
            cp.start()

    @pl.when(c != half)
    def _():
        for cp in overs:
            cp.start()

    lo = pl.multiple_of(c * 64, 64)
    other = pl.multiple_of(64 - lo, 64)
    gws = [Gather(wm.at[ch], lo, 64, 32, c, fs, tp, g_s.at[ch], g_r.at[ch]) for ch in range(2)]
    gw, gv = gws
    gu = Gather(ug, 0, 128, 64, c, fs, tp, g_s.at[2], g_r.at[2])
    gd = Gather(dwn, 0, 688, 352, 1 - c, fs, tp, g_s.at[3], g_r.at[3])

    def share(ch, k, dp, ds):
        blk = gws[ch].view(dp, ds)
        cp = rcopy(blk, blk, d_s.at[ch, k], d_r.at[ch, k], mate)
        cp.start()
        drains.append(cp)

    def shared(ch):
        for k in range(16):
            blk = wm.at[ch, k // 4, k % 4, pl.ds(other, 64)]
            rcopy(blk, blk, d_s.at[ch, k], d_r.at[ch, k], mate).wait_recv()

    def w_start(ch):
        for k in range(4):
            row = pl.multiple_of(lo + k * 16, 16)
            blk = wm.at[ch, z, y, pl.ds(row, 16)]
            rcopy(blk, blk, wx_s.at[ch, 0], wx_r.at[ch, k], mate).wait_recv()
        gws[ch].start()
        share(ch, 0, 0, 0)

    def w_near(ch):
        gws[ch].near()
        share(ch, 1, -1, 0)
        share(ch, 2, 1, 0)

    def w_far(ch):
        gws[ch].far()
        share(ch, 3, 2, 0)

    def w_cross(ch, i):
        gws[ch].cross(i)
        share(ch, 4 + 2 * i, Gather.REL[i], -1)
        share(ch, 5 + 2 * i, Gather.REL[i], 1)

    def w_last(ch):
        for i in range(4):
            gws[ch].last(i)
            share(ch, 12 + i, Gather.REL[i], 2)

    ph("w_start")
    w_start(0)
    w_start(1)

    ph("prep")
    zero_rows = jnp.zeros((HID - 688, 128), BF16)

    @pl.loop(0, 16)
    def _(f):
        dwn[f // 4, f % 4, pl.ds(688, HID - 688)] = zero_rows

    cw[...] = jnp.zeros((8, HID), F32)
    cw[0:3, 0:688] = cw_in[...]
    cw[3:4, 0:688] = cb_in[...].reshape(1, 688)
    ld_up.wait()
    ld_gate.wait()
    gn = gain[:, pl.ds(pl.multiple_of(fs * 128, 128), 128)]
    for i in range(5):
        for k in range(2):
            t = upt[k, pl.ds(i * 128, 128), :].astype(F32) * gn
            ug[z, y, :, pl.ds(i * 256 + k * 128, 128)] = t.T.astype(BF16)
    gap = jnp.zeros((16, 128), F32)
    t = [upt[0, pl.ds(640, 48), :].astype(F32) * gn, gap,
         upt[1, pl.ds(640, 48), :].astype(F32) * gn, gap]
    ug[z, y, :, pl.ds(1280, 128)] = jnp.concatenate(t, axis=0).T.astype(BF16)

    def mix(ch, n):
        w = wm[ch, :, :, :, n * 512:(n + 1) * 512].reshape(D, 512)
        s = jnp.dot(mx[...], w, preferred_element_type=F32)
        at = ch * CH + n * 512
        s = rs[:, at:at + 512].astype(F32) + s
        tok[x, c, ch, :, n * 512:(n + 1) * 512] = s.astype(BF16)

    def send_tok(xsrc, h, ch, to_right, sidx):
        blk = tok.at[xsrc, c, ch, pl.ds(h * HALF, HALF)]
        side = 0 if to_right else 1
        cp = rcopy(blk, blk, t_s.at[side, sidx], t_r.at[side, sidx],
                   (xr if to_right else xl) * 2 + c)
        cp.start()
        drains.append(cp)

    def tok_wait(from_left, idx, xsrc, h, ch):
        blk = tok.at[xsrc, c, ch, pl.ds(h * HALF, HALF)]
        side = 0 if from_left else 1
        rcopy(blk, blk, t_s.at[side, idx], t_r.at[side, idx], mate).wait_recv()

    def factor(xsrc, h):
        acc = None
        for ch in range(2):
            for k in range(CH // 128):
                v = tok[xsrc, c, ch, h * HALF:(h + 1) * HALF, k * 128:(k + 1) * 128].astype(F32)
                acc = v * v if acc is None else acc + v * v
        m = jnp.sum(acc, axis=-1, keepdims=True) * (1.0 / D)
        rr[xsrc, c, h] = jnp.broadcast_to(lax.rsqrt(m + NORM_EPS), (HALF, 128))

    def to_mate(k, xsrc, h):
        blk = tok.at[xsrc, c, :, pl.ds(h * HALF, HALF)]
        cp = rcopy(blk, blk, td_s.at[k], td_r.at[k], mate)
        cp.start()
        drains.append(cp)
        factor(xsrc, h)
        blk = rr.at[xsrc, c, h]
        cp = rcopy(blk, blk, rd_s.at[k], rd_r.at[k], mate)
        cp.start()
        drains.append(cp)

    def mate_wait(k, xsrc, h):
        blk = tok.at[xsrc, 1 - c, :, pl.ds(h * HALF, HALF)]
        rcopy(blk, blk, td_s.at[k], td_r.at[k], mate).wait_recv()
        blk = rr.at[xsrc, 1 - c, h]
        rcopy(blk, blk, rd_s.at[k], rd_r.at[k], mate).wait_recv()

    ph("w0_near")
    w_near(0)
    ph("w0_c0")
    w_cross(0, 0)
    ph("w0_far")
    w_far(0)
    ph("w1_near")
    w_near(1)
    ph("w0_c1")
    w_cross(0, 1)
    ph("w0_c2")
    w_cross(0, 2)
    ph("w1_c0")
    w_cross(1, 0)
    ph("w1_far")
    w_far(1)
    ph("w0_c3")
    w_cross(0, 3)
    ph("w1_c1")
    w_cross(1, 1)
    ph("w0_last")
    w_last(0)
    ph("w0_shared")
    shared(0)
    ld_mx.wait()
    ld_rs.wait()
    ph("mix0")
    mix(0, 0)
    ph("w1_c2")
    w_cross(1, 2)
    ph("mix1")
    mix(0, 1)
    send_tok(x, 0, 0, True, 0)
    send_tok(x, 1, 0, False, 0)
    send_tok(x, 1, 0, True, 1)
    send_tok(x, 0, 0, False, 1)
    ph("w1_c3")
    w_cross(1, 3)
    gu.start()
    ph("w1_last")
    w_last(1)
    ph("w1_shared")
    shared(1)
    ph("mix2")
    mix(1, 0)
    mix(1, 1)
    ph("tokA0")
    tok_wait(True, 0, xl, 0, 0)
    send_tok(xl, 0, 0, True, 2)
    send_tok(x, 0, 1, True, 3)
    tok_wait(False, 0, xr, 1, 0)
    send_tok(xr, 1, 0, False, 2)
    send_tok(x, 1, 1, False, 3)
    ph("gu_near")
    gu.near()
    ph("own_mate")
    to_mate(0, x, 0)
    to_mate(1, x, 1)

    tails = []
    for h in range(2):
        f = rr[x, c, h, HALF - 8:HALF, :][:, 0:1]
        for r in (6, 7):
            for q in range(8):
                ch, col = q // 4, (q % 4) * 256
                v = tok[x, c, ch, (h + 1) * HALF - 16:(h + 1) * HALF, col:col + 256].astype(F32)
                tails.append(v[r + 8:r + 9] * f[r:r + 1])
    hal[tp] = jnp.concatenate(tails, axis=0).astype(BF16)
    for k in range(1, 8):
        cp = rcopy(hal.at[tp], hal.at[tp], h_s.at[k], h_r.at[8 - k], (tp + k) % 8)
        cp.start()
        drains.append(cp)

    ph("gu_c0")
    gu.cross(0)
    ph("gu_far")
    gu.far()
    ld_dw.wait()
    gd.start()
    ph("gu_c1")
    gu.cross(1)
    ph("gu_c2")
    gu.cross(2)
    ph("gu_c3")
    gu.cross(3)
    ph("gd_near")
    gd.near()
    ph("gu_last")
    for i in range(4):
        gu.last(i)
    ph("tokA1")
    tok_wait(True, 3, xl, 0, 1)
    send_tok(xl, 0, 1, True, 4)
    send_tok(x, 1, 1, True, 5)
    tok_wait(False, 3, xr, 1, 1)
    send_tok(xr, 1, 1, False, 4)
    send_tok(x, 0, 1, False, 5)
    to_mate(2, xl, 0)
    to_mate(3, xr, 1)

    ph("xexp")
    for k in range(1, 8):
        src = (tp + k) % 8
        rcopy(hal.at[src], hal.at[src], h_s.at[k], h_r.at[k], mate).wait_recv()
    hv = hal[...].reshape(256, 256).astype(F32)
    rid = lax.broadcasted_iota(jnp.int32, (256, 256), 0) % 8
    for q in range(8):
        xexp[:, q * 256:(q + 1) * 256] = jnp.where(rid == q, hv, 0.0).astype(BF16)

    ph("gd_c0")
    gd.cross(0)
    ph("hu")

    @pl.loop(0, 6)
    def _(i):
        w = ug[:, :, :, pl.ds(pl.multiple_of(i * 256, 256), 128)].reshape(D, 128)
        r = jnp.dot(xexp[...], w, preferred_element_type=F32)
        r = jnp.sum(r.reshape(32, 8, 128), axis=1)
        cols = pl.ds(pl.multiple_of(i * 128, 128), 128)
        hu[0, 0:2, cols] = jnp.zeros((2, 128), F32)
        for q in range(15):
            hu[q + 1, 0:2, cols] = r[2 * q:2 * q + 2]

    row8 = lax.broadcasted_iota(jnp.int32, (8, 128), 0)

    def hidden(xs, hs, cc, to):
        unit = [(xs[k] * 2 + cc) * 2 + hs[k] for k in range(2)]
        a = [[tok[xs[k], cc, ch, hs[k] * HALF:(hs[k] + 1) * HALF, :] for ch in range(2)]
             for k in range(2)]
        a = jnp.concatenate([jnp.concatenate(v, axis=1) for v in a], axis=0)

        def act(i, u, g):
            cols = pl.ds(i * 128, 128)
            taps = [cw[k:k + 1, cols] for k in range(4)]
            for k in range(2):
                f = rr[xs[k], cc, hs[k]]
                uk, gk = u[k * HALF:(k + 1) * HALF] * f, g[k * HALF:(k + 1) * HALF] * f
                before = hu[unit[k], :, cols]
                h0, h1 = before[0:1], before[1:2]
                u1, u2 = pltpu.roll(uk, 1, 0), pltpu.roll(uk, 2, 0)
                f1 = jnp.where(row8 == 0, h1, u1[:8])
                f2 = jnp.where(row8 == 0, h0, jnp.where(row8 == 1, h1, u2[:8]))
                u1 = jnp.concatenate([f1, u1[8:]], axis=0)
                u2 = jnp.concatenate([f2, u2[8:]], axis=0)
                s = taps[3] + taps[0] * u2 + taps[1] * u1 + taps[2] * uk
                hid[to, pl.ds(k * HALF, HALF), cols] = gated_gelu(s, gk).astype(BF16)

        for i, width in ((0, 512), (2, 512), (4, 384)):
            w = ug[:, :, :, pl.ds(i * 256, width)].reshape(D, width)
            r = jnp.dot(a, w, preferred_element_type=F32)
            act(i, r[:, :128], r[:, 128:256])
            if width == 512:
                act(i + 1, r[:, 256:384], r[:, 384:])
            else:
                act(i + 1, r[:, 256:384], pltpu.roll(r[:, 256:384], 64, 1))

    def down(frm, xs, hs, cls):
        @pl.loop(0, 4)
        def _(n):
            w = jnp.concatenate([dwn[n, k] for k in range(4)], axis=1)
            r = jnp.dot(hid[frm], w, preferred_element_type=F32).astype(BF16)
            cols = pl.ds(pl.multiple_of(n * 512, 512), 512)
            for k in range(2):
                pbuf[cls, xs[k], hs[k], :, cols] = r[k * HALF:(k + 1) * HALF]

        @pl.when(cls == 0)
        def _():
            for k in range(2):
                rcopy(pbuf.at[0, xs[k], hs[k]], precv.at[xs[k], hs[k]], p_s.at[xs[k], hs[k]],
                      p_r.at[xs[k], hs[k]], mate).start()

    def core_of(cls):
        return (1 - c) * (1 - cls) + c * cls

    def group(xs, hs, slot=None, up=True, dn=True):
        @pl.loop(0, 2)
        def _(cls):
            to = cls if slot is None else slot + cls
            if up:
                hidden(xs, hs, core_of(cls), to)
            if dn:
                down(to, xs, hs, cls)

    ph("gd_far")
    gd.far()
    ph("gd_c1")
    gd.cross(1)
    ph("mate_own")
    mate_wait(0, x, 0)
    mate_wait(1, x, 1)
    ph("h_own")
    group((x, x), (0, 1), 2, dn=False)
    ph("gd_c23")
    gd.cross(2)
    gd.cross(3)

    ph("tok_opp")
    tok_wait(True, 2, xo, 0, 0)
    tok_wait(True, 4, xo, 0, 1)
    to_mate(4, xo, 0)
    tok_wait(False, 2, xo, 1, 0)
    tok_wait(False, 4, xo, 1, 1)
    to_mate(5, xo, 1)
    ph("mate_opp")
    mate_wait(4, xo, 0)
    mate_wait(5, xo, 1)
    ph("h_opp")
    group((xo, xo), (0, 1), 0, dn=False)
    ph("gd_last")
    for i in range(4):
        gd.last(i)
    mate_wait(2, xl, 0)
    mate_wait(3, xr, 1)

    def joined(xx, h, extra=None):
        rcopy(pbuf.at[0, xx, h], precv.at[xx, h], p_s.at[xx, h], p_r.at[xx, h], mate).wait_recv()

        @pl.loop(0, HALF // 16)
        def _(r):
            rr = pl.ds(pl.multiple_of(r * 16, 16), 16)
            v = pbuf[1, xx, h, rr, :].astype(F32) + precv[xx, h, rr, :].astype(F32)
            if extra is not None:
                v = v + extra[rr, :].astype(F32)
            pbuf[1, xx, h, rr, :] = v.astype(BF16)

    def send_sum(xx, h, to_right, dst, k):
        side = 0 if to_right else 1
        cp = rcopy(pbuf.at[1, xx, h], dst, x_s.at[side, k], x_r.at[side, k],
                   (xr if to_right else xl) * 2 + c)
        cp.start()
        drains.append(cp)

    def wait_sum(from_left, dst, k):
        side = 0 if from_left else 1
        rcopy(dst, dst, x_s.at[side, k], x_r.at[side, k], mate).wait_recv()

    ph("d_opp")
    group((xo, xo), (0, 1), 0, up=False)
    ph("j_opp")
    joined(xo, 0)
    send_sum(xo, 0, True, xfwd.at[0], 0)
    joined(xo, 1)
    send_sum(xo, 1, False, xfwd.at[1], 0)
    ph("g_near1")
    group((xr, xl), (1, 0))
    ph("j_near1")
    joined(xr, 1)
    send_sum(xr, 1, True, xfin.at[0, 1], 1)
    joined(xl, 0)
    send_sum(xl, 0, False, xfin.at[1, 0], 1)

    ph("tok_near2")
    tok_wait(True, 1, xl, 1, 0)
    tok_wait(True, 5, xl, 1, 1)
    to_mate(6, xl, 1)
    tok_wait(False, 1, xr, 0, 0)
    tok_wait(False, 5, xr, 0, 1)
    to_mate(7, xr, 0)
    mate_wait(6, xl, 1)
    mate_wait(7, xr, 0)
    ph("g_near2")
    group((xr, xl), (0, 1))
    ph("j_near2")
    wait_sum(True, xfwd.at[0], 0)
    joined(xr, 0, xfwd.at[0])
    send_sum(xr, 0, True, xfin.at[0, 0], 2)
    ph("j_near2b")
    wait_sum(False, xfwd.at[1], 0)
    joined(xl, 1, xfwd.at[1])
    send_sum(xl, 1, False, xfin.at[1, 1], 2)

    ph("d_own")
    group((x, x), (0, 1), 2, up=False)
    ph("base")
    outs = []
    for h in range(2):
        rcopy(pbuf.at[0, x, h], precv.at[x, h], p_s.at[x, h], p_r.at[x, h], mate).wait_recv()

        @pl.loop(0, HALF // 16)
        def _(r):
            row = pl.ds(pl.multiple_of(r * 16, 16), 16)
            at = pl.ds(pl.multiple_of(h * HALF + r * 16, 16), 16)
            for ch in range(2):
                cols = pl.ds(ch * CH, CH)
                v = tok[x, c, ch, at, :].astype(F32) + pbuf[1, x, h, row, cols].astype(F32)
                base[at, cols] = v + precv[x, h, row, cols].astype(F32)

        cp = pltpu.make_async_copy(base.at[pl.ds(h * HALF, HALF)], out.at[pl.ds(h * HALF, HALF)],
                                   lsem.at[5 + h])
        cp.start()
        outs.append(cp)
    for cp in outs:
        cp.wait()

    ph("fin_w1")
    wait_sum(True, xfin.at[0, 1], 1)
    wait_sum(False, xfin.at[1, 0], 1)
    ph("fin_w2")
    wait_sum(True, xfin.at[0, 0], 2)
    wait_sum(False, xfin.at[1, 1], 2)

    ph("drain")
    @pl.when(c != half)
    def _():
        for cp in overs:
            cp.wait_send()

    for cp in drains:
        cp.wait_send()
    gw.drain()
    gv.drain()
    gu.drain()
    gd.drain()
    for xx in range(4):
        for h in range(2):
            rcopy(pbuf.at[0, xx, h], precv.at[xx, h], p_s.at[xx, h], p_r.at[xx, h],
                  mate).wait_send()
    ph("")


def body(mixed, residual, mix_weight, norm_gain, up_weight, gate_weight, conv_weight, conv_bias,
         down_weight):
    any_ = pl.BlockSpec(memory_space=pl.ANY)
    vm = pl.BlockSpec(memory_space=pltpu.VMEM)
    dma = pltpu.SemaphoreType.DMA
    part, sums = pl.pallas_call(
        kernel,
        out_shape=(jax.ShapeDtypeStruct((TOK, D), F32),
                   jax.ShapeDtypeStruct((2, 2, HALF, D), BF16)),
        in_specs=[any_, any_, any_, vm, any_, any_, vm, vm, any_],
        out_specs=(any_, any_),
        scratch_shapes=[
            pltpu.VMEM((2, 4, 4, 128, CH), BF16),
            pltpu.VMEM((4, 4, 128, UG), BF16),
            pltpu.VMEM((4, 4, HID, 128), BF16),
            pltpu.VMEM((2, 688, 128), BF16),
            pltpu.VMEM((8, HID), F32),
            pltpu.VMEM((4, 2, 2, TOK, CH), BF16),
            pltpu.VMEM((4, 2, 2, HALF, 128), F32),
            pltpu.VMEM((TOK, D), BF16),
            pltpu.VMEM((TOK, D), BF16),
            pltpu.VMEM((8, 32, 256), BF16),
            pltpu.VMEM((256, D), BF16),
            pltpu.VMEM((16, 8, HID), F32),
            pltpu.VMEM((4, TOK, HID), BF16),
            pltpu.VMEM((2, 4, 2, HALF, D), BF16),
            pltpu.VMEM((4, 2, HALF, D), BF16),
            pltpu.VMEM((2, HALF, D), BF16),
            pltpu.VMEM((TOK, D), F32),
            dma((7,)), dma((2, 4)), dma((2, 4)),
            dma((4, 16)), dma((4, 16)),
            dma((2, 16)), dma((2, 16)),
            dma((2, 6)), dma((2, 6)),
            dma((8,)), dma((8,)), dma((8,)), dma((8,)),
            dma((8,)), dma((8,)),
            dma((4, 2)), dma((4, 2)),
            dma((2, 3)), dma((2, 3)),
        ],
        compiler_params=pltpu.CompilerParams(
            collective_id=0, has_side_effects=True, vmem_limit_bytes=67_043_328),
    )(mixed, residual, mix_weight, norm_gain[None], up_weight.T, gate_weight.T, conv_weight, conv_bias,
      down_weight)
    sums = sums.reshape(2, TOK, D).astype(F32)
    return (part + sums[0] + sums[1]).astype(BF16)


def solution(mesh):
    rows = P(("fs", "tp"), None)
    in_specs = (rows, rows, rows, P(), P("fs", "tp"), P("fs", "tp"), P(None, "tp"), P("tp"),
                P("tp", "fs"))
    return jax.shard_map(body, mesh=mesh, in_specs=in_specs, out_specs=rows, check_vma=False)
```

```python
import functools

import jax
import jax.numpy as jnp
from jax import lax
from jax.experimental import pallas as pl
from jax.experimental.pallas import tpu as pltpu
from jax.sharding import PartitionSpec as P

MESH = pl.DeviceIdType.MESH
F32 = jnp.float32
BF16 = jnp.bfloat16
NORM_EPS = 1e-06
GELU_C = 0.7978845608028654

D = 2048
TOK = 384
CH = 1024
HALF = 192
UG = 1408
HID = 768


def gated_gelu(v, gate):
    t = jnp.tanh(v * (GELU_C + (GELU_C * 0.044715) * (v * v)))
    v = 0.5 * v
    return (v + v * t) * gate


class Phases:
    def __init__(self):
        self.scope = None

    def __call__(self, name):
        if self.scope is not None:
            self.scope.__exit__(None, None, None)
        self.scope = jax.named_scope(name) if name else None
        if name:
            self.scope.__enter__()


class Gather:
    def __init__(self, ref, lo, rows, split, flip, fs, tp, send_sem, recv_sem):
        self.ref, self.lo, self.rows, self.split, self.flip = ref, lo, rows, split, flip
        self.tp, self.ss, self.rs = tp, send_sem, recv_sem
        z, y = fs // 4, fs % 4
        self.p = y * (1 - flip) + z * flip
        self.s = z * (1 - flip) + y * flip
        self.n = 0
        self.sends = []

    def zy(self, dp, ds):
        p, s = (self.p + dp + 4) % 4, (self.s + ds + 4) % 4
        return s * (1 - self.flip) + p * self.flip, p * (1 - self.flip) + s * self.flip

    def view(self, dp, ds, a=0, n=None):
        z, y = self.zy(dp, ds)
        n = self.rows if n is None else n
        return self.ref.at[z, y, pl.ds(self.lo + a, n)]

    def copy(self, k, blk, to):
        z, y = self.zy(*to)
        return pltpu.make_async_remote_copy(
            src_ref=blk, dst_ref=blk, send_sem=self.ss.at[self.n % 16], recv_sem=self.rs.at[k],
            device_id={"fs": z * 4 + y, "tp": self.tp}, device_id_type=MESH)

    def send(self, k, blk, to):
        c = self.copy(k, blk, to)
        c.start()
        self.sends.append(c)
        self.n += 1

    def wait(self, k, blk):
        self.copy(k, blk, (1, 0)).wait_recv()

    REL = (0, -1, 1, 2)

    def both(self, i):
        blk = self.view(self.REL[i], 0)
        self.send(4 + i, blk, (0, 1))
        self.send(8 + i, blk, (0, -1))

    def start(self):
        own = self.view(0, 0)
        self.send(0, own, (1, 0))
        self.send(1, own, (-1, 0))
        self.both(0)

    def near(self):
        s = self.split
        self.wait(0, self.view(-1, 0))
        self.send(2, self.view(-1, 0, 0, s), (1, 0))
        self.both(1)
        self.wait(1, self.view(1, 0))
        if s < self.rows:
            self.send(3, self.view(1, 0, s, self.rows - s), (-1, 0))
        self.both(2)

    def far(self):
        s = self.split
        self.wait(2, self.view(2, 0, 0, s))
        if s < self.rows:
            self.wait(3, self.view(2, 0, s, self.rows - s))
        self.both(3)

    def cross(self, i):
        below, above = self.view(self.REL[i], -1), self.view(self.REL[i], 1)
        self.wait(4 + i, below)
        if i < 2:
            self.send(12 + i, below, (0, 1))
        self.wait(8 + i, above)
        if i >= 2:
            self.send(12 + i, above, (0, -1))

    def last(self, i):
        self.wait(12 + i, self.view(self.REL[i], 2))

    def drain(self):
        for c in self.sends:
            c.wait_send()


def kernel(mixed, resid, wm_in, gain, up_in, gate_in, cw_in, cb_in, dw_in, out, sum_l, sum_r,
           wm, ug, dwn, upt, cw, tok, rr, mx, rs, hal, hu, hid, pbuf, precv, xfwd, base,
           lsem, wx_s, wx_r, g_s, g_r, d_s, d_r, t_s, t_r, td_s, td_r, rd_s, rd_r, h_s, h_r,
           p_s, p_r, x_s, x_r, xw_s, xw_r, xd_s, xd_r):
    fs, tp = lax.axis_index("fs"), lax.axis_index("tp")
    z, y, x, c = fs // 4, fs % 4, tp // 2, tp % 2
    xr, xl, xo = (x + 1) % 4, (x + 3) % 4, (x + 2) % 4
    mate = x * 2 + (1 - c)
    drains = []

    def rcopy(src, dst, ss, rsem, tp_to, fs_to=None):
        return pltpu.make_async_remote_copy(
            src_ref=src, dst_ref=dst, send_sem=ss, recv_sem=rsem,
            device_id={"fs": fs if fs_to is None else fs_to, "tp": tp_to}, device_id_type=MESH)

    ph = Phases()
    ph("load")
    ld_up = pltpu.make_async_copy(up_in, upt.at[0], lsem.at[0])
    ld_gate = pltpu.make_async_copy(gate_in, upt.at[1], lsem.at[4])
    ld_dw = pltpu.make_async_copy(dw_in, dwn.at[z, y, pl.ds(0, 688)], lsem.at[1])
    ld_mx = pltpu.make_async_copy(mixed, mx, lsem.at[2])
    ld_rs = pltpu.make_async_copy(resid, rs, lsem.at[3])
    row16 = pl.multiple_of(tp * 16, 16)
    ld_own = pltpu.make_async_copy(wm_in.at[:, pl.ds(CH, CH)], wm.at[1, z, y, pl.ds(row16, 16)],
                                   lsem.at[7])
    ld_own.start()
    ld_up.start()
    ld_gate.start()
    ld_mx.start()
    ld_rs.start()
    ld_dw.start()

    ph("barrier")
    bar = pltpu.get_barrier_semaphore()
    peers = [(fs, (tp + k) % 8) for k in range(1, 8)]
    peers += [(z * 4 + (y + 1) % 4, tp), (z * 4 + (y + 3) % 4, tp)]
    peers += [(((z + 1) % 4) * 4 + y, tp), (((z + 3) % 4) * 4 + y, tp)]
    for f, t in peers:
        pl.semaphore_signal(bar, inc=1, device_id={"fs": f, "tp": t}, device_id_type=MESH)
    pl.semaphore_wait(bar, len(peers))

    ph("wx")
    half = tp // 4
    slot = tp % 4
    src = wm_in.at[:, pl.ds(0, CH)]
    dst = wm.at[0, z, y, pl.ds(row16, 16)]
    for k in range(1, 4):
        cp = rcopy(src, dst, wx_s.at[k], wx_r.at[slot], ((x + k) % 4) * 2 + half)
        cp.start()
        drains.append(cp)
    stay = pltpu.make_async_copy(src, dst, wx_r.at[slot])
    over = rcopy(src, dst, wx_s.at[0], wx_r.at[slot], mate)

    @pl.when(c == half)
    def _():
        stay.start()

    @pl.when(c != half)
    def _():
        over.start()

    lo = pl.multiple_of(c * 64, 64)
    other = pl.multiple_of(64 - lo, 64)
    gw = Gather(wm.at[0], lo, 64, 32, c, fs, tp, g_s.at[0], g_r.at[0])
    gv = Gather(wm.at[1], row16, 16, 16, c, fs, tp, g_s.at[1], g_r.at[1])
    gu = Gather(ug, 0, 128, 64, c, fs, tp, g_s.at[2], g_r.at[2])
    gd = Gather(dwn, 0, 688, 352, 1 - c, fs, tp, g_s.at[3], g_r.at[3])

    def share(k, dp, ds):
        blk = gw.view(dp, ds)
        cp = rcopy(blk, blk, d_s.at[k], d_r.at[k], mate)
        cp.start()
        drains.append(cp)

    def w_cross(i):
        gw.cross(i)
        share(4 + 2 * i, Gather.REL[i], -1)
        share(5 + 2 * i, Gather.REL[i], 1)

    def w_rows(xsrc, core, z0=0, nz=4):
        return wm.at[1, pl.ds(z0, nz), :, pl.ds(pl.multiple_of((xsrc * 2 + core) * 16, 16), 16)]

    def line_send(to_right, k, xsrc, z0, nz):
        side, blk = 0 if to_right else 1, w_rows(xsrc, c, z0, nz)
        cp = rcopy(blk, blk, xw_s.at[side, k], xw_r.at[side, k], (xr if to_right else xl) * 2 + c)
        cp.start()
        drains.append(cp)

    def line_wait(from_left, k, xsrc, z0, nz):
        side, blk = 0 if from_left else 1, w_rows(xsrc, c, z0, nz)
        rcopy(blk, blk, xw_s.at[side, k], xw_r.at[side, k], mate).wait_recv()

    def line_share(k, xsrc):
        blk = w_rows(xsrc, c)
        cp = rcopy(blk, blk, xd_s.at[k], xd_r.at[k], mate)
        cp.start()
        drains.append(cp)

    ph("v_start")
    ld_own.wait()
    gv.start()
    gv.near()
    ph("w_start")
    for k in range(4):
        row = pl.multiple_of(lo + k * 16, 16)
        blk = wm.at[0, z, y, pl.ds(row, 16)]
        rcopy(blk, blk, wx_s.at[0], wx_r.at[k], mate).wait_recv()
    gw.start()
    share(0, 0, 0)
    ph("v_far")
    gv.cross(0)
    gv.far()

    ph("prep")
    zero_rows = jnp.zeros((HID - 688, 128), BF16)

    @pl.loop(0, 16)
    def _(f):
        dwn[f // 4, f % 4, pl.ds(688, HID - 688)] = zero_rows

    cw[...] = jnp.zeros((8, HID), F32)
    cw[0:3, 0:688] = cw_in[...]
    cw[3:4, 0:688] = cb_in[...].reshape(1, 688)
    ld_up.wait()
    ld_gate.wait()
    gn = gain[:, pl.ds(pl.multiple_of(fs * 128, 128), 128)]
    for i in range(5):
        for k in range(2):
            t = upt[k, pl.ds(i * 128, 128), :].astype(F32) * gn
            ug[z, y, :, pl.ds(i * 256 + k * 128, 128)] = t.T.astype(BF16)
    gap = jnp.zeros((16, 128), F32)
    t = [upt[0, pl.ds(640, 48), :].astype(F32) * gn, gap,
         upt[1, pl.ds(640, 48), :].astype(F32) * gn, gap]
    ug[z, y, :, pl.ds(1280, 128)] = jnp.concatenate(t, axis=0).T.astype(BF16)

    def mix(ch, n):
        w = wm[ch, :, :, :, n * 512:(n + 1) * 512].reshape(D, 512)
        s = jnp.dot(mx[...], w, preferred_element_type=F32)
        at = ch * CH + n * 512
        s = rs[:, at:at + 512].astype(F32) + s
        tok[x, c, ch, :, n * 512:(n + 1) * 512] = s.astype(BF16)

    def send_tok(xsrc, h, ch, to_right, sidx):
        blk = tok.at[xsrc, c, ch, pl.ds(h * HALF, HALF)]
        side = 0 if to_right else 1
        cp = rcopy(blk, blk, t_s.at[side, sidx], t_r.at[side, sidx],
                   (xr if to_right else xl) * 2 + c)
        cp.start()
        drains.append(cp)

    def tok_wait(from_left, idx, xsrc, h, ch):
        blk = tok.at[xsrc, c, ch, pl.ds(h * HALF, HALF)]
        side = 0 if from_left else 1
        rcopy(blk, blk, t_s.at[side, idx], t_r.at[side, idx], mate).wait_recv()

    def factor(xsrc, h):
        acc = None
        for ch in range(2):
            for k in range(CH // 128):
                v = tok[xsrc, c, ch, h * HALF:(h + 1) * HALF, k * 128:(k + 1) * 128].astype(F32)
                acc = v * v if acc is None else acc + v * v
        m = jnp.sum(acc, axis=-1, keepdims=True) * (1.0 / D)
        rr[xsrc, c, h] = jnp.broadcast_to(lax.rsqrt(m + NORM_EPS), (HALF, 128))

    def pass_on(k, xsrc, h, ch):
        blk = tok.at[xsrc, c, ch, pl.ds(h * HALF, HALF)]
        cp = rcopy(blk, blk, td_s.at[k, ch], td_r.at[k, ch], mate)
        cp.start()
        drains.append(cp)

    def pass_factor(k, xsrc, h):
        factor(xsrc, h)
        blk = rr.at[xsrc, c, h]
        cp = rcopy(blk, blk, rd_s.at[k], rd_r.at[k], mate)
        cp.start()
        drains.append(cp)

    def mate_wait(k, xsrc, h):
        for ch in range(2):
            blk = tok.at[xsrc, 1 - c, ch, pl.ds(h * HALF, HALF)]
            rcopy(blk, blk, td_s.at[k, ch], td_r.at[k, ch], mate).wait_recv()
        blk = rr.at[xsrc, 1 - c, h]
        rcopy(blk, blk, rd_s.at[k], rd_r.at[k], mate).wait_recv()

    ph("w_near")
    gw.near()
    share(1, -1, 0)
    share(2, 1, 0)
    ph("v_c12")
    gv.cross(1)
    gv.cross(2)
    ph("w_c0")
    w_cross(0)
    ph("v_last")
    gv.cross(3)
    for i in range(4):
        gv.last(i)
    line_send(True, 0, x, 0, 4)
    line_send(False, 0, x, 0, 4)
    line_share(0, x)
    ph("w_far")
    gw.far()
    share(3, 2, 0)
    ph("w_c1")
    w_cross(1)
    ph("w_c2")
    w_cross(2)
    ph("w_c3")
    w_cross(3)
    gu.start()
    ph("w_last")
    for i in range(4):
        gw.last(i)
        share(12 + i, Gather.REL[i], 2)
    ph("line_fwd")
    line_wait(True, 0, xl, 0, 4)
    line_send(True, 1, xl, 0, 2)
    line_share(1, xl)
    line_wait(False, 0, xr, 0, 4)
    line_send(False, 1, xr, 2, 2)
    line_share(2, xr)
    ph("w_shared")
    for k in range(16):
        blk = wm.at[0, k // 4, k % 4, pl.ds(other, 64)]
        rcopy(blk, blk, d_s.at[k], d_r.at[k], mate).wait_recv()
    ld_mx.wait()
    ld_rs.wait()
    ph("mix0")
    mix(0, 0)
    mix(0, 1)
    send_tok(x, 0, 0, True, 0)
    send_tok(x, 1, 0, False, 0)
    pass_on(0, x, 0, 0)
    pass_on(1, x, 1, 0)
    ph("gu_near")
    gu.near()
    ph("line_far")
    line_wait(True, 1, xo, 0, 2)
    line_wait(False, 1, xo, 2, 2)
    line_share(3, xo)
    for k, xsrc in enumerate((x, xl, xr, xo)):
        blk = w_rows(xsrc, 1 - c)
        rcopy(blk, blk, xd_s.at[k], xd_r.at[k], mate).wait_recv()
    ph("mix1")
    mix(1, 0)
    mix(1, 1)
    send_tok(x, 0, 1, True, 1)
    send_tok(x, 1, 1, False, 1)
    pass_on(0, x, 0, 1)
    pass_on(1, x, 1, 1)
    ph("gu_c0")
    gu.cross(0)
    ph("own_mate")
    pass_factor(0, x, 0)
    pass_factor(1, x, 1)

    tails = []
    for h in range(2):
        f = rr[x, c, h, HALF - 8:HALF, :][:, 0:1]
        for r in (6, 7):
            for q in range(8):
                ch, col = q // 4, (q % 4) * 256
                v = tok[x, c, ch, (h + 1) * HALF - 16:(h + 1) * HALF, col:col + 256].astype(F32)
                tails.append(v[r + 8:r + 9] * f[r:r + 1])
    hal[tp] = jnp.concatenate(tails, axis=0).astype(BF16)
    for k in range(1, 8):
        cp = rcopy(hal.at[tp], hal.at[tp], h_s.at[k], h_r.at[8 - k], (tp + k) % 8)
        cp.start()
        drains.append(cp)

    ph("gu_far")
    gu.far()
    ph("tokA0")
    tok_wait(True, 0, xl, 0, 0)
    send_tok(xl, 0, 0, True, 2)
    pass_on(2, xl, 0, 0)
    tok_wait(False, 0, xr, 1, 0)
    send_tok(xr, 1, 0, False, 2)
    pass_on(3, xr, 1, 0)
    ph("gu_c1")
    gu.cross(1)
    ph("gu_c2")
    gu.cross(2)
    ph("gu_c3")
    gu.cross(3)
    ld_dw.wait()
    gd.start()
    ph("tokA1")
    tok_wait(True, 1, xl, 0, 1)
    send_tok(xl, 0, 1, True, 3)
    send_tok(x, 1, 0, True, 4)
    send_tok(x, 1, 1, True, 5)
    pass_on(2, xl, 0, 1)
    tok_wait(False, 1, xr, 1, 1)
    send_tok(xr, 1, 1, False, 3)
    send_tok(x, 0, 0, False, 4)
    send_tok(x, 0, 1, False, 5)
    pass_on(3, xr, 1, 1)
    pass_factor(2, xl, 0)
    pass_factor(3, xr, 1)
    ph("gu_last")
    for i in range(4):
        gu.last(i)
    ph("gd_near")
    gd.near()

    ph("xexp")
    for k in range(1, 8):
        src = (tp + k) % 8
        rcopy(hal.at[src], hal.at[src], h_s.at[k], h_r.at[k], mate).wait_recv()
    hv = hal[...].reshape(256, 256).astype(F32)
    rid = lax.broadcasted_iota(jnp.int32, (256, 256), 0) % 8
    for q in range(8):
        mx[0:256, q * 256:(q + 1) * 256] = jnp.where(rid == q, hv, 0.0).astype(BF16)

    ph("gd_c0")
    gd.cross(0)
    ph("hu")

    @pl.loop(0, 6)
    def _(i):
        w = ug[:, :, :, pl.ds(pl.multiple_of(i * 256, 256), 128)].reshape(D, 128)
        r = jnp.dot(mx[0:256, :], w, preferred_element_type=F32)
        r = jnp.sum(r.reshape(32, 8, 128), axis=1)
        cols = pl.ds(pl.multiple_of(i * 128, 128), 128)
        hu[0, 0:2, cols] = jnp.zeros((2, 128), F32)
        for q in range(15):
            hu[q + 1, 0:2, cols] = r[2 * q:2 * q + 2]

    row8 = lax.broadcasted_iota(jnp.int32, (8, 128), 0)

    def hidden(xs, hs, cc, to):
        unit = [(xs[k] * 2 + cc) * 2 + hs[k] for k in range(2)]
        a = [[tok[xs[k], cc, ch, hs[k] * HALF:(hs[k] + 1) * HALF, :] for ch in range(2)]
             for k in range(2)]
        a = jnp.concatenate([jnp.concatenate(v, axis=1) for v in a], axis=0)

        def act(i, u, g):
            cols = pl.ds(i * 128, 128)
            taps = [cw[k:k + 1, cols] for k in range(4)]
            for k in range(2):
                f = rr[xs[k], cc, hs[k]]
                uk, gk = u[k * HALF:(k + 1) * HALF] * f, g[k * HALF:(k + 1) * HALF] * f
                before = hu[unit[k], :, cols]
                h0, h1 = before[0:1], before[1:2]
                u1, u2 = pltpu.roll(uk, 1, 0), pltpu.roll(uk, 2, 0)
                f1 = jnp.where(row8 == 0, h1, u1[:8])
                f2 = jnp.where(row8 == 0, h0, jnp.where(row8 == 1, h1, u2[:8]))
                u1 = jnp.concatenate([f1, u1[8:]], axis=0)
                u2 = jnp.concatenate([f2, u2[8:]], axis=0)
                s = taps[3] + taps[0] * u2 + taps[1] * u1 + taps[2] * uk
                hid[to, pl.ds(k * HALF, HALF), cols] = gated_gelu(s, gk).astype(BF16)

        for i, width in ((0, 512), (2, 512), (4, 384)):
            w = ug[:, :, :, pl.ds(i * 256, width)].reshape(D, width)
            r = jnp.dot(a, w, preferred_element_type=F32)
            act(i, r[:, :128], r[:, 128:256])
            if width == 512:
                act(i + 1, r[:, 256:384], r[:, 384:])
            else:
                act(i + 1, r[:, 256:384], pltpu.roll(r[:, 256:384], 64, 1))

    def down(frm, xs, hs, cls):
        @pl.loop(0, 4)
        def _(n):
            w = jnp.concatenate([dwn[n, k] for k in range(4)], axis=1)
            r = jnp.dot(hid[frm], w, preferred_element_type=F32).astype(BF16)
            cols = pl.ds(pl.multiple_of(n * 512, 512), 512)
            for k in range(2):
                pbuf[cls, xs[k], hs[k], :, cols] = r[k * HALF:(k + 1) * HALF]

        @pl.when(cls == 0)
        def _():
            for k in range(2):
                rcopy(pbuf.at[0, xs[k], hs[k]], precv.at[xs[k], hs[k]], p_s.at[xs[k], hs[k]],
                      p_r.at[xs[k], hs[k]], mate).start()

    def core_of(cls):
        return (1 - c) * (1 - cls) + c * cls

    def group(xs, hs, slot=None, up=True, dn=True):
        @pl.loop(0, 2)
        def _(cls):
            to = cls if slot is None else slot + cls
            if up:
                hidden(xs, hs, core_of(cls), to)
            if dn:
                down(to, xs, hs, cls)

    def joined(xx, h, extra=None):
        rcopy(pbuf.at[0, xx, h], precv.at[xx, h], p_s.at[xx, h], p_r.at[xx, h], mate).wait_recv()

        @pl.loop(0, HALF // 16)
        def _(r):
            rr = pl.ds(pl.multiple_of(r * 16, 16), 16)
            v = pbuf[1, xx, h, rr, :].astype(F32) + precv[xx, h, rr, :].astype(F32)
            if extra is not None:
                v = v + extra[rr, :].astype(F32)
            pbuf[1, xx, h, rr, :] = v.astype(BF16)

    def send_sum(xx, h, to_right, dst, k):
        side = 0 if to_right else 1
        cp = rcopy(pbuf.at[1, xx, h], dst, x_s.at[side, k], x_r.at[side, k],
                   (xr if to_right else xl) * 2 + c)
        cp.start()
        drains.append(cp)

    def wait_sum(from_left, dst, k):
        side = 0 if from_left else 1
        rcopy(dst, dst, x_s.at[side, k], x_r.at[side, k], mate).wait_recv()

    ph("gd_far")
    gd.far()
    ph("mate_own")
    mate_wait(0, x, 0)
    mate_wait(1, x, 1)
    ph("h_own0")
    hidden((x, x), (0, 1), core_of(0), 2)
    ph("gd_c12")
    gd.cross(1)
    gd.cross(2)
    ph("h_own1")
    hidden((x, x), (0, 1), core_of(1), 3)
    ph("gd_c3")
    gd.cross(3)

    ph("tok_opp")
    tok_wait(True, 2, xo, 0, 0)
    pass_on(4, xo, 0, 0)
    tok_wait(False, 2, xo, 1, 0)
    pass_on(5, xo, 1, 0)
    tok_wait(True, 3, xo, 0, 1)
    pass_on(4, xo, 0, 1)
    pass_factor(4, xo, 0)
    tok_wait(False, 3, xo, 1, 1)
    pass_on(5, xo, 1, 1)
    pass_factor(5, xo, 1)
    ph("h_opp1")
    hidden((xo, xo), (0, 1), core_of(1), 1)
    ph("mate_opp")
    mate_wait(4, xo, 0)
    mate_wait(5, xo, 1)
    ph("h_opp0")
    hidden((xo, xo), (0, 1), core_of(0), 0)
    ph("gd_last")
    for i in range(4):
        gd.last(i)

    ph("d_opp")
    group((xo, xo), (0, 1), 0, up=False)
    ph("j_opp")
    joined(xo, 0)
    send_sum(xo, 0, True, xfwd.at[0], 0)
    joined(xo, 1)
    send_sum(xo, 1, False, xfwd.at[1], 0)
    ph("mate_near1")
    mate_wait(2, xl, 0)
    mate_wait(3, xr, 1)
    ph("g_near1")
    group((xr, xl), (1, 0))
    ph("j_near1")
    joined(xr, 1)
    send_sum(xr, 1, True, sum_l.at[pl.ds(HALF, HALF)], 1)
    joined(xl, 0)
    send_sum(xl, 0, False, sum_r.at[pl.ds(0, HALF)], 1)

    ph("tok_near2")
    tok_wait(True, 4, xl, 1, 0)
    pass_on(6, xl, 1, 0)
    tok_wait(False, 4, xr, 0, 0)
    pass_on(7, xr, 0, 0)
    tok_wait(True, 5, xl, 1, 1)
    pass_on(6, xl, 1, 1)
    pass_factor(6, xl, 1)
    tok_wait(False, 5, xr, 0, 1)
    pass_on(7, xr, 0, 1)
    pass_factor(7, xr, 0)
    mate_wait(6, xl, 1)
    mate_wait(7, xr, 0)
    ph("g_near2")
    group((xr, xl), (0, 1))
    ph("j_near2")
    wait_sum(True, xfwd.at[0], 0)
    joined(xr, 0, xfwd.at[0])
    send_sum(xr, 0, True, sum_l.at[pl.ds(0, HALF)], 2)
    ph("j_near2b")
    wait_sum(False, xfwd.at[1], 0)
    joined(xl, 1, xfwd.at[1])
    send_sum(xl, 1, False, sum_r.at[pl.ds(HALF, HALF)], 2)

    ph("d_own")
    group((x, x), (0, 1), 2, up=False)
    ph("base")
    outs = []
    for h in range(2):
        rcopy(pbuf.at[0, x, h], precv.at[x, h], p_s.at[x, h], p_r.at[x, h], mate).wait_recv()

        @pl.loop(0, HALF // 16)
        def _(r):
            row = pl.ds(pl.multiple_of(r * 16, 16), 16)
            at = pl.ds(pl.multiple_of(h * HALF + r * 16, 16), 16)
            for ch in range(2):
                cols = pl.ds(ch * CH, CH)
                v = tok[x, c, ch, at, :].astype(F32) + pbuf[1, x, h, row, cols].astype(F32)
                base[at, cols] = v + precv[x, h, row, cols].astype(F32)

        cp = pltpu.make_async_copy(base.at[pl.ds(h * HALF, HALF)], out.at[pl.ds(h * HALF, HALF)],
                                   lsem.at[5 + h])
        cp.start()
        outs.append(cp)
    for cp in outs:
        cp.wait()

    ph("fin_w1")
    wait_sum(True, sum_l.at[pl.ds(HALF, HALF)], 1)
    wait_sum(False, sum_r.at[pl.ds(0, HALF)], 1)
    ph("fin_w2")
    wait_sum(True, sum_l.at[pl.ds(0, HALF)], 2)
    wait_sum(False, sum_r.at[pl.ds(HALF, HALF)], 2)

    ph("drain")
    @pl.when(c != half)
    def _():
        over.wait_send()

    for cp in drains:
        cp.wait_send()
    gw.drain()
    gv.drain()
    gu.drain()
    gd.drain()
    for xx in range(4):
        for h in range(2):
            rcopy(pbuf.at[0, xx, h], precv.at[xx, h], p_s.at[xx, h], p_r.at[xx, h],
                  mate).wait_send()
    ph("")


def body(mixed, residual, mix_weight, norm_gain, up_weight, gate_weight, conv_weight, conv_bias,
         down_weight):
    any_ = pl.BlockSpec(memory_space=pl.ANY)
    vm = pl.BlockSpec(memory_space=pltpu.VMEM)
    dma = pltpu.SemaphoreType.DMA
    part, sum_l, sum_r = pl.pallas_call(
        kernel,
        out_shape=(jax.ShapeDtypeStruct((TOK, D), F32),
                   jax.ShapeDtypeStruct((TOK, D), BF16), jax.ShapeDtypeStruct((TOK, D), BF16)),
        in_specs=[any_, any_, any_, vm, any_, any_, vm, vm, any_],
        out_specs=(any_, any_, any_),
        scratch_shapes=[
            pltpu.VMEM((2, 4, 4, 128, CH), BF16),
            pltpu.VMEM((4, 4, 128, UG), BF16),
            pltpu.VMEM((4, 4, HID, 128), BF16),
            pltpu.VMEM((2, 688, 128), BF16),
            pltpu.VMEM((8, HID), F32),
            pltpu.VMEM((4, 2, 2, TOK, CH), BF16),
            pltpu.VMEM((4, 2, 2, HALF, 128), F32),
            pltpu.VMEM((TOK, D), BF16),
            pltpu.VMEM((TOK, D), BF16),
            pltpu.VMEM((8, 32, 256), BF16),
            pltpu.VMEM((16, 8, HID), F32),
            pltpu.VMEM((4, TOK, HID), BF16),
            pltpu.VMEM((2, 4, 2, HALF, D), BF16),
            pltpu.VMEM((4, 2, HALF, D), BF16),
            pltpu.VMEM((2, HALF, D), BF16),
            pltpu.VMEM((TOK, D), F32),
            dma((8,)), dma((4,)), dma((4,)),
            dma((4, 16)), dma((4, 16)),
            dma((16,)), dma((16,)),
            dma((2, 6)), dma((2, 6)),
            dma((8, 2)), dma((8, 2)), dma((8,)), dma((8,)),
            dma((8,)), dma((8,)),
            dma((4, 2)), dma((4, 2)),
            dma((2, 3)), dma((2, 3)),
            dma((2, 2)), dma((2, 2)), dma((4,)), dma((4,)),
        ],
        compiler_params=pltpu.CompilerParams(
            collective_id=0, has_side_effects=True, vmem_limit_bytes=67_043_328),
    )(mixed, residual, mix_weight, norm_gain[None], up_weight.T, gate_weight.T, conv_weight, conv_bias,
      down_weight)
    return (part + sum_l.astype(F32) + sum_r.astype(F32)).astype(BF16)


def solution(mesh):
    rows = P(("fs", "tp"), None)
    in_specs = (rows, rows, rows, P(), P("fs", "tp"), P("fs", "tp"), P(None, "tp"), P("tp"),
                P("tp", "fs"))
    return jax.shard_map(body, mesh=mesh, in_specs=in_specs, out_specs=rows, check_vma=False)
```

```python
import functools

import jax
import jax.numpy as jnp
from jax import lax
from jax.experimental import pallas as pl
from jax.experimental.pallas import tpu as pltpu
from jax.sharding import PartitionSpec as P

MESH = pl.DeviceIdType.MESH
F32 = jnp.float32
BF16 = jnp.bfloat16
NORM_EPS = 1e-06
GELU_C = 0.7978845608028654

D = 2048
TOK = 384
CH = 1024
HALF = 192
UG = 1408
HID = 768


def gated_gelu(v, gate):
    t = jnp.tanh(v * (GELU_C + (GELU_C * 0.044715) * (v * v)))
    v = 0.5 * v
    return (v + v * t) * gate


class Phases:
    def __init__(self):
        self.scope = None

    def __call__(self, name):
        if self.scope is not None:
            self.scope.__exit__(None, None, None)
        self.scope = jax.named_scope(name) if name else None
        if name:
            self.scope.__enter__()


class Gather:
    def __init__(self, ref, lo, rows, split, flip, fs, tp, send_sem, recv_sem, total=None):
        self.total = total
        self.ref, self.lo, self.rows, self.split, self.flip = ref, lo, rows, split, flip
        self.tp, self.ss, self.rs = tp, send_sem, recv_sem
        z, y = fs // 4, fs % 4
        self.p = y * (1 - flip) + z * flip
        self.s = z * (1 - flip) + y * flip
        self.n = 0
        self.sends = []

    def zy(self, dp, ds):
        p, s = (self.p + dp + 4) % 4, (self.s + ds + 4) % 4
        return s * (1 - self.flip) + p * self.flip, p * (1 - self.flip) + s * self.flip

    def view(self, dp, ds, a=0, n=None):
        z, y = self.zy(dp, ds)
        n = self.rows if n is None else n
        return self.ref.at[z, y, pl.ds(self.lo + a, n)]

    def copy(self, k, blk, to):
        z, y = self.zy(*to)
        return pltpu.make_async_remote_copy(
            src_ref=blk, dst_ref=blk, send_sem=self.ss if self.total is not None else self.ss.at[self.n], recv_sem=self.rs.at[k],
            device_id={"fs": z * 4 + y, "tp": self.tp}, device_id_type=MESH)

    def send(self, k, blk, to):
        c = self.copy(k, blk, to)
        c.start()
        self.sends.append(c)
        self.n += 1

    def wait(self, k, blk):
        self.copy(k, blk, (1, 0)).wait_recv()

    REL = (0, -1, 1, 2)

    def both(self, i):
        blk = self.view(self.REL[i], 0)
        self.send(4 + i, blk, (0, 1))
        self.send(8 + i, blk, (0, -1))

    def start(self):
        own = self.view(0, 0)
        self.send(0, own, (1, 0))
        self.send(1, own, (-1, 0))
        self.both(0)

    def near(self):
        s = self.split
        self.wait(0, self.view(-1, 0))
        self.send(2, self.view(-1, 0, 0, s), (1, 0))
        self.both(1)
        self.wait(1, self.view(1, 0))
        if s < self.rows:
            self.send(3, self.view(1, 0, s, self.rows - s), (-1, 0))
        self.both(2)

    def far(self):
        s = self.split
        self.wait(2, self.view(2, 0, 0, s))
        if s < self.rows:
            self.wait(3, self.view(2, 0, s, self.rows - s))
        self.both(3)

    def cross(self, i):
        below, above = self.view(self.REL[i], -1), self.view(self.REL[i], 1)
        self.wait(4 + i, below)
        if i < 2:
            self.send(12 + i, below, (0, 1))
        self.wait(8 + i, above)
        if i >= 2:
            self.send(12 + i, above, (0, -1))

    def last(self, i):
        self.wait(12 + i, self.view(self.REL[i], 2))

    def drain(self):
        if self.total is not None:
            self.copy(0, self.total, (1, 0)).wait_send()
        else:
            for c in self.sends:
                c.wait_send()


def kernel(mixed, resid, wm_in, gain, up_in, gate_in, cw_in, cb_in, dw_in, out, last,
           wm, ug, dwn, upt, cw, tok, rr, mx, rs, hal, hu, hid, pbuf, precv, xfwd, base,
           lsem, wx_s, wx_r, g_s, g_r, t_r, td_r, rd_r, p_r, x_r, xw_r, one):
    fs, tp = lax.axis_index("fs"), lax.axis_index("tp")
    z, y, x, c = fs // 4, fs % 4, tp // 2, tp % 2
    xr, xl, xo = (x + 1) % 4, (x + 3) % 4, (x + 2) % 4
    mate = x * 2 + (1 - c)
    drains = []
    (w_sem, v_sem, d_s, d_r, t_s, td_s, rd_s, h_s, h_r, p_s, x_s, xw_s, xd_s, xd_r) = (
        one.at[k] for k in range(14))

    def rcopy(src, dst, ss, rsem, tp_to, fs_to=None):
        return pltpu.make_async_remote_copy(
            src_ref=src, dst_ref=dst, send_sem=ss, recv_sem=rsem,
            device_id={"fs": fs if fs_to is None else fs_to, "tp": tp_to}, device_id_type=MESH)

    ph = Phases()
    ph("load")
    ld_up = pltpu.make_async_copy(up_in, upt.at[0], lsem.at[0])
    ld_gate = pltpu.make_async_copy(gate_in, upt.at[1], lsem.at[4])
    ld_dw = pltpu.make_async_copy(dw_in, dwn.at[z, y, pl.ds(0, 688)], lsem.at[1])
    ld_mx = pltpu.make_async_copy(mixed, mx, lsem.at[2])
    ld_rs = pltpu.make_async_copy(resid, rs, lsem.at[3])
    row16 = pl.multiple_of(tp * 16, 16)
    ld_own = pltpu.make_async_copy(wm_in.at[:, pl.ds(CH, CH)], wm.at[1, z, y, pl.ds(row16, 16)],
                                   lsem.at[7])
    ld_own.start()
    ld_up.start()
    ld_gate.start()
    ld_mx.start()
    ld_rs.start()
    ld_dw.start()

    ph("barrier")
    bar = pltpu.get_barrier_semaphore()
    peers = [(fs, (tp + k) % 8) for k in range(1, 8)]
    peers += [(z * 4 + (y + 1) % 4, tp), (z * 4 + (y + 3) % 4, tp)]
    peers += [(((z + 1) % 4) * 4 + y, tp), (((z + 3) % 4) * 4 + y, tp)]
    for f, t in peers:
        pl.semaphore_signal(bar, inc=1, device_id={"fs": f, "tp": t}, device_id_type=MESH)
    pl.semaphore_wait(bar, len(peers))

    ph("wx")
    half = tp // 4
    slot = tp % 4
    src = wm_in.at[:, pl.ds(0, CH)]
    dst = wm.at[0, z, y, pl.ds(row16, 16)]
    for k in range(1, 4):
        cp = rcopy(src, dst, wx_s.at[k], wx_r.at[slot], ((x + k) % 4) * 2 + half)
        cp.start()
        drains.append(cp)
    stay = pltpu.make_async_copy(src, dst, wx_r.at[slot])
    over = rcopy(src, dst, wx_s.at[0], wx_r.at[slot], mate)

    @pl.when(c == half)
    def _():
        stay.start()

    @pl.when(c != half)
    def _():
        over.start()

    lo = pl.multiple_of(c * 64, 64)
    other = pl.multiple_of(64 - lo, 64)
    gw = Gather(wm.at[0], lo, 64, 32, c, fs, tp, w_sem, g_r.at[0],
                wm.at[0, pl.ds(0, 3), :, pl.ds(0, 80)])
    gv = Gather(wm.at[1], row16, 16, 16, c, fs, tp, v_sem, g_r.at[1],
                wm.at[1, pl.ds(0, 3), 0, pl.ds(0, 80)])
    gu = Gather(ug, 0, 128, 64, c, fs, tp, g_s.at[0], g_r.at[2])
    gd = Gather(dwn, 0, 688, 352, 1 - c, fs, tp, g_s.at[1], g_r.at[3])

    def share(k, dp, ds):
        blk = gw.view(dp, ds)
        cp = rcopy(blk, blk, d_s, d_r, mate)
        cp.start()

    def w_cross(i):
        gw.cross(i)
        share(4 + 2 * i, Gather.REL[i], -1)
        share(5 + 2 * i, Gather.REL[i], 1)

    def w_rows(xsrc, core, z0=0, nz=4):
        return wm.at[1, pl.ds(z0, nz), :, pl.ds(pl.multiple_of((xsrc * 2 + core) * 16, 16), 16)]

    def line_send(to_right, k, xsrc, z0, nz):
        side, blk = 0 if to_right else 1, w_rows(xsrc, c, z0, nz)
        cp = rcopy(blk, blk, xw_s, xw_r.at[side, k], (xr if to_right else xl) * 2 + c)
        cp.start()

    def line_wait(from_left, k, xsrc, z0, nz):
        side, blk = 0 if from_left else 1, w_rows(xsrc, c, z0, nz)
        rcopy(blk, blk, xw_s, xw_r.at[side, k], mate).wait_recv()

    def line_share(xsrc):
        blk = w_rows(xsrc, c)
        cp = rcopy(blk, blk, xd_s, xd_r, mate)
        cp.start()

    ph("v_start")
    ld_own.wait()
    gv.start()
    gv.near()
    ph("w_start")
    for k in range(4):
        row = pl.multiple_of(lo + k * 16, 16)
        blk = wm.at[0, z, y, pl.ds(row, 16)]
        rcopy(blk, blk, wx_s.at[0], wx_r.at[k], mate).wait_recv()
    gw.start()
    share(0, 0, 0)
    ph("v_far")
    gv.cross(0)
    gv.far()

    ph("prep")
    zero_rows = jnp.zeros((HID - 688, 128), BF16)

    @pl.loop(0, 16)
    def _(f):
        dwn[f // 4, f % 4, pl.ds(688, HID - 688)] = zero_rows

    cw[...] = jnp.zeros((8, HID), F32)
    cw[0:3, 0:688] = cw_in[...]
    cw[3:4, 0:688] = cb_in[...].reshape(1, 688)
    ld_up.wait()
    ld_gate.wait()
    gn = gain[:, pl.ds(pl.multiple_of(fs * 128, 128), 128)]
    for i in range(5):
        for k in range(2):
            t = upt[k, pl.ds(i * 128, 128), :].astype(F32) * gn
            ug[z, y, :, pl.ds(i * 256 + k * 128, 128)] = t.T.astype(BF16)
    gap = jnp.zeros((16, 128), F32)
    t = [upt[0, pl.ds(640, 48), :].astype(F32) * gn, gap,
         upt[1, pl.ds(640, 48), :].astype(F32) * gn, gap]
    ug[z, y, :, pl.ds(1280, 128)] = jnp.concatenate(t, axis=0).T.astype(BF16)

    def mix(ch, n):
        w = wm[ch, :, :, :, n * 512:(n + 1) * 512].reshape(D, 512)
        s = jnp.dot(mx[...], w, preferred_element_type=F32)
        at = ch * CH + n * 512
        s = rs[:, at:at + 512].astype(F32) + s
        tok[x, c, ch, :, n * 512:(n + 1) * 512] = s.astype(BF16)

    def send_tok(xsrc, h, ch, to_right, sidx):
        blk = tok.at[xsrc, c, ch, pl.ds(h * HALF, HALF)]
        side = 0 if to_right else 1
        cp = rcopy(blk, blk, t_s, t_r.at[side, sidx],
                   (xr if to_right else xl) * 2 + c)
        cp.start()

    def tok_wait(from_left, idx, xsrc, h, ch):
        blk = tok.at[xsrc, c, ch, pl.ds(h * HALF, HALF)]
        side = 0 if from_left else 1
        rcopy(blk, blk, t_s, t_r.at[side, idx], mate).wait_recv()

    def factor(xsrc, h):
        acc = None
        for ch in range(2):
            for k in range(CH // 128):
                v = tok[xsrc, c, ch, h * HALF:(h + 1) * HALF, k * 128:(k + 1) * 128].astype(F32)
                acc = v * v if acc is None else acc + v * v
        m = jnp.sum(acc, axis=-1, keepdims=True) * (1.0 / D)
        rr[xsrc, c, h] = jnp.broadcast_to(lax.rsqrt(m + NORM_EPS), (HALF, 128))

    def pass_on(k, xsrc, h, ch):
        blk = tok.at[xsrc, c, ch, pl.ds(h * HALF, HALF)]
        cp = rcopy(blk, blk, td_s, td_r.at[k], mate)
        cp.start()

    def pass_factor(k, xsrc, h):
        factor(xsrc, h)
        blk = rr.at[xsrc, c, h]
        cp = rcopy(blk, blk, rd_s, rd_r.at[k], mate)
        cp.start()

    def mate_wait(k, xsrc, h):
        blk = tok.at[xsrc, 1 - c, :, pl.ds(h * HALF, HALF)]
        rcopy(blk, blk, td_s, td_r.at[k], mate).wait_recv()
        blk = rr.at[xsrc, 1 - c, h]
        rcopy(blk, blk, rd_s, rd_r.at[k], mate).wait_recv()

    ph("w_near")
    gw.near()
    share(1, -1, 0)
    share(2, 1, 0)
    ph("v_c12")
    gv.cross(1)
    gv.cross(2)
    ph("w_c0")
    w_cross(0)
    ph("v_last")
    gv.cross(3)
    for i in range(4):
        gv.last(i)
    line_send(True, 0, x, 0, 4)
    line_send(False, 0, x, 0, 4)
    line_share(x)
    ph("w_far")
    gw.far()
    share(3, 2, 0)
    ph("w_c1")
    w_cross(1)
    ph("w_c2")
    w_cross(2)
    ph("w_c3")
    w_cross(3)
    gu.start()
    ph("w_last")
    for i in range(4):
        gw.last(i)
        share(12 + i, Gather.REL[i], 2)
    ph("line_fwd")
    line_wait(True, 0, xl, 0, 4)
    line_send(True, 1, xl, 0, 2)
    line_share(xl)
    line_wait(False, 0, xr, 0, 4)
    line_send(False, 1, xr, 2, 2)
    line_share(xr)
    ph("w_shared")
    blk = wm.at[0, :, :, pl.ds(other, 64)]
    rcopy(blk, blk, d_s, d_r, mate).wait_recv()
    ld_mx.wait()
    ld_rs.wait()
    ph("mix0")
    mix(0, 0)
    mix(0, 1)
    send_tok(x, 0, 0, True, 0)
    send_tok(x, 1, 0, False, 0)
    pass_on(0, x, 0, 0)
    pass_on(1, x, 1, 0)
    ph("gu_near")
    gu.near()
    ph("line_far")
    line_wait(True, 1, xo, 0, 2)
    line_wait(False, 1, xo, 2, 2)
    line_share(xo)
    blk = wm.at[1, :, :, pl.ds(0, 64)]
    rcopy(blk, blk, xd_s, xd_r, mate).wait_recv()
    ph("mix1")
    mix(1, 0)
    mix(1, 1)
    send_tok(x, 0, 1, True, 1)
    send_tok(x, 1, 1, False, 1)
    pass_on(0, x, 0, 1)
    pass_on(1, x, 1, 1)
    ph("gu_c0")
    gu.cross(0)
    ph("own_mate")
    pass_factor(0, x, 0)
    pass_factor(1, x, 1)

    tails = []
    for h in range(2):
        f = rr[x, c, h, HALF - 8:HALF, :][:, 0:1]
        for r in (6, 7):
            for q in range(8):
                ch, col = q // 4, (q % 4) * 256
                v = tok[x, c, ch, (h + 1) * HALF - 16:(h + 1) * HALF, col:col + 256].astype(F32)
                tails.append(v[r + 8:r + 9] * f[r:r + 1])
    hal[tp] = jnp.concatenate(tails, axis=0).astype(BF16)
    for k in range(1, 8):
        rcopy(hal.at[tp], hal.at[tp], h_s, h_r, (tp + k) % 8).start()

    ph("gu_far")
    gu.far()
    ph("tokA0")
    tok_wait(True, 0, xl, 0, 0)
    send_tok(xl, 0, 0, True, 2)
    pass_on(2, xl, 0, 0)
    tok_wait(False, 0, xr, 1, 0)
    send_tok(xr, 1, 0, False, 2)
    pass_on(3, xr, 1, 0)
    ph("gu_c1")
    gu.cross(1)
    ph("gu_c2")
    gu.cross(2)
    ph("gu_c3")
    gu.cross(3)
    ld_dw.wait()
    gd.start()
    ph("tokA1")
    tok_wait(True, 1, xl, 0, 1)
    send_tok(xl, 0, 1, True, 3)
    send_tok(x, 1, 0, True, 4)
    send_tok(x, 1, 1, True, 5)
    pass_on(2, xl, 0, 1)
    tok_wait(False, 1, xr, 1, 1)
    send_tok(xr, 1, 1, False, 3)
    send_tok(x, 0, 0, False, 4)
    send_tok(x, 0, 1, False, 5)
    pass_on(3, xr, 1, 1)
    pass_factor(2, xl, 0)
    pass_factor(3, xr, 1)
    ph("gu_last")
    for i in range(4):
        gu.last(i)
    ph("gd_near")
    gd.near()

    ph("xexp")
    blk = hal.at[pl.ds(0, 7)]
    rcopy(blk, blk, h_s, h_r, mate).wait_recv()
    hv = hal[...].reshape(256, 256).astype(F32)
    rid = lax.broadcasted_iota(jnp.int32, (256, 256), 0) % 8
    for q in range(8):
        mx[0:256, q * 256:(q + 1) * 256] = jnp.where(rid == q, hv, 0.0).astype(BF16)

    ph("gd_c0")
    gd.cross(0)
    ph("hu")

    @pl.loop(0, 6)
    def _(i):
        w = ug[:, :, :, pl.ds(pl.multiple_of(i * 256, 256), 128)].reshape(D, 128)
        r = jnp.dot(mx[0:256, :], w, preferred_element_type=F32)
        r = jnp.sum(r.reshape(32, 8, 128), axis=1)
        cols = pl.ds(pl.multiple_of(i * 128, 128), 128)
        hu[0, 0:2, cols] = jnp.zeros((2, 128), F32)
        for q in range(15):
            hu[q + 1, 0:2, cols] = r[2 * q:2 * q + 2]

    row8 = lax.broadcasted_iota(jnp.int32, (8, 128), 0)

    def hidden(xs, hs, cc, to):
        unit = [(xs[k] * 2 + cc) * 2 + hs[k] for k in range(2)]
        a = [[tok[xs[k], cc, ch, hs[k] * HALF:(hs[k] + 1) * HALF, :] for ch in range(2)]
             for k in range(2)]
        a = jnp.concatenate([jnp.concatenate(v, axis=1) for v in a], axis=0)

        def act(i, u, g):
            cols = pl.ds(i * 128, 128)
            taps = [cw[k:k + 1, cols] for k in range(4)]
            for k in range(2):
                f = rr[xs[k], cc, hs[k]]
                uk, gk = u[k * HALF:(k + 1) * HALF] * f, g[k * HALF:(k + 1) * HALF] * f
                before = hu[unit[k], :, cols]
                h0, h1 = before[0:1], before[1:2]
                u1, u2 = pltpu.roll(uk, 1, 0), pltpu.roll(uk, 2, 0)
                f1 = jnp.where(row8 == 0, h1, u1[:8])
                f2 = jnp.where(row8 == 0, h0, jnp.where(row8 == 1, h1, u2[:8]))
                u1 = jnp.concatenate([f1, u1[8:]], axis=0)
                u2 = jnp.concatenate([f2, u2[8:]], axis=0)
                s = taps[3] + taps[0] * u2 + taps[1] * u1 + taps[2] * uk
                hid[to, pl.ds(k * HALF, HALF), cols] = gated_gelu(s, gk).astype(BF16)

        for i, width in ((0, 512), (2, 512), (4, 384)):
            w = ug[:, :, :, pl.ds(i * 256, width)].reshape(D, width)
            r = jnp.dot(a, w, preferred_element_type=F32)
            act(i, r[:, :128], r[:, 128:256])
            if width == 512:
                act(i + 1, r[:, 256:384], r[:, 384:])
            else:
                act(i + 1, r[:, 256:384], pltpu.roll(r[:, 256:384], 64, 1))

    def down(frm, xs, hs, cls):
        @pl.loop(0, 4)
        def _(n):
            w = jnp.concatenate([dwn[n, k] for k in range(4)], axis=1)
            r = jnp.dot(hid[frm], w, preferred_element_type=F32).astype(BF16)
            cols = pl.ds(pl.multiple_of(n * 512, 512), 512)
            for k in range(2):
                pbuf[cls, xs[k], hs[k], :, cols] = r[k * HALF:(k + 1) * HALF]

        @pl.when(cls == 0)
        def _():
            for k in range(2):
                rcopy(pbuf.at[0, xs[k], hs[k]], precv.at[xs[k], hs[k]], p_s,
                      p_r.at[xs[k], hs[k]], mate).start()

    def core_of(cls):
        return (1 - c) * (1 - cls) + c * cls

    def group(xs, hs, slot=None, up=True, dn=True):
        @pl.loop(0, 2)
        def _(cls):
            to = cls if slot is None else slot + cls
            if up:
                hidden(xs, hs, core_of(cls), to)
            if dn:
                down(to, xs, hs, cls)

    def joined(xx, h, extra=None):
        rcopy(pbuf.at[0, xx, h], precv.at[xx, h], p_s, p_r.at[xx, h], mate).wait_recv()

        @pl.loop(0, HALF // 16)
        def _(r):
            rr = pl.ds(pl.multiple_of(r * 16, 16), 16)
            v = pbuf[1, xx, h, rr, :].astype(F32) + precv[xx, h, rr, :].astype(F32)
            if extra is not None:
                v = v + extra[rr, :].astype(F32)
            pbuf[1, xx, h, rr, :] = v.astype(BF16)

    def send_sum(xx, h, to_right, dst, k):
        side = 0 if to_right else 1
        cp = rcopy(pbuf.at[1, xx, h], dst, x_s, x_r.at[side, k],
                   (xr if to_right else xl) * 2 + c)
        cp.start()

    def wait_sum(from_left, dst, k):
        side = 0 if from_left else 1
        rcopy(dst, dst, x_s, x_r.at[side, k], mate).wait_recv()

    ph("gd_far")
    gd.far()
    ph("mate_own")
    mate_wait(0, x, 0)
    mate_wait(1, x, 1)
    ph("h_own0")
    hidden((x, x), (0, 1), core_of(0), 2)
    ph("gd_c12")
    gd.cross(1)
    gd.cross(2)
    ph("h_own1")
    hidden((x, x), (0, 1), core_of(1), 3)
    ph("gd_c3")
    gd.cross(3)

    ph("tok_opp")
    tok_wait(True, 2, xo, 0, 0)
    pass_on(4, xo, 0, 0)
    tok_wait(False, 2, xo, 1, 0)
    pass_on(5, xo, 1, 0)
    tok_wait(True, 3, xo, 0, 1)
    pass_on(4, xo, 0, 1)
    pass_factor(4, xo, 0)
    tok_wait(False, 3, xo, 1, 1)
    pass_on(5, xo, 1, 1)
    pass_factor(5, xo, 1)
    ph("h_opp1")
    hidden((xo, xo), (0, 1), core_of(1), 1)
    ph("mate_opp")
    mate_wait(4, xo, 0)
    mate_wait(5, xo, 1)
    ph("h_opp0")
    hidden((xo, xo), (0, 1), core_of(0), 0)
    ph("gd_last")
    for i in range(4):
        gd.last(i)

    ph("d_opp")
    group((xo, xo), (0, 1), 0, up=False)
    ph("j_opp")
    joined(xo, 0)
    send_sum(xo, 0, True, xfwd.at[0], 0)
    joined(xo, 1)
    send_sum(xo, 1, False, xfwd.at[1], 0)
    ph("mate_near1")
    mate_wait(2, xl, 0)
    mate_wait(3, xr, 1)
    ph("g_near1")
    group((xr, xl), (1, 0))
    ph("j_near1")
    joined(xr, 1)
    send_sum(xr, 1, True, rs.at[pl.ds(HALF, HALF)], 1)
    joined(xl, 0)
    send_sum(xl, 0, False, rs.at[pl.ds(0, HALF)], 1)

    ph("tok_near2")
    tok_wait(True, 4, xl, 1, 0)
    pass_on(6, xl, 1, 0)
    tok_wait(False, 4, xr, 0, 0)
    pass_on(7, xr, 0, 0)
    tok_wait(True, 5, xl, 1, 1)
    pass_on(6, xl, 1, 1)
    pass_factor(6, xl, 1)
    tok_wait(False, 5, xr, 0, 1)
    pass_on(7, xr, 0, 1)
    pass_factor(7, xr, 0)
    mate_wait(6, xl, 1)
    mate_wait(7, xr, 0)
    ph("g_near2")
    group((xr, xl), (0, 1))
    ph("j_near2")
    wait_sum(True, xfwd.at[0], 0)
    joined(xr, 0, xfwd.at[0])
    send_sum(xr, 0, True, last.at[pl.ds(0, HALF)], 2)
    ph("j_near2b")
    wait_sum(False, xfwd.at[1], 0)
    joined(xl, 1, xfwd.at[1])
    send_sum(xl, 1, False, last.at[pl.ds(HALF, HALF)], 2)

    ph("d_own")
    group((x, x), (0, 1), 2, up=False)
    ph("base")
    outs = []
    for h in range(2):
        rcopy(pbuf.at[0, x, h], precv.at[x, h], p_s, p_r.at[x, h], mate).wait_recv()

        @pl.loop(0, HALF // 16)
        def _(r):
            row = pl.ds(pl.multiple_of(r * 16, 16), 16)
            at = pl.ds(pl.multiple_of(h * HALF + r * 16, 16), 16)
            for ch in range(2):
                cols = pl.ds(ch * CH, CH)
                v = tok[x, c, ch, at, :].astype(F32) + pbuf[1, x, h, row, cols].astype(F32)
                base[at, cols] = v + precv[x, h, row, cols].astype(F32)

    ph("fin_w1")
    wait_sum(True, rs.at[pl.ds(HALF, HALF)], 1)
    wait_sum(False, rs.at[pl.ds(0, HALF)], 1)
    for h in range(2):
        @pl.loop(h * 12, h * 12 + 12)
        def _(r):
            at = pl.ds(pl.multiple_of(r * 16, 16), 16)
            base[at, :] = base[at, :] + rs[at, :].astype(F32)

        cp = pltpu.make_async_copy(base.at[pl.ds(h * HALF, HALF)], out.at[pl.ds(h * HALF, HALF)],
                                   lsem.at[5 + h])
        cp.start()
        outs.append(cp)
    for cp in outs:
        cp.wait()

    ph("fin_w2")
    wait_sum(True, last.at[pl.ds(0, HALF)], 2)
    wait_sum(False, last.at[pl.ds(HALF, HALF)], 2)

    ph("drain")
    @pl.when(c != half)
    def _():
        over.wait_send()

    for cp in drains:
        cp.wait_send()
    gw.drain()
    gv.drain()
    gu.drain()
    gd.drain()
    for sem, view in (
            (d_s, wm.at[0, :, :, pl.ds(0, 64)]),
            (xw_s, wm.at[1, :, :, pl.ds(0, 48)]),
            (xd_s, wm.at[1, :, :, pl.ds(0, 64)]),
            (t_s, tok.at[pl.ds(0, 3), 0]),
            (td_s, tok.at[:, 0]),
            (rd_s, rr.at[:, 0]),
            (h_s, hal.at[pl.ds(0, 7)]),
            (p_s, pbuf.at[0]),
            (x_s, precv.at[pl.ds(0, 3)])):
        rcopy(view, view, sem, lsem.at[0], mate).wait_send()
    ph("")


def body(mixed, residual, mix_weight, norm_gain, up_weight, gate_weight, conv_weight, conv_bias,
         down_weight):
    any_ = pl.BlockSpec(memory_space=pl.ANY)
    vm = pl.BlockSpec(memory_space=pltpu.VMEM)
    dma = pltpu.SemaphoreType.DMA
    part, last = pl.pallas_call(
        kernel,
        out_shape=(jax.ShapeDtypeStruct((TOK, D), F32),
                   jax.ShapeDtypeStruct((TOK, D), BF16)),
        in_specs=[any_, any_, any_, vm, any_, any_, vm, vm, any_],
        out_specs=(any_, any_),
        scratch_shapes=[
            pltpu.VMEM((2, 4, 4, 128, CH), BF16),
            pltpu.VMEM((4, 4, 128, UG), BF16),
            pltpu.VMEM((4, 4, HID, 128), BF16),
            pltpu.VMEM((2, 688, 128), BF16),
            pltpu.VMEM((8, HID), F32),
            pltpu.VMEM((4, 2, 2, TOK, CH), BF16),
            pltpu.VMEM((4, 2, 2, HALF, 128), F32),
            pltpu.VMEM((TOK, D), BF16),
            pltpu.VMEM((TOK, D), BF16),
            pltpu.VMEM((8, 32, 256), BF16),
            pltpu.VMEM((16, 8, HID), F32),
            pltpu.VMEM((4, TOK, HID), BF16),
            pltpu.VMEM((2, 4, 2, HALF, D), BF16),
            pltpu.VMEM((4, 2, HALF, D), BF16),
            pltpu.VMEM((2, HALF, D), BF16),
            pltpu.VMEM((TOK, D), F32),
            dma((8,)), dma((4,)), dma((4,)),
            dma((2, 16)), dma((4, 16)),
            dma((2, 6)), dma((8,)), dma((8,)),
            dma((4, 2)), dma((2, 3)), dma((2, 2)),
            dma((14,)),
        ],
        compiler_params=pltpu.CompilerParams(
            collective_id=0, has_side_effects=True, vmem_limit_bytes=67_043_328),
    )(mixed, residual, mix_weight, norm_gain[None], up_weight.T, gate_weight.T, conv_weight, conv_bias,
      down_weight)
    return (part + last.astype(F32)).astype(BF16)


def solution(mesh):
    rows = P(("fs", "tp"), None)
    in_specs = (rows, rows, rows, P(), P("fs", "tp"), P("fs", "tp"), P(None, "tp"), P("tp"),
                P("tp", "fs"))
    return jax.shard_map(body, mesh=mesh, in_specs=in_specs, out_specs=rows, check_vma=False)
```

```python
import functools

import jax
import jax.numpy as jnp
from jax import lax
from jax.experimental import pallas as pl
from jax.experimental.pallas import tpu as pltpu
from jax.sharding import PartitionSpec as P

MESH = pl.DeviceIdType.MESH
F32 = jnp.float32
BF16 = jnp.bfloat16
NORM_EPS = 1e-06
GELU_C = 0.7978845608028654

D = 2048
TOK = 384
CH = 1024
HALF = 192
UG = 1408
HID = 768


def gated_gelu(v, gate):
    t = jnp.tanh(v * (GELU_C + (GELU_C * 0.044715) * (v * v)))
    v = 0.5 * v
    return (v + v * t) * gate


class Phases:
    def __init__(self):
        self.scope = None

    def __call__(self, name):
        if self.scope is not None:
            self.scope.__exit__(None, None, None)
        self.scope = jax.named_scope(name) if name else None
        if name:
            self.scope.__enter__()


class Gather:
    def __init__(self, ref, lo, rows, split, flip, fs, tp, send_sem, recv_sem, total=None):
        self.total = total
        self.ref, self.lo, self.rows, self.split, self.flip = ref, lo, rows, split, flip
        self.tp, self.ss, self.rs = tp, send_sem, recv_sem
        z, y = fs // 4, fs % 4
        self.p = y * (1 - flip) + z * flip
        self.s = z * (1 - flip) + y * flip
        self.n = 0
        self.sends = []

    def zy(self, dp, ds):
        p, s = (self.p + dp + 4) % 4, (self.s + ds + 4) % 4
        return s * (1 - self.flip) + p * self.flip, p * (1 - self.flip) + s * self.flip

    def view(self, dp, ds, a=0, n=None):
        z, y = self.zy(dp, ds)
        n = self.rows if n is None else n
        return self.ref.at[z, y, pl.ds(self.lo + a, n)]

    def copy(self, k, blk, to):
        z, y = self.zy(*to)
        return pltpu.make_async_remote_copy(
            src_ref=blk, dst_ref=blk, send_sem=self.ss if self.total is not None else self.ss.at[self.n], recv_sem=self.rs.at[k],
            device_id={"fs": z * 4 + y, "tp": self.tp}, device_id_type=MESH)

    def send(self, k, blk, to):
        c = self.copy(k, blk, to)
        c.start()
        self.sends.append(c)
        self.n += 1

    def wait(self, k, blk):
        self.copy(k, blk, (1, 0)).wait_recv()

    REL = (0, -1, 1, 2)

    def both(self, i):
        blk = self.view(self.REL[i], 0)
        self.send(4 + i, blk, (0, 1))
        self.send(8 + i, blk, (0, -1))

    def start(self):
        own = self.view(0, 0)
        self.send(0, own, (1, 0))
        self.send(1, own, (-1, 0))
        self.both(0)

    def near(self):
        s = self.split
        self.wait(0, self.view(-1, 0))
        self.send(2, self.view(-1, 0, 0, s), (1, 0))
        self.both(1)
        self.wait(1, self.view(1, 0))
        if s < self.rows:
            self.send(3, self.view(1, 0, s, self.rows - s), (-1, 0))
        self.both(2)

    def far(self):
        s = self.split
        self.wait(2, self.view(2, 0, 0, s))
        if s < self.rows:
            self.wait(3, self.view(2, 0, s, self.rows - s))
        self.both(3)

    def cross(self, i):
        below, above = self.view(self.REL[i], -1), self.view(self.REL[i], 1)
        self.wait(4 + i, below)
        if i < 2:
            self.send(12 + i, below, (0, 1))
        self.wait(8 + i, above)
        if i >= 2:
            self.send(12 + i, above, (0, -1))

    def last(self, i):
        self.wait(12 + i, self.view(self.REL[i], 2))

    def drain(self):
        if self.total is not None:
            self.copy(0, self.total, (1, 0)).wait_send()
        else:
            for c in self.sends:
                c.wait_send()


def kernel(mixed, resid, wm_in, gain, up_in, gate_in, cw_in, cb_in, dw_in, out, last,
           wm, ug, dwn, upt, cw, tok, rr, mx, rs, hal, hu, hid, pbuf, precv, xfwd, base,
           lsem, wx_s, wx_r, g_s, g_r, t_r, td_r, rd_r, p_r, x_r, xw_r, one):
    fs, tp = lax.axis_index("fs"), lax.axis_index("tp")
    z, y, x, c = fs // 4, fs % 4, tp // 2, tp % 2
    xr, xl, xo = (x + 1) % 4, (x + 3) % 4, (x + 2) % 4
    mate = x * 2 + (1 - c)
    drains = []
    (w_sem, v_sem, d_s, d_r, t_s, td_s, rd_s, h_s, h_r, p_s, x_s, xw_s, xd_s, xd_r) = (
        one.at[k] for k in range(14))

    def rcopy(src, dst, ss, rsem, tp_to, fs_to=None):
        return pltpu.make_async_remote_copy(
            src_ref=src, dst_ref=dst, send_sem=ss, recv_sem=rsem,
            device_id={"fs": fs if fs_to is None else fs_to, "tp": tp_to}, device_id_type=MESH)

    ph = Phases()
    ph("load")
    ld_up = pltpu.make_async_copy(up_in, upt.at[0], lsem.at[0])
    ld_gate = pltpu.make_async_copy(gate_in, upt.at[1], lsem.at[4])
    ld_dw = pltpu.make_async_copy(dw_in, dwn.at[z, y, pl.ds(0, 688)], lsem.at[1])
    ld_mx = pltpu.make_async_copy(mixed, mx, lsem.at[2])
    ld_rs = pltpu.make_async_copy(resid, rs, lsem.at[3])
    row16 = pl.multiple_of(tp * 16, 16)
    ld_own = pltpu.make_async_copy(wm_in.at[:, pl.ds(CH, CH)], wm.at[1, z, y, pl.ds(row16, 16)],
                                   lsem.at[7])
    ld_own.start()
    ld_up.start()
    ld_gate.start()
    ld_mx.start()
    ld_rs.start()
    ld_dw.start()

    ph("barrier")
    bar = pltpu.get_barrier_semaphore()
    peers = [(fs, (tp + k) % 8) for k in range(1, 8)]
    peers += [(z * 4 + (y + 1) % 4, tp), (z * 4 + (y + 3) % 4, tp)]
    peers += [(((z + 1) % 4) * 4 + y, tp), (((z + 3) % 4) * 4 + y, tp)]
    for f, t in peers:
        pl.semaphore_signal(bar, inc=1, device_id={"fs": f, "tp": t}, device_id_type=MESH)
    pl.semaphore_wait(bar, len(peers))

    ph("wx")
    half = tp // 4
    slot = tp % 4
    src = wm_in.at[:, pl.ds(0, CH)]
    dst = wm.at[0, z, y, pl.ds(row16, 16)]
    for k in range(1, 4):
        cp = rcopy(src, dst, wx_s.at[k], wx_r.at[slot], ((x + k) % 4) * 2 + half)
        cp.start()
        drains.append(cp)
    stay = pltpu.make_async_copy(src, dst, wx_r.at[slot])
    over = rcopy(src, dst, wx_s.at[0], wx_r.at[slot], mate)

    @pl.when(c == half)
    def _():
        stay.start()

    @pl.when(c != half)
    def _():
        over.start()

    lo = pl.multiple_of(c * 64, 64)
    other = pl.multiple_of(64 - lo, 64)
    gw = Gather(wm.at[0], lo, 64, 32, c, fs, tp, w_sem, g_r.at[0],
                wm.at[0, pl.ds(0, 3), :, pl.ds(0, 80)])
    gv = Gather(wm.at[1], row16, 16, 16, c, fs, tp, v_sem, g_r.at[1],
                wm.at[1, pl.ds(0, 3), 0, pl.ds(0, 80)])
    gu = Gather(ug, 0, 128, 64, c, fs, tp, g_s.at[0], g_r.at[2])
    gd = Gather(dwn, 0, 688, 352, 1 - c, fs, tp, g_s.at[1], g_r.at[3])

    def share(k, dp, ds):
        blk = gw.view(dp, ds)
        cp = rcopy(blk, blk, d_s, d_r, mate)
        cp.start()

    def w_cross(i):
        gw.cross(i)
        share(4 + 2 * i, Gather.REL[i], -1)
        share(5 + 2 * i, Gather.REL[i], 1)

    def w_rows(xsrc, core, z0=0, nz=4):
        return wm.at[1, pl.ds(z0, nz), :, pl.ds(pl.multiple_of((xsrc * 2 + core) * 16, 16), 16)]

    def line_send(to_right, k, xsrc, z0, nz):
        side, blk = 0 if to_right else 1, w_rows(xsrc, c, z0, nz)
        cp = rcopy(blk, blk, xw_s, xw_r.at[side, k], (xr if to_right else xl) * 2 + c)
        cp.start()

    def line_wait(from_left, k, xsrc, z0, nz):
        side, blk = 0 if from_left else 1, w_rows(xsrc, c, z0, nz)
        rcopy(blk, blk, xw_s, xw_r.at[side, k], mate).wait_recv()

    def line_share(xsrc, z0=0, nz=4):
        blk = w_rows(xsrc, c, z0, nz)
        cp = rcopy(blk, blk, xd_s, xd_r, mate)
        cp.start()

    ph("v_start")
    ld_own.wait()
    gv.start()
    gv.near()
    ph("w_start")
    for k in range(4):
        row = pl.multiple_of(lo + k * 16, 16)
        blk = wm.at[0, z, y, pl.ds(row, 16)]
        rcopy(blk, blk, wx_s.at[0], wx_r.at[k], mate).wait_recv()
    gw.start()
    share(0, 0, 0)
    ph("v_far")
    gv.cross(0)
    gv.far()

    ph("prep")
    zero_rows = jnp.zeros((HID - 688, 128), BF16)

    @pl.loop(0, 16)
    def _(f):
        dwn[f // 4, f % 4, pl.ds(688, HID - 688)] = zero_rows

    cw[...] = jnp.zeros((8, HID), F32)
    cw[0:3, 0:688] = cw_in[...]
    cw[3:4, 0:688] = cb_in[...].reshape(1, 688)
    ld_up.wait()
    ld_gate.wait()
    gn = gain[:, pl.ds(pl.multiple_of(fs * 128, 128), 128)]
    for i in range(5):
        for k in range(2):
            t = upt[k, pl.ds(i * 128, 128), :].astype(F32) * gn
            ug[z, y, :, pl.ds(i * 256 + k * 128, 128)] = t.T.astype(BF16)
    gap = jnp.zeros((16, 128), F32)
    t = [upt[0, pl.ds(640, 48), :].astype(F32) * gn, gap,
         upt[1, pl.ds(640, 48), :].astype(F32) * gn, gap]
    ug[z, y, :, pl.ds(1280, 128)] = jnp.concatenate(t, axis=0).T.astype(BF16)

    def mix(ch, n):
        w = wm[ch, :, :, :, n * 512:(n + 1) * 512].reshape(D, 512)
        s = jnp.dot(mx[...], w, preferred_element_type=F32)
        at = ch * CH + n * 512
        s = rs[:, at:at + 512].astype(F32) + s
        tok[x, c, ch, :, n * 512:(n + 1) * 512] = s.astype(BF16)

    def send_tok(xsrc, h, ch, to_right, sidx):
        blk = tok.at[xsrc, c, ch, pl.ds(h * HALF, HALF)]
        side = 0 if to_right else 1
        cp = rcopy(blk, blk, t_s, t_r.at[side, sidx],
                   (xr if to_right else xl) * 2 + c)
        cp.start()

    def tok_wait(from_left, idx, xsrc, h, ch):
        blk = tok.at[xsrc, c, ch, pl.ds(h * HALF, HALF)]
        side = 0 if from_left else 1
        rcopy(blk, blk, t_s, t_r.at[side, idx], mate).wait_recv()

    def factor(xsrc, h):
        acc = None
        for ch in range(2):
            for k in range(CH // 128):
                v = tok[xsrc, c, ch, h * HALF:(h + 1) * HALF, k * 128:(k + 1) * 128].astype(F32)
                acc = v * v if acc is None else acc + v * v
        m = jnp.sum(acc, axis=-1, keepdims=True) * (1.0 / D)
        rr[xsrc, c, h] = jnp.broadcast_to(lax.rsqrt(m + NORM_EPS), (HALF, 128))

    def pass_on(k, xsrc, h, ch):
        blk = tok.at[xsrc, c, ch, pl.ds(h * HALF, HALF)]
        cp = rcopy(blk, blk, td_s, td_r.at[k], mate)
        cp.start()

    def pass_factor(k, xsrc, h):
        factor(xsrc, h)
        blk = rr.at[xsrc, c, h]
        cp = rcopy(blk, blk, rd_s, rd_r.at[k], mate)
        cp.start()

    def mate_wait(k, xsrc, h):
        blk = tok.at[xsrc, 1 - c, :, pl.ds(h * HALF, HALF)]
        rcopy(blk, blk, td_s, td_r.at[k], mate).wait_recv()
        blk = rr.at[xsrc, 1 - c, h]
        rcopy(blk, blk, rd_s, rd_r.at[k], mate).wait_recv()

    ph("w_near")
    gw.near()
    share(1, -1, 0)
    share(2, 1, 0)
    ph("v_c12")
    gv.cross(1)
    gv.cross(2)
    ph("w_c0")
    w_cross(0)
    ph("v_last")
    gv.cross(3)
    for i in range(4):
        gv.last(i)
    line_send(True, 0, x, 0, 2)
    line_send(False, 0, x, 2, 2)
    line_send(True, 2, x, 2, 2)
    line_send(False, 2, x, 0, 2)
    line_share(x)
    ph("w_far")
    gw.far()
    share(3, 2, 0)
    ph("w_c1")
    w_cross(1)
    ph("w_c2")
    w_cross(2)
    ph("w_c3")
    w_cross(3)
    gu.start()
    ph("w_last")
    for i in range(4):
        gw.last(i)
        share(12 + i, Gather.REL[i], 2)
    ph("line_fwd")
    line_wait(True, 0, xl, 0, 2)
    line_send(True, 1, xl, 0, 2)
    line_share(xl, 0, 2)
    line_wait(False, 0, xr, 2, 2)
    line_send(False, 1, xr, 2, 2)
    line_share(xr, 2, 2)
    ph("w_shared")
    blk = wm.at[0, :, :, pl.ds(other, 64)]
    rcopy(blk, blk, d_s, d_r, mate).wait_recv()
    ld_mx.wait()
    ld_rs.wait()
    ph("mix0")
    mix(0, 0)
    mix(0, 1)
    send_tok(x, 0, 0, True, 0)
    send_tok(x, 1, 0, False, 0)
    pass_on(0, x, 0, 0)
    pass_on(1, x, 1, 0)
    ph("gu_near")
    gu.near()
    ph("line_far")
    line_wait(True, 2, xl, 2, 2)
    line_share(xl, 2, 2)
    line_wait(False, 2, xr, 0, 2)
    line_share(xr, 0, 2)
    line_wait(True, 1, xo, 0, 2)
    line_wait(False, 1, xo, 2, 2)
    line_share(xo)
    blk = wm.at[1, :, :, pl.ds(0, 64)]
    rcopy(blk, blk, xd_s, xd_r, mate).wait_recv()
    ph("mix1")
    mix(1, 0)
    mix(1, 1)
    send_tok(x, 0, 1, True, 1)
    send_tok(x, 1, 1, False, 1)
    pass_on(0, x, 0, 1)
    pass_on(1, x, 1, 1)
    ph("gu_c0")
    gu.cross(0)
    ph("own_mate")
    pass_factor(0, x, 0)
    pass_factor(1, x, 1)

    tails = []
    for h in range(2):
        f = rr[x, c, h, HALF - 8:HALF, :][:, 0:1]
        for r in (6, 7):
            for q in range(8):
                ch, col = q // 4, (q % 4) * 256
                v = tok[x, c, ch, (h + 1) * HALF - 16:(h + 1) * HALF, col:col + 256].astype(F32)
                tails.append(v[r + 8:r + 9] * f[r:r + 1])
    hal[tp] = jnp.concatenate(tails, axis=0).astype(BF16)
    for k in range(1, 8):
        rcopy(hal.at[tp], hal.at[tp], h_s, h_r, (tp + k) % 8).start()

    ph("gu_far")
    gu.far()
    ph("tokA0")
    tok_wait(True, 0, xl, 0, 0)
    send_tok(xl, 0, 0, True, 2)
    pass_on(2, xl, 0, 0)
    tok_wait(False, 0, xr, 1, 0)
    send_tok(xr, 1, 0, False, 2)
    pass_on(3, xr, 1, 0)
    ph("gu_c1")
    gu.cross(1)
    ph("gu_c2")
    gu.cross(2)
    ph("gu_c3")
    gu.cross(3)
    ld_dw.wait()
    gd.start()
    ph("tokA1")
    tok_wait(True, 1, xl, 0, 1)
    send_tok(xl, 0, 1, True, 3)
    send_tok(x, 1, 0, True, 4)
    send_tok(x, 1, 1, True, 5)
    pass_on(2, xl, 0, 1)
    tok_wait(False, 1, xr, 1, 1)
    send_tok(xr, 1, 1, False, 3)
    send_tok(x, 0, 0, False, 4)
    send_tok(x, 0, 1, False, 5)
    pass_on(3, xr, 1, 1)
    pass_factor(2, xl, 0)
    pass_factor(3, xr, 1)
    ph("gu_last")
    for i in range(4):
        gu.last(i)
    ph("gd_near")
    gd.near()

    ph("xexp")
    blk = hal.at[pl.ds(0, 7)]
    rcopy(blk, blk, h_s, h_r, mate).wait_recv()
    hv = hal[...].reshape(256, 256).astype(F32)
    rid = lax.broadcasted_iota(jnp.int32, (256, 256), 0) % 8
    for q in range(8):
        mx[0:256, q * 256:(q + 1) * 256] = jnp.where(rid == q, hv, 0.0).astype(BF16)

    ph("gd_c0")
    gd.cross(0)
    ph("hu")

    @pl.loop(0, 6)
    def _(i):
        w = ug[:, :, :, pl.ds(pl.multiple_of(i * 256, 256), 128)].reshape(D, 128)
        r = jnp.dot(mx[0:256, :], w, preferred_element_type=F32)
        r = jnp.sum(r.reshape(32, 8, 128), axis=1)
        cols = pl.ds(pl.multiple_of(i * 128, 128), 128)
        hu[0, 0:2, cols] = jnp.zeros((2, 128), F32)
        for q in range(15):
            hu[q + 1, 0:2, cols] = r[2 * q:2 * q + 2]

    row8 = lax.broadcasted_iota(jnp.int32, (8, 128), 0)

    def hidden(xs, hs, cc, to):
        unit = [(xs[k] * 2 + cc) * 2 + hs[k] for k in range(2)]
        a = [[tok[xs[k], cc, ch, hs[k] * HALF:(hs[k] + 1) * HALF, :] for ch in range(2)]
             for k in range(2)]
        a = jnp.concatenate([jnp.concatenate(v, axis=1) for v in a], axis=0)

        def act(i, u, g):
            cols = pl.ds(i * 128, 128)
            taps = [cw[k:k + 1, cols] for k in range(4)]
            for k in range(2):
                f = rr[xs[k], cc, hs[k]]
                uk, gk = u[k * HALF:(k + 1) * HALF] * f, g[k * HALF:(k + 1) * HALF] * f
                before = hu[unit[k], :, cols]
                h0, h1 = before[0:1], before[1:2]
                u1, u2 = pltpu.roll(uk, 1, 0), pltpu.roll(uk, 2, 0)
                f1 = jnp.where(row8 == 0, h1, u1[:8])
                f2 = jnp.where(row8 == 0, h0, jnp.where(row8 == 1, h1, u2[:8]))
                u1 = jnp.concatenate([f1, u1[8:]], axis=0)
                u2 = jnp.concatenate([f2, u2[8:]], axis=0)
                s = taps[3] + taps[0] * u2 + taps[1] * u1 + taps[2] * uk
                hid[to, pl.ds(k * HALF, HALF), cols] = gated_gelu(s, gk).astype(BF16)

        for i, width in ((0, 512), (2, 512), (4, 384)):
            w = ug[:, :, :, pl.ds(i * 256, width)].reshape(D, width)
            r = jnp.dot(a, w, preferred_element_type=F32)
            act(i, r[:, :128], r[:, 128:256])
            if width == 512:
                act(i + 1, r[:, 256:384], r[:, 384:])
            else:
                act(i + 1, r[:, 256:384], pltpu.roll(r[:, 256:384], 64, 1))

    def down(frm, xs, hs, cls):
        @pl.loop(0, 4)
        def _(n):
            w = jnp.concatenate([dwn[n, k] for k in range(4)], axis=1)
            r = jnp.dot(hid[frm], w, preferred_element_type=F32).astype(BF16)
            cols = pl.ds(pl.multiple_of(n * 512, 512), 512)
            for k in range(2):
                pbuf[cls, xs[k], hs[k], :, cols] = r[k * HALF:(k + 1) * HALF]

        @pl.when(cls == 0)
        def _():
            for k in range(2):
                rcopy(pbuf.at[0, xs[k], hs[k]], precv.at[xs[k], hs[k]], p_s,
                      p_r.at[xs[k], hs[k]], mate).start()

    def core_of(cls):
        return (1 - c) * (1 - cls) + c * cls

    def group(xs, hs, slot=None, up=True, dn=True):
        @pl.loop(0, 2)
        def _(cls):
            to = cls if slot is None else slot + cls
            if up:
                hidden(xs, hs, core_of(cls), to)
            if dn:
                down(to, xs, hs, cls)

    def joined(xx, h, extra=None):
        rcopy(pbuf.at[0, xx, h], precv.at[xx, h], p_s, p_r.at[xx, h], mate).wait_recv()

        @pl.loop(0, HALF // 16)
        def _(r):
            rr = pl.ds(pl.multiple_of(r * 16, 16), 16)
            v = pbuf[1, xx, h, rr, :].astype(F32) + precv[xx, h, rr, :].astype(F32)
            if extra is not None:
                v = v + extra[rr, :].astype(F32)
            pbuf[1, xx, h, rr, :] = v.astype(BF16)

    def send_sum(xx, h, to_right, dst, k):
        side = 0 if to_right else 1
        cp = rcopy(pbuf.at[1, xx, h], dst, x_s, x_r.at[side, k],
                   (xr if to_right else xl) * 2 + c)
        cp.start()

    def wait_sum(from_left, dst, k):
        side = 0 if from_left else 1
        rcopy(dst, dst, x_s, x_r.at[side, k], mate).wait_recv()

    ph("gd_far")
    gd.far()
    ph("gd_c123")
    gd.cross(1)
    gd.cross(2)
    gd.cross(3)

    ph("tok_opp")
    tok_wait(True, 2, xo, 0, 0)
    pass_on(4, xo, 0, 0)
    tok_wait(False, 2, xo, 1, 0)
    pass_on(5, xo, 1, 0)
    tok_wait(True, 3, xo, 0, 1)
    pass_on(4, xo, 0, 1)
    pass_factor(4, xo, 0)
    tok_wait(False, 3, xo, 1, 1)
    pass_on(5, xo, 1, 1)
    pass_factor(5, xo, 1)
    ph("h_opp1")
    hidden((xo, xo), (0, 1), core_of(1), 1)
    ph("mate_opp")
    mate_wait(4, xo, 0)
    mate_wait(5, xo, 1)
    ph("h_opp0")
    hidden((xo, xo), (0, 1), core_of(0), 0)
    ph("gd_last")
    for i in range(4):
        gd.last(i)

    ph("d_opp")
    group((xo, xo), (0, 1), 0, up=False)
    ph("j_opp")
    joined(xo, 0)
    send_sum(xo, 0, True, xfwd.at[0], 0)
    joined(xo, 1)
    send_sum(xo, 1, False, xfwd.at[1], 0)
    ph("mate_near1")
    mate_wait(2, xl, 0)
    mate_wait(3, xr, 1)
    ph("g_near1")
    group((xr, xl), (1, 0))
    ph("j_near1")
    joined(xr, 1)
    send_sum(xr, 1, True, rs.at[pl.ds(HALF, HALF)], 1)
    joined(xl, 0)
    send_sum(xl, 0, False, rs.at[pl.ds(0, HALF)], 1)

    ph("tok_near2")
    tok_wait(True, 4, xl, 1, 0)
    pass_on(6, xl, 1, 0)
    tok_wait(False, 4, xr, 0, 0)
    pass_on(7, xr, 0, 0)
    tok_wait(True, 5, xl, 1, 1)
    pass_on(6, xl, 1, 1)
    pass_factor(6, xl, 1)
    tok_wait(False, 5, xr, 0, 1)
    pass_on(7, xr, 0, 1)
    pass_factor(7, xr, 0)
    mate_wait(6, xl, 1)
    mate_wait(7, xr, 0)
    ph("g_near2")
    group((xr, xl), (0, 1))
    ph("j_near2")
    wait_sum(True, xfwd.at[0], 0)
    joined(xr, 0, xfwd.at[0])
    send_sum(xr, 0, True, last.at[pl.ds(0, HALF)], 2)
    ph("j_near2b")
    wait_sum(False, xfwd.at[1], 0)
    joined(xl, 1, xfwd.at[1])
    send_sum(xl, 1, False, last.at[pl.ds(HALF, HALF)], 2)

    ph("mate_own")
    mate_wait(0, x, 0)
    mate_wait(1, x, 1)
    ph("g_own")
    group((x, x), (0, 1))
    ph("base")
    outs = []
    for h in range(2):
        rcopy(pbuf.at[0, x, h], precv.at[x, h], p_s, p_r.at[x, h], mate).wait_recv()

        @pl.loop(0, HALF // 16)
        def _(r):
            row = pl.ds(pl.multiple_of(r * 16, 16), 16)
            at = pl.ds(pl.multiple_of(h * HALF + r * 16, 16), 16)
            for ch in range(2):
                cols = pl.ds(ch * CH, CH)
                v = tok[x, c, ch, at, :].astype(F32) + pbuf[1, x, h, row, cols].astype(F32)
                base[at, cols] = v + precv[x, h, row, cols].astype(F32)

    ph("fin_w1")
    wait_sum(True, rs.at[pl.ds(HALF, HALF)], 1)
    wait_sum(False, rs.at[pl.ds(0, HALF)], 1)
    for h in range(2):
        @pl.loop(h * 12, h * 12 + 12)
        def _(r):
            at = pl.ds(pl.multiple_of(r * 16, 16), 16)
            base[at, :] = base[at, :] + rs[at, :].astype(F32)

        cp = pltpu.make_async_copy(base.at[pl.ds(h * HALF, HALF)], out.at[pl.ds(h * HALF, HALF)],
                                   lsem.at[5 + h])
        cp.start()
        outs.append(cp)
    for cp in outs:
        cp.wait()

    ph("fin_w2")
    wait_sum(True, last.at[pl.ds(0, HALF)], 2)
    wait_sum(False, last.at[pl.ds(HALF, HALF)], 2)

    ph("drain")
    @pl.when(c != half)
    def _():
        over.wait_send()

    for cp in drains:
        cp.wait_send()
    gw.drain()
    gv.drain()
    gu.drain()
    gd.drain()
    for sem, view in (
            (d_s, wm.at[0, :, :, pl.ds(0, 64)]),
            (xw_s, wm.at[1, :, :, pl.ds(0, 48)]),
            (xd_s, wm.at[1, :, :, pl.ds(0, 64)]),
            (t_s, tok.at[pl.ds(0, 3), 0]),
            (td_s, tok.at[:, 0]),
            (rd_s, rr.at[:, 0]),
            (h_s, hal.at[pl.ds(0, 7)]),
            (p_s, pbuf.at[0]),
            (x_s, precv.at[pl.ds(0, 3)])):
        rcopy(view, view, sem, lsem.at[0], mate).wait_send()
    ph("")


def body(mixed, residual, mix_weight, norm_gain, up_weight, gate_weight, conv_weight, conv_bias,
         down_weight):
    any_ = pl.BlockSpec(memory_space=pl.ANY)
    vm = pl.BlockSpec(memory_space=pltpu.VMEM)
    dma = pltpu.SemaphoreType.DMA
    part, last = pl.pallas_call(
        kernel,
        out_shape=(jax.ShapeDtypeStruct((TOK, D), F32),
                   jax.ShapeDtypeStruct((TOK, D), BF16)),
        in_specs=[any_, any_, any_, vm, any_, any_, vm, vm, any_],
        out_specs=(any_, any_),
        scratch_shapes=[
            pltpu.VMEM((2, 4, 4, 128, CH), BF16),
            pltpu.VMEM((4, 4, 128, UG), BF16),
            pltpu.VMEM((4, 4, HID, 128), BF16),
            pltpu.VMEM((2, 688, 128), BF16),
            pltpu.VMEM((8, HID), F32),
            pltpu.VMEM((4, 2, 2, TOK, CH), BF16),
            pltpu.VMEM((4, 2, 2, HALF, 128), F32),
            pltpu.VMEM((TOK, D), BF16),
            pltpu.VMEM((TOK, D), BF16),
            pltpu.VMEM((8, 32, 256), BF16),
            pltpu.VMEM((16, 8, HID), F32),
            pltpu.VMEM((2, TOK, HID), BF16),
            pltpu.VMEM((2, 4, 2, HALF, D), BF16),
            pltpu.VMEM((4, 2, HALF, D), BF16),
            pltpu.VMEM((2, HALF, D), BF16),
            pltpu.VMEM((TOK, D), F32),
            dma((8,)), dma((4,)), dma((4,)),
            dma((2, 16)), dma((4, 16)),
            dma((2, 6)), dma((8,)), dma((8,)),
            dma((4, 2)), dma((2, 3)), dma((2, 3)),
            dma((14,)),
        ],
        compiler_params=pltpu.CompilerParams(
            collective_id=0, has_side_effects=True, vmem_limit_bytes=67_043_328),
    )(mixed, residual, mix_weight, norm_gain[None], up_weight.T, gate_weight.T, conv_weight, conv_bias,
      down_weight)
    return (part + last.astype(F32)).astype(BF16)


def solution(mesh):
    rows = P(("fs", "tp"), None)
    in_specs = (rows, rows, rows, P(), P("fs", "tp"), P("fs", "tp"), P(None, "tp"), P("tp"),
                P("tp", "fs"))
    return jax.shard_map(body, mesh=mesh, in_specs=in_specs, out_specs=rows, check_vma=False)
```

```python
import functools

import jax
import jax.numpy as jnp
from jax import lax
from jax.experimental import pallas as pl
from jax.experimental.pallas import tpu as pltpu
from jax.sharding import PartitionSpec as P

MESH = pl.DeviceIdType.MESH
F32 = jnp.float32
BF16 = jnp.bfloat16
NORM_EPS = 1e-06
GELU_C = 0.7978845608028654

D = 2048
TOK = 384
CH = 1024
HALF = 192
UG = 1408
HID = 768


def gated_gelu(v, gate):
    t = jnp.tanh(v * (GELU_C + (GELU_C * 0.044715) * (v * v)))
    v = 0.5 * v
    return (v + v * t) * gate


class Phases:
    def __init__(self):
        self.scope = None

    def __call__(self, name):
        if self.scope is not None:
            self.scope.__exit__(None, None, None)
        self.scope = jax.named_scope(name) if name else None
        if name:
            self.scope.__enter__()


class Gather:
    def __init__(self, ref, lo, rows, split, flip, fs, tp, send_sem, recv_sem, total=None,
                 direct=False):
        self.direct = direct
        self.total = total
        self.ref, self.lo, self.rows, self.split, self.flip = ref, lo, rows, split, flip
        self.tp, self.ss, self.rs = tp, send_sem, recv_sem
        z, y = fs // 4, fs % 4
        self.p = y * (1 - flip) + z * flip
        self.s = z * (1 - flip) + y * flip
        self.n = 0
        self.sends = []

    def zy(self, dp, ds):
        p, s = (self.p + dp + 4) % 4, (self.s + ds + 4) % 4
        return s * (1 - self.flip) + p * self.flip, p * (1 - self.flip) + s * self.flip

    def view(self, dp, ds, a=0, n=None):
        z, y = self.zy(dp, ds)
        n = self.rows if n is None else n
        return self.ref.at[z, y, pl.ds(self.lo + a, n)]

    def copy(self, k, blk, to):
        z, y = self.zy(*to)
        return pltpu.make_async_remote_copy(
            src_ref=blk, dst_ref=blk, send_sem=self.ss if self.total is not None else self.ss.at[self.n], recv_sem=self.rs.at[k],
            device_id={"fs": z * 4 + y, "tp": self.tp}, device_id_type=MESH)

    def send(self, k, blk, to):
        c = self.copy(k, blk, to)
        c.start()
        self.sends.append(c)
        self.n += 1

    def wait(self, k, blk):
        self.copy(k, blk, (1, 0)).wait_recv()

    REL = (0, -1, 1, 2)

    def both(self, i):
        blk = self.view(self.REL[i], 0)
        self.send(4 + i, blk, (0, 1))
        self.send(8 + i, blk, (0, -1))
        if self.direct:
            self.send(12 + i, blk, (0, 2))

    def start(self):
        own = self.view(0, 0)
        self.send(0, own, (1, 0))
        self.send(1, own, (-1, 0))
        if self.direct:
            self.send(2, own, (2, 0))
        self.both(0)

    def near(self):
        s = self.split
        self.wait(0, self.view(-1, 0))
        if not self.direct:
            self.send(2, self.view(-1, 0, 0, s), (1, 0))
        self.both(1)
        self.wait(1, self.view(1, 0))
        if s < self.rows:
            self.send(3, self.view(1, 0, s, self.rows - s), (-1, 0))
        self.both(2)

    def far(self):
        s = self.split
        self.wait(2, self.view(2, 0, 0, s))
        if s < self.rows:
            self.wait(3, self.view(2, 0, s, self.rows - s))
        self.both(3)

    def cross(self, i):
        below, above = self.view(self.REL[i], -1), self.view(self.REL[i], 1)
        self.wait(4 + i, below)
        if i < 2 and not self.direct:
            self.send(12 + i, below, (0, 1))
        self.wait(8 + i, above)
        if i >= 2 and not self.direct:
            self.send(12 + i, above, (0, -1))

    def last(self, i):
        self.wait(12 + i, self.view(self.REL[i], 2))

    def drain(self):
        if self.total is not None:
            self.copy(0, self.total, (1, 0)).wait_send()
        else:
            for c in self.sends:
                c.wait_send()


def kernel(mixed, resid, wm_in, gain, up_in, gate_in, cw_in, cb_in, dw_in, out, last,
           wm, ug, dwn, upt, cw, tok, rr, mx, rs, hal, hu, hid, pbuf, precv, xfwd, base,
           lsem, wx_s, wx_r, g_s, g_r, t_r, td_r, rd_r, p_r, x_r, xw_r, one):
    fs, tp = lax.axis_index("fs"), lax.axis_index("tp")
    z, y, x, c = fs // 4, fs % 4, tp // 2, tp % 2
    xr, xl, xo = (x + 1) % 4, (x + 3) % 4, (x + 2) % 4
    mate = x * 2 + (1 - c)
    drains = []
    (w_sem, v_sem, d_s, d_r, t_s, td_s, rd_s, h_s, h_r, p_s, x_s, xw_s, xd_s, xd_r) = (
        one.at[k] for k in range(14))

    def rcopy(src, dst, ss, rsem, tp_to, fs_to=None):
        return pltpu.make_async_remote_copy(
            src_ref=src, dst_ref=dst, send_sem=ss, recv_sem=rsem,
            device_id={"fs": fs if fs_to is None else fs_to, "tp": tp_to}, device_id_type=MESH)

    ph = Phases()
    ph("load")
    ld_up = pltpu.make_async_copy(up_in, upt.at[0], lsem.at[0])
    ld_gate = pltpu.make_async_copy(gate_in, upt.at[1], lsem.at[4])
    ld_dw = pltpu.make_async_copy(dw_in, dwn.at[z, y, pl.ds(0, 688)], lsem.at[1])
    ld_mx = pltpu.make_async_copy(mixed, mx, lsem.at[2])
    ld_rs = pltpu.make_async_copy(resid, rs, lsem.at[3])
    row16 = pl.multiple_of(tp * 16, 16)
    ld_own = pltpu.make_async_copy(wm_in.at[:, pl.ds(CH, CH)], wm.at[1, z, y, pl.ds(row16, 16)],
                                   lsem.at[7])
    ld_own.start()
    ld_up.start()
    ld_gate.start()
    ld_mx.start()
    ld_rs.start()
    ld_dw.start()

    ph("barrier")
    bar = pltpu.get_barrier_semaphore()
    peers = [(fs, (tp + k) % 8) for k in range(1, 8)]
    peers += [(z * 4 + (y + 1) % 4, tp), (z * 4 + (y + 3) % 4, tp)]
    peers += [(((z + 1) % 4) * 4 + y, tp), (((z + 3) % 4) * 4 + y, tp)]
    peers += [(z * 4 + (y + 2) % 4, tp), (((z + 2) % 4) * 4 + y, tp)]
    for f, t in peers:
        pl.semaphore_signal(bar, inc=1, device_id={"fs": f, "tp": t}, device_id_type=MESH)
    pl.semaphore_wait(bar, len(peers))

    ph("wx")
    half = tp // 4
    slot = tp % 4
    src = wm_in.at[:, pl.ds(0, CH)]
    dst = wm.at[0, z, y, pl.ds(row16, 16)]
    for k in range(1, 4):
        cp = rcopy(src, dst, wx_s.at[k], wx_r.at[slot], ((x + k) % 4) * 2 + half)
        cp.start()
        drains.append(cp)
    stay = pltpu.make_async_copy(src, dst, wx_r.at[slot])
    over = rcopy(src, dst, wx_s.at[0], wx_r.at[slot], mate)

    @pl.when(c == half)
    def _():
        stay.start()

    @pl.when(c != half)
    def _():
        over.start()

    lo = pl.multiple_of(c * 64, 64)
    other = pl.multiple_of(64 - lo, 64)
    gw = Gather(wm.at[0], lo, 64, 32, c, fs, tp, w_sem, g_r.at[0],
                wm.at[0, pl.ds(0, 3), :, pl.ds(0, 80)])
    gv = Gather(wm.at[1], row16, 16, 16, c, fs, tp, v_sem, g_r.at[1],
                wm.at[1, pl.ds(0, 3), 0, pl.ds(0, 80)], True)
    gu = Gather(ug, 0, 128, 64, c, fs, tp, g_s.at[0], g_r.at[2])
    gd = Gather(dwn, 0, 688, 352, 1 - c, fs, tp, g_s.at[1], g_r.at[3])

    def share(k, dp, ds):
        blk = gw.view(dp, ds)
        cp = rcopy(blk, blk, d_s, d_r, mate)
        cp.start()

    def w_cross(i):
        gw.cross(i)
        share(4 + 2 * i, Gather.REL[i], -1)
        share(5 + 2 * i, Gather.REL[i], 1)

    def w_rows(xsrc, core, z0=0, nz=4):
        return wm.at[1, pl.ds(z0, nz), :, pl.ds(pl.multiple_of((xsrc * 2 + core) * 16, 16), 16)]

    def line_send(to_right, k, xsrc, z0, nz):
        side, blk = 0 if to_right else 1, w_rows(xsrc, c, z0, nz)
        cp = rcopy(blk, blk, xw_s, xw_r.at[side, k], (xr if to_right else xl) * 2 + c)
        cp.start()

    def line_wait(from_left, k, xsrc, z0, nz):
        side, blk = 0 if from_left else 1, w_rows(xsrc, c, z0, nz)
        rcopy(blk, blk, xw_s, xw_r.at[side, k], mate).wait_recv()

    def line_share(xsrc, z0=0, nz=4):
        blk = w_rows(xsrc, c, z0, nz)
        cp = rcopy(blk, blk, xd_s, xd_r, mate)
        cp.start()

    ph("v_start")
    ld_own.wait()
    gv.start()
    gv.near()
    gv.far()
    ph("w_start")
    for k in range(4):
        row = pl.multiple_of(lo + k * 16, 16)
        blk = wm.at[0, z, y, pl.ds(row, 16)]
        rcopy(blk, blk, wx_s.at[0], wx_r.at[k], mate).wait_recv()
    gw.start()
    share(0, 0, 0)
    ph("prep")
    zero_rows = jnp.zeros((HID - 688, 128), BF16)

    @pl.loop(0, 16)
    def _(f):
        dwn[f // 4, f % 4, pl.ds(688, HID - 688)] = zero_rows

    cw[...] = jnp.zeros((8, HID), F32)
    cw[0:3, 0:688] = cw_in[...]
    cw[3:4, 0:688] = cb_in[...].reshape(1, 688)
    ld_up.wait()
    ld_gate.wait()
    gn = gain[:, pl.ds(pl.multiple_of(fs * 128, 128), 128)]
    for i in range(5):
        for k in range(2):
            t = upt[k, pl.ds(i * 128, 128), :].astype(F32) * gn
            ug[z, y, :, pl.ds(i * 256 + k * 128, 128)] = t.T.astype(BF16)
    gap = jnp.zeros((16, 128), F32)
    t = [upt[0, pl.ds(640, 48), :].astype(F32) * gn, gap,
         upt[1, pl.ds(640, 48), :].astype(F32) * gn, gap]
    ug[z, y, :, pl.ds(1280, 128)] = jnp.concatenate(t, axis=0).T.astype(BF16)

    def mix(ch, n):
        w = wm[ch, :, :, :, n * 512:(n + 1) * 512].reshape(D, 512)
        s = jnp.dot(mx[...], w, preferred_element_type=F32)
        at = ch * CH + n * 512
        s = rs[:, at:at + 512].astype(F32) + s
        tok[x, c, ch, :, n * 512:(n + 1) * 512] = s.astype(BF16)

    def send_tok(xsrc, h, ch, to_right, sidx):
        blk = tok.at[xsrc, c, ch, pl.ds(h * HALF, HALF)]
        side = 0 if to_right else 1
        cp = rcopy(blk, blk, t_s, t_r.at[side, sidx],
                   (xr if to_right else xl) * 2 + c)
        cp.start()

    def tok_wait(from_left, idx, xsrc, h, ch):
        blk = tok.at[xsrc, c, ch, pl.ds(h * HALF, HALF)]
        side = 0 if from_left else 1
        rcopy(blk, blk, t_s, t_r.at[side, idx], mate).wait_recv()

    def factor(xsrc, h):
        acc = None
        for ch in range(2):
            for k in range(CH // 128):
                v = tok[xsrc, c, ch, h * HALF:(h + 1) * HALF, k * 128:(k + 1) * 128].astype(F32)
                acc = v * v if acc is None else acc + v * v
        m = jnp.sum(acc, axis=-1, keepdims=True) * (1.0 / D)
        rr[xsrc, c, h] = jnp.broadcast_to(lax.rsqrt(m + NORM_EPS), (HALF, 128))

    def pass_on(k, xsrc, h, ch):
        blk = tok.at[xsrc, c, ch, pl.ds(h * HALF, HALF)]
        cp = rcopy(blk, blk, td_s, td_r.at[k], mate)
        cp.start()

    def pass_factor(k, xsrc, h):
        factor(xsrc, h)
        blk = rr.at[xsrc, c, h]
        cp = rcopy(blk, blk, rd_s, rd_r.at[k], mate)
        cp.start()

    def mate_wait(k, xsrc, h):
        blk = tok.at[xsrc, 1 - c, :, pl.ds(h * HALF, HALF)]
        rcopy(blk, blk, td_s, td_r.at[k], mate).wait_recv()
        blk = rr.at[xsrc, 1 - c, h]
        rcopy(blk, blk, rd_s, rd_r.at[k], mate).wait_recv()

    ph("w_near")
    gw.near()
    share(1, -1, 0)
    share(2, 1, 0)
    ph("w_c0")
    w_cross(0)
    ph("v_last")
    for i in range(4):
        gv.cross(i)
        gv.last(i)
    line_send(True, 0, x, 0, 2)
    line_send(False, 0, x, 2, 2)
    line_send(True, 2, x, 2, 2)
    line_send(False, 2, x, 0, 2)
    line_share(x)
    ph("w_far")
    gw.far()
    share(3, 2, 0)
    ph("w_c1")
    w_cross(1)
    ph("w_c2")
    w_cross(2)
    ph("w_c3")
    w_cross(3)
    gu.start()
    ph("w_last")
    for i in range(4):
        gw.last(i)
        share(12 + i, Gather.REL[i], 2)
    ph("line_fwd")
    line_wait(True, 0, xl, 0, 2)
    line_send(True, 1, xl, 0, 2)
    line_share(xl, 0, 2)
    line_wait(False, 0, xr, 2, 2)
    line_send(False, 1, xr, 2, 2)
    line_share(xr, 2, 2)
    ph("w_shared")
    blk = wm.at[0, :, :, pl.ds(other, 64)]
    rcopy(blk, blk, d_s, d_r, mate).wait_recv()
    ld_mx.wait()
    ld_rs.wait()
    ph("mix0")
    mix(0, 0)
    mix(0, 1)
    send_tok(x, 0, 0, True, 0)
    send_tok(x, 1, 0, False, 0)
    pass_on(0, x, 0, 0)
    pass_on(1, x, 1, 0)
    ph("gu_near")
    gu.near()
    ph("line_far")
    line_wait(True, 2, xl, 2, 2)
    line_share(xl, 2, 2)
    line_wait(False, 2, xr, 0, 2)
    line_share(xr, 0, 2)
    line_wait(True, 1, xo, 0, 2)
    line_wait(False, 1, xo, 2, 2)
    line_share(xo)
    blk = wm.at[1, :, :, pl.ds(0, 64)]
    rcopy(blk, blk, xd_s, xd_r, mate).wait_recv()
    ph("mix1")
    mix(1, 0)
    mix(1, 1)
    send_tok(x, 0, 1, True, 1)
    send_tok(x, 1, 1, False, 1)
    pass_on(0, x, 0, 1)
    pass_on(1, x, 1, 1)
    ph("gu_c0")
    gu.cross(0)
    ph("own_mate")
    pass_factor(0, x, 0)
    pass_factor(1, x, 1)

    tails = []
    for h in range(2):
        f = rr[x, c, h, HALF - 8:HALF, :][:, 0:1]
        for r in (6, 7):
            for q in range(8):
                ch, col = q // 4, (q % 4) * 256
                v = tok[x, c, ch, (h + 1) * HALF - 16:(h + 1) * HALF, col:col + 256].astype(F32)
                tails.append(v[r + 8:r + 9] * f[r:r + 1])
    hal[tp] = jnp.concatenate(tails, axis=0).astype(BF16)
    for k in range(1, 8):
        rcopy(hal.at[tp], hal.at[tp], h_s, h_r, (tp + k) % 8).start()

    ph("gu_far")
    gu.far()
    ph("tokA0")
    tok_wait(True, 0, xl, 0, 0)
    send_tok(xl, 0, 0, True, 2)
    pass_on(2, xl, 0, 0)
    tok_wait(False, 0, xr, 1, 0)
    send_tok(xr, 1, 0, False, 2)
    pass_on(3, xr, 1, 0)
    ph("gu_c1")
    gu.cross(1)
    ph("gu_c2")
    gu.cross(2)
    ph("gu_c3")
    gu.cross(3)
    ld_dw.wait()
    gd.start()
    ph("tokA1")
    tok_wait(True, 1, xl, 0, 1)
    send_tok(xl, 0, 1, True, 3)
    send_tok(x, 1, 0, True, 4)
    send_tok(x, 1, 1, True, 5)
    pass_on(2, xl, 0, 1)
    tok_wait(False, 1, xr, 1, 1)
    send_tok(xr, 1, 1, False, 3)
    send_tok(x, 0, 0, False, 4)
    send_tok(x, 0, 1, False, 5)
    pass_on(3, xr, 1, 1)
    pass_factor(2, xl, 0)
    pass_factor(3, xr, 1)
    ph("gu_last")
    for i in range(4):
        gu.last(i)
    ph("gd_near")
    gd.near()

    ph("xexp")
    blk = hal.at[pl.ds(0, 7)]
    rcopy(blk, blk, h_s, h_r, mate).wait_recv()
    hv = hal[...].reshape(256, 256).astype(F32)
    rid = lax.broadcasted_iota(jnp.int32, (256, 256), 0) % 8
    for q in range(8):
        mx[0:256, q * 256:(q + 1) * 256] = jnp.where(rid == q, hv, 0.0).astype(BF16)

    ph("gd_c0")
    gd.cross(0)
    ph("hu")

    @pl.loop(0, 6)
    def _(i):
        w = ug[:, :, :, pl.ds(pl.multiple_of(i * 256, 256), 128)].reshape(D, 128)
        r = jnp.dot(mx[0:256, :], w, preferred_element_type=F32)
        r = jnp.sum(r.reshape(32, 8, 128), axis=1)
        cols = pl.ds(pl.multiple_of(i * 128, 128), 128)
        hu[0, 0:2, cols] = jnp.zeros((2, 128), F32)
        for q in range(15):
            hu[q + 1, 0:2, cols] = r[2 * q:2 * q + 2]

    row8 = lax.broadcasted_iota(jnp.int32, (8, 128), 0)

    def hidden(xs, hs, cc, to):
        unit = [(xs[k] * 2 + cc) * 2 + hs[k] for k in range(2)]
        a = [[tok[xs[k], cc, ch, hs[k] * HALF:(hs[k] + 1) * HALF, :] for ch in range(2)]
             for k in range(2)]
        a = jnp.concatenate([jnp.concatenate(v, axis=1) for v in a], axis=0)

        def act(i, u, g):
            cols = pl.ds(i * 128, 128)
            taps = [cw[k:k + 1, cols] for k in range(4)]
            for k in range(2):
                f = rr[xs[k], cc, hs[k]]
                uk, gk = u[k * HALF:(k + 1) * HALF] * f, g[k * HALF:(k + 1) * HALF] * f
                before = hu[unit[k], :, cols]
                h0, h1 = before[0:1], before[1:2]
                u1, u2 = pltpu.roll(uk, 1, 0), pltpu.roll(uk, 2, 0)
                f1 = jnp.where(row8 == 0, h1, u1[:8])
                f2 = jnp.where(row8 == 0, h0, jnp.where(row8 == 1, h1, u2[:8]))
                u1 = jnp.concatenate([f1, u1[8:]], axis=0)
                u2 = jnp.concatenate([f2, u2[8:]], axis=0)
                s = taps[3] + taps[0] * u2 + taps[1] * u1 + taps[2] * uk
                hid[to, pl.ds(k * HALF, HALF), cols] = gated_gelu(s, gk).astype(BF16)

        for i, width in ((0, 512), (2, 512), (4, 384)):
            w = ug[:, :, :, pl.ds(i * 256, width)].reshape(D, width)
            r = jnp.dot(a, w, preferred_element_type=F32)
            act(i, r[:, :128], r[:, 128:256])
            if width == 512:
                act(i + 1, r[:, 256:384], r[:, 384:])
            else:
                act(i + 1, r[:, 256:384], pltpu.roll(r[:, 256:384], 64, 1))

    def down(frm, xs, hs, cls):
        @pl.loop(0, 4)
        def _(n):
            w = jnp.concatenate([dwn[n, k] for k in range(4)], axis=1)
            r = jnp.dot(hid[frm], w, preferred_element_type=F32).astype(BF16)
            cols = pl.ds(pl.multiple_of(n * 512, 512), 512)
            for k in range(2):
                pbuf[cls, xs[k], hs[k], :, cols] = r[k * HALF:(k + 1) * HALF]

        @pl.when(cls == 0)
        def _():
            for k in range(2):
                rcopy(pbuf.at[0, xs[k], hs[k]], precv.at[xs[k], hs[k]], p_s,
                      p_r.at[xs[k], hs[k]], mate).start()

    def core_of(cls):
        return (1 - c) * (1 - cls) + c * cls

    def group(xs, hs, slot=None, up=True, dn=True):
        @pl.loop(0, 2)
        def _(cls):
            to = cls if slot is None else slot + cls
            if up:
                hidden(xs, hs, core_of(cls), to)
            if dn:
                down(to, xs, hs, cls)

    def joined(xx, h, extra=None):
        rcopy(pbuf.at[0, xx, h], precv.at[xx, h], p_s, p_r.at[xx, h], mate).wait_recv()

        @pl.loop(0, HALF // 16)
        def _(r):
            rr = pl.ds(pl.multiple_of(r * 16, 16), 16)
            v = pbuf[1, xx, h, rr, :].astype(F32) + precv[xx, h, rr, :].astype(F32)
            if extra is not None:
                v = v + extra[rr, :].astype(F32)
            pbuf[1, xx, h, rr, :] = v.astype(BF16)

    def send_sum(xx, h, to_right, dst, k):
        side = 0 if to_right else 1
        cp = rcopy(pbuf.at[1, xx, h], dst, x_s, x_r.at[side, k],
                   (xr if to_right else xl) * 2 + c)
        cp.start()

    def wait_sum(from_left, dst, k):
        side = 0 if from_left else 1
        rcopy(dst, dst, x_s, x_r.at[side, k], mate).wait_recv()

    ph("gd_far")
    gd.far()
    ph("gd_c123")
    gd.cross(1)
    gd.cross(2)
    gd.cross(3)

    ph("tok_opp")
    tok_wait(True, 2, xo, 0, 0)
    pass_on(4, xo, 0, 0)
    tok_wait(False, 2, xo, 1, 0)
    pass_on(5, xo, 1, 0)
    tok_wait(True, 3, xo, 0, 1)
    pass_on(4, xo, 0, 1)
    pass_factor(4, xo, 0)
    tok_wait(False, 3, xo, 1, 1)
    pass_on(5, xo, 1, 1)
    pass_factor(5, xo, 1)
    ph("h_opp1")
    hidden((xo, xo), (0, 1), core_of(1), 1)
    ph("mate_opp")
    mate_wait(4, xo, 0)
    mate_wait(5, xo, 1)
    ph("h_opp0")
    hidden((xo, xo), (0, 1), core_of(0), 0)
    ph("gd_last")
    for i in range(4):
        gd.last(i)

    ph("d_opp")
    group((xo, xo), (0, 1), 0, up=False)
    ph("j_opp")
    joined(xo, 0)
    send_sum(xo, 0, True, xfwd.at[0], 0)
    joined(xo, 1)
    send_sum(xo, 1, False, xfwd.at[1], 0)
    ph("mate_near1")
    mate_wait(2, xl, 0)
    mate_wait(3, xr, 1)
    ph("g_near1")
    group((xr, xl), (1, 0))
    ph("j_near1")
    joined(xr, 1)
    send_sum(xr, 1, True, rs.at[pl.ds(HALF, HALF)], 1)
    joined(xl, 0)
    send_sum(xl, 0, False, rs.at[pl.ds(0, HALF)], 1)

    ph("tok_near2")
    tok_wait(True, 4, xl, 1, 0)
    pass_on(6, xl, 1, 0)
    tok_wait(False, 4, xr, 0, 0)
    pass_on(7, xr, 0, 0)
    tok_wait(True, 5, xl, 1, 1)
    pass_on(6, xl, 1, 1)
    pass_factor(6, xl, 1)
    tok_wait(False, 5, xr, 0, 1)
    pass_on(7, xr, 0, 1)
    pass_factor(7, xr, 0)
    mate_wait(6, xl, 1)
    mate_wait(7, xr, 0)
    ph("g_near2")
    group((xr, xl), (0, 1))
    ph("j_near2")
    wait_sum(True, xfwd.at[0], 0)
    joined(xr, 0, xfwd.at[0])
    send_sum(xr, 0, True, last.at[pl.ds(0, HALF)], 2)
    ph("j_near2b")
    wait_sum(False, xfwd.at[1], 0)
    joined(xl, 1, xfwd.at[1])
    send_sum(xl, 1, False, last.at[pl.ds(HALF, HALF)], 2)

    ph("mate_own")
    mate_wait(0, x, 0)
    mate_wait(1, x, 1)
    ph("g_own")
    group((x, x), (0, 1))
    ph("base")
    outs = []
    for h in range(2):
        rcopy(pbuf.at[0, x, h], precv.at[x, h], p_s, p_r.at[x, h], mate).wait_recv()

        @pl.loop(0, HALF // 16)
        def _(r):
            row = pl.ds(pl.multiple_of(r * 16, 16), 16)
            at = pl.ds(pl.multiple_of(h * HALF + r * 16, 16), 16)
            for ch in range(2):
                cols = pl.ds(ch * CH, CH)
                v = tok[x, c, ch, at, :].astype(F32) + pbuf[1, x, h, row, cols].astype(F32)
                base[at, cols] = v + precv[x, h, row, cols].astype(F32)

    ph("fin_w1")
    wait_sum(True, rs.at[pl.ds(HALF, HALF)], 1)
    wait_sum(False, rs.at[pl.ds(0, HALF)], 1)
    for h in range(2):
        @pl.loop(h * 12, h * 12 + 12)
        def _(r):
            at = pl.ds(pl.multiple_of(r * 16, 16), 16)
            base[at, :] = base[at, :] + rs[at, :].astype(F32)

        cp = pltpu.make_async_copy(base.at[pl.ds(h * HALF, HALF)], out.at[pl.ds(h * HALF, HALF)],
                                   lsem.at[5 + h])
        cp.start()
        outs.append(cp)
    for cp in outs:
        cp.wait()

    ph("fin_w2")
    wait_sum(True, last.at[pl.ds(0, HALF)], 2)
    wait_sum(False, last.at[pl.ds(HALF, HALF)], 2)

    ph("drain")
    @pl.when(c != half)
    def _():
        over.wait_send()

    for cp in drains:
        cp.wait_send()
    gw.drain()
    gv.drain()
    gu.drain()
    gd.drain()
    for sem, view in (
            (d_s, wm.at[0, :, :, pl.ds(0, 64)]),
            (xw_s, wm.at[1, :, :, pl.ds(0, 48)]),
            (xd_s, wm.at[1, :, :, pl.ds(0, 64)]),
            (t_s, tok.at[pl.ds(0, 3), 0]),
            (td_s, tok.at[:, 0]),
            (rd_s, rr.at[:, 0]),
            (h_s, hal.at[pl.ds(0, 7)]),
            (p_s, pbuf.at[0]),
            (x_s, precv.at[pl.ds(0, 3)])):
        rcopy(view, view, sem, lsem.at[0], mate).wait_send()
    ph("")


def body(mixed, residual, mix_weight, norm_gain, up_weight, gate_weight, conv_weight, conv_bias,
         down_weight):
    any_ = pl.BlockSpec(memory_space=pl.ANY)
    vm = pl.BlockSpec(memory_space=pltpu.VMEM)
    dma = pltpu.SemaphoreType.DMA
    part, last = pl.pallas_call(
        kernel,
        out_shape=(jax.ShapeDtypeStruct((TOK, D), F32),
                   jax.ShapeDtypeStruct((TOK, D), BF16)),
        in_specs=[any_, any_, any_, vm, any_, any_, vm, vm, any_],
        out_specs=(any_, any_),
        scratch_shapes=[
            pltpu.VMEM((2, 4, 4, 128, CH), BF16),
            pltpu.VMEM((4, 4, 128, UG), BF16),
            pltpu.VMEM((4, 4, HID, 128), BF16),
            pltpu.VMEM((2, 688, 128), BF16),
            pltpu.VMEM((8, HID), F32),
            pltpu.VMEM((4, 2, 2, TOK, CH), BF16),
            pltpu.VMEM((4, 2, 2, HALF, 128), F32),
            pltpu.VMEM((TOK, D), BF16),
            pltpu.VMEM((TOK, D), BF16),
            pltpu.VMEM((8, 32, 256), BF16),
            pltpu.VMEM((16, 8, HID), F32),
            pltpu.VMEM((2, TOK, HID), BF16),
            pltpu.VMEM((2, 4, 2, HALF, D), BF16),
            pltpu.VMEM((4, 2, HALF, D), BF16),
            pltpu.VMEM((2, HALF, D), BF16),
            pltpu.VMEM((TOK, D), F32),
            dma((8,)), dma((4,)), dma((4,)),
            dma((2, 16)), dma((4, 16)),
            dma((2, 6)), dma((8,)), dma((8,)),
            dma((4, 2)), dma((2, 3)), dma((2, 3)),
            dma((14,)),
        ],
        compiler_params=pltpu.CompilerParams(
            collective_id=0, has_side_effects=True, vmem_limit_bytes=67_043_328),
    )(mixed, residual, mix_weight, norm_gain[None], up_weight.T, gate_weight.T, conv_weight, conv_bias,
      down_weight)
    return (part + last.astype(F32)).astype(BF16)


def solution(mesh):
    rows = P(("fs", "tp"), None)
    in_specs = (rows, rows, rows, P(), P("fs", "tp"), P("fs", "tp"), P(None, "tp"), P("tp"),
                P("tp", "fs"))
    return jax.shard_map(body, mesh=mesh, in_specs=in_specs, out_specs=rows, check_vma=False)
```

```python
import functools

import jax
import jax.numpy as jnp
from jax import lax
from jax.experimental import pallas as pl
from jax.experimental.pallas import tpu as pltpu
from jax.sharding import PartitionSpec as P

MESH = pl.DeviceIdType.MESH
F32 = jnp.float32
BF16 = jnp.bfloat16
NORM_EPS = 1e-06
GELU_C = 0.7978845608028654

D = 2048
TOK = 384
CH = 1024
HALF = 192
UG = 1408
HID = 768


def gated_gelu(v, gate):
    t = jnp.tanh(v * (GELU_C + (GELU_C * 0.044715) * (v * v)))
    v = 0.5 * v
    return (v + v * t) * gate


class Phases:
    def __init__(self):
        self.scope = None

    def __call__(self, name):
        if self.scope is not None:
            self.scope.__exit__(None, None, None)
        self.scope = jax.named_scope(name) if name else None
        if name:
            self.scope.__enter__()


class Gather:
    def __init__(self, ref, lo, rows, split, flip, fs, tp, send_sem, recv_sem, total=None,
                 direct=False):
        self.direct = direct
        self.total = total
        self.ref, self.lo, self.rows, self.split, self.flip = ref, lo, rows, split, flip
        self.tp, self.ss, self.rs = tp, send_sem, recv_sem
        z, y = fs // 4, fs % 4
        self.p = y * (1 - flip) + z * flip
        self.s = z * (1 - flip) + y * flip
        self.n = 0
        self.sends = []

    def zy(self, dp, ds):
        p, s = (self.p + dp + 4) % 4, (self.s + ds + 4) % 4
        return s * (1 - self.flip) + p * self.flip, p * (1 - self.flip) + s * self.flip

    def view(self, dp, ds, a=0, n=None):
        z, y = self.zy(dp, ds)
        n = self.rows if n is None else n
        return self.ref.at[z, y, pl.ds(self.lo + a, n)]

    def copy(self, k, blk, to):
        z, y = self.zy(*to)
        return pltpu.make_async_remote_copy(
            src_ref=blk, dst_ref=blk, send_sem=self.ss if self.total is not None else self.ss.at[self.n], recv_sem=self.rs.at[k],
            device_id={"fs": z * 4 + y, "tp": self.tp}, device_id_type=MESH)

    def send(self, k, blk, to):
        c = self.copy(k, blk, to)
        c.start()
        self.sends.append(c)
        self.n += 1

    def wait(self, k, blk):
        self.copy(k, blk, (1, 0)).wait_recv()

    REL = (0, -1, 1, 2)

    def both(self, i):
        blk = self.view(self.REL[i], 0)
        self.send(4 + i, blk, (0, 1))
        self.send(8 + i, blk, (0, -1))
        if self.direct:
            self.send(12 + i, blk, (0, 2))

    def start(self):
        own = self.view(0, 0)
        self.send(0, own, (1, 0))
        self.send(1, own, (-1, 0))
        if self.direct:
            self.send(2, own, (2, 0))
        self.both(0)

    def near(self):
        s = self.split
        self.wait(0, self.view(-1, 0))
        if not self.direct:
            self.send(2, self.view(-1, 0, 0, s), (1, 0))
        self.both(1)
        self.wait(1, self.view(1, 0))
        if s < self.rows:
            self.send(3, self.view(1, 0, s, self.rows - s), (-1, 0))
        self.both(2)

    def far(self):
        s = self.split
        self.wait(2, self.view(2, 0, 0, s))
        if s < self.rows:
            self.wait(3, self.view(2, 0, s, self.rows - s))
        self.both(3)

    def cross(self, i):
        below, above = self.view(self.REL[i], -1), self.view(self.REL[i], 1)
        self.wait(4 + i, below)
        if i < 2 and not self.direct:
            self.send(12 + i, below, (0, 1))
        self.wait(8 + i, above)
        if i >= 2 and not self.direct:
            self.send(12 + i, above, (0, -1))

    def last(self, i):
        self.wait(12 + i, self.view(self.REL[i], 2))

    def drain(self):
        if self.total is not None:
            self.copy(0, self.total, (1, 0)).wait_send()
        else:
            for c in self.sends:
                c.wait_send()


def kernel(mixed, resid, wm_in, gain, up_in, gate_in, cw_in, cb_in, dw_in, out, last,
           wm, ug, dwn, upt, cw, tok, rr, mx, rs, hal, hu, hid, pbuf, precv, xfwd, base,
           lsem, wx_s, wx_r, g_s, g_r, t_r, td_r, rd_r, p_r, x_r, xw_r, one):
    fs, tp = lax.axis_index("fs"), lax.axis_index("tp")
    z, y, x, c = fs // 4, fs % 4, tp // 2, tp % 2
    xr, xl, xo = (x + 1) % 4, (x + 3) % 4, (x + 2) % 4
    mate = x * 2 + (1 - c)
    drains = []
    (w_sem, v_sem, d_s, d_r, t_s, td_s, rd_s, h_s, h_r, p_s, x_s, xw_s, xd_s, xd_r) = (
        one.at[k] for k in range(14))

    def rcopy(src, dst, ss, rsem, tp_to, fs_to=None):
        return pltpu.make_async_remote_copy(
            src_ref=src, dst_ref=dst, send_sem=ss, recv_sem=rsem,
            device_id={"fs": fs if fs_to is None else fs_to, "tp": tp_to}, device_id_type=MESH)

    ph = Phases()
    ph("load")
    ld_up = pltpu.make_async_copy(up_in, upt.at[0], lsem.at[0])
    ld_gate = pltpu.make_async_copy(gate_in, upt.at[1], lsem.at[4])
    ld_dw = pltpu.make_async_copy(dw_in, dwn.at[z, y, pl.ds(0, 688)], lsem.at[1])
    ld_mx = pltpu.make_async_copy(mixed, mx, lsem.at[2])
    ld_rs = pltpu.make_async_copy(resid, rs, lsem.at[3])
    row16 = pl.multiple_of(tp * 16, 16)
    ld_own = pltpu.make_async_copy(wm_in.at[:, pl.ds(CH, CH)], wm.at[1, z, y, pl.ds(row16, 16)],
                                   lsem.at[7])
    ld_own.start()
    ld_up.start()
    ld_gate.start()
    ld_mx.start()
    ld_rs.start()
    ld_dw.start()

    ph("barrier")
    bar = pltpu.get_barrier_semaphore()
    peers = [(fs, (tp + k) % 8) for k in range(1, 8)]
    peers += [(z * 4 + (y + 1) % 4, tp), (z * 4 + (y + 3) % 4, tp)]
    peers += [(((z + 1) % 4) * 4 + y, tp), (((z + 3) % 4) * 4 + y, tp)]
    peers += [(z * 4 + (y + 2) % 4, tp), (((z + 2) % 4) * 4 + y, tp)]
    for f, t in peers:
        pl.semaphore_signal(bar, inc=1, device_id={"fs": f, "tp": t}, device_id_type=MESH)
    pl.semaphore_wait(bar, len(peers))

    ph("wx")
    half = tp // 4
    slot = tp % 4
    src = wm_in.at[:, pl.ds(0, CH)]
    dst = wm.at[0, z, y, pl.ds(row16, 16)]
    for k in range(1, 4):
        cp = rcopy(src, dst, wx_s.at[k], wx_r.at[slot], ((x + k) % 4) * 2 + half)
        cp.start()
        drains.append(cp)
    stay = pltpu.make_async_copy(src, dst, wx_r.at[slot])
    over = rcopy(src, dst, wx_s.at[0], wx_r.at[slot], mate)

    @pl.when(c == half)
    def _():
        stay.start()

    @pl.when(c != half)
    def _():
        over.start()

    lo = pl.multiple_of(c * 64, 64)
    other = pl.multiple_of(64 - lo, 64)
    gw = Gather(wm.at[0], lo, 64, 32, c, fs, tp, w_sem, g_r.at[0],
                wm.at[0, pl.ds(0, 3), :, pl.ds(0, 80)])
    gv = Gather(wm.at[1], row16, 16, 16, c, fs, tp, v_sem, g_r.at[1],
                wm.at[1, pl.ds(0, 3), 0, pl.ds(0, 80)], True)
    gu = Gather(ug, 0, 128, 64, c, fs, tp, g_s.at[0], g_r.at[2])
    gd = Gather(dwn, 0, 688, 352, 1 - c, fs, tp, g_s.at[1], g_r.at[3])

    def share(k, dp, ds):
        blk = gw.view(dp, ds)
        cp = rcopy(blk, blk, d_s, d_r, mate)
        cp.start()

    def w_cross(i):
        gw.cross(i)
        share(4 + 2 * i, Gather.REL[i], -1)
        share(5 + 2 * i, Gather.REL[i], 1)

    def w_rows(xsrc, core, z0=0, nz=4):
        return wm.at[1, pl.ds(z0, nz), :, pl.ds(pl.multiple_of((xsrc * 2 + core) * 16, 16), 16)]

    def line_send(to_right, k, xsrc, z0, nz):
        side, blk = 0 if to_right else 1, w_rows(xsrc, c, z0, nz)
        cp = rcopy(blk, blk, xw_s, xw_r.at[side, k], (xr if to_right else xl) * 2 + c)
        cp.start()

    def line_wait(from_left, k, xsrc, z0, nz):
        side, blk = 0 if from_left else 1, w_rows(xsrc, c, z0, nz)
        rcopy(blk, blk, xw_s, xw_r.at[side, k], mate).wait_recv()

    def line_share(xsrc, z0=0, nz=4):
        blk = w_rows(xsrc, c, z0, nz)
        cp = rcopy(blk, blk, xd_s, xd_r, mate)
        cp.start()

    ph("v_start")
    ld_own.wait()
    gv.start()
    gv.near()
    gv.far()
    ph("w_start")
    for k in range(4):
        row = pl.multiple_of(lo + k * 16, 16)
        blk = wm.at[0, z, y, pl.ds(row, 16)]
        rcopy(blk, blk, wx_s.at[0], wx_r.at[k], mate).wait_recv()
    gw.start()
    share(0, 0, 0)
    ph("prep")
    zero_rows = jnp.zeros((HID - 688, 128), BF16)

    @pl.loop(0, 16)
    def _(f):
        dwn[f // 4, f % 4, pl.ds(688, HID - 688)] = zero_rows

    cw[...] = jnp.zeros((8, HID), F32)
    cw[0:3, 0:688] = cw_in[...]
    cw[3:4, 0:688] = cb_in[...].reshape(1, 688)
    ld_up.wait()
    ld_gate.wait()
    gn = gain[:, pl.ds(pl.multiple_of(fs * 128, 128), 128)]
    for i in range(5):
        for k in range(2):
            t = upt[k, pl.ds(i * 128, 128), :].astype(F32) * gn
            ug[z, y, :, pl.ds(i * 256 + k * 128, 128)] = t.T.astype(BF16)
    gap = jnp.zeros((16, 128), F32)
    t = [upt[0, pl.ds(640, 48), :].astype(F32) * gn, gap,
         upt[1, pl.ds(640, 48), :].astype(F32) * gn, gap]
    ug[z, y, :, pl.ds(1280, 128)] = jnp.concatenate(t, axis=0).T.astype(BF16)

    def mix(ch, n):
        w = wm[ch, :, :, :, n * 512:(n + 1) * 512].reshape(D, 512)
        s = jnp.dot(mx[...], w, preferred_element_type=F32)
        at = ch * CH + n * 512
        s = rs[:, at:at + 512].astype(F32) + s
        tok[x, c, ch, :, n * 512:(n + 1) * 512] = s.astype(BF16)

    def send_tok(xsrc, h, ch, to_right, sidx):
        blk = tok.at[xsrc, c, ch, pl.ds(h * HALF, HALF)]
        side = 0 if to_right else 1
        cp = rcopy(blk, blk, t_s, t_r.at[side, sidx],
                   (xr if to_right else xl) * 2 + c)
        cp.start()

    def tok_wait(from_left, idx, xsrc, h, ch):
        blk = tok.at[xsrc, c, ch, pl.ds(h * HALF, HALF)]
        side = 0 if from_left else 1
        rcopy(blk, blk, t_s, t_r.at[side, idx], mate).wait_recv()

    def factor(xsrc, h):
        acc = None
        for ch in range(2):
            for k in range(CH // 128):
                v = tok[xsrc, c, ch, h * HALF:(h + 1) * HALF, k * 128:(k + 1) * 128].astype(F32)
                acc = v * v if acc is None else acc + v * v
        m = jnp.sum(acc, axis=-1, keepdims=True) * (1.0 / D)
        rr[xsrc, c, h] = jnp.broadcast_to(lax.rsqrt(m + NORM_EPS), (HALF, 128))

    def pass_on(k, xsrc, h, ch):
        blk = tok.at[xsrc, c, ch, pl.ds(h * HALF, HALF)]
        cp = rcopy(blk, blk, td_s, td_r.at[k], mate)
        cp.start()

    def pass_factor(k, xsrc, h):
        factor(xsrc, h)
        blk = rr.at[xsrc, c, h]
        cp = rcopy(blk, blk, rd_s, rd_r.at[k], mate)
        cp.start()

    def mate_wait(k, xsrc, h):
        blk = tok.at[xsrc, 1 - c, :, pl.ds(h * HALF, HALF)]
        rcopy(blk, blk, td_s, td_r.at[k], mate).wait_recv()
        blk = rr.at[xsrc, 1 - c, h]
        rcopy(blk, blk, rd_s, rd_r.at[k], mate).wait_recv()

    ph("w_near")
    gw.near()
    share(1, -1, 0)
    share(2, 1, 0)
    ph("w_c0")
    w_cross(0)
    ph("v_last")
    for i in range(4):
        gv.cross(i)
        gv.last(i)
    line_send(True, 0, x, 0, 2)
    line_send(False, 0, x, 2, 2)
    line_send(True, 2, x, 2, 2)
    line_send(False, 2, x, 0, 2)
    line_share(x)
    ph("w_far")
    gw.far()
    share(3, 2, 0)
    ph("w_c1")
    w_cross(1)
    ph("w_c2")
    w_cross(2)
    ph("w_c3")
    w_cross(3)
    gu.start()
    ph("line_fwd")
    line_wait(True, 0, xl, 0, 2)
    line_send(True, 1, xl, 0, 2)
    line_share(xl, 0, 2)
    line_wait(False, 0, xr, 2, 2)
    line_send(False, 1, xr, 2, 2)
    line_share(xr, 2, 2)
    ph("w_last")
    for i in range(4):
        gw.last(i)
        share(12 + i, Gather.REL[i], 2)
    ph("w_shared")
    blk = wm.at[0, :, :, pl.ds(other, 64)]
    rcopy(blk, blk, d_s, d_r, mate).wait_recv()
    ld_mx.wait()
    ld_rs.wait()
    ph("mix0")
    mix(0, 0)
    mix(0, 1)
    send_tok(x, 0, 0, True, 0)
    send_tok(x, 1, 0, False, 0)
    pass_on(0, x, 0, 0)
    pass_on(1, x, 1, 0)
    ph("gu_near")
    gu.near()
    ph("line_far")
    line_wait(True, 2, xl, 2, 2)
    line_share(xl, 2, 2)
    line_wait(False, 2, xr, 0, 2)
    line_share(xr, 0, 2)
    line_wait(True, 1, xo, 0, 2)
    line_wait(False, 1, xo, 2, 2)
    line_share(xo)
    blk = wm.at[1, :, :, pl.ds(0, 64)]
    rcopy(blk, blk, xd_s, xd_r, mate).wait_recv()
    ph("mix1")
    mix(1, 0)
    mix(1, 1)
    send_tok(x, 0, 1, True, 1)
    send_tok(x, 1, 1, False, 1)
    pass_on(0, x, 0, 1)
    pass_on(1, x, 1, 1)
    ph("gu_c0")
    gu.cross(0)
    ph("own_mate")
    pass_factor(0, x, 0)
    pass_factor(1, x, 1)

    tails = []
    for h in range(2):
        f = rr[x, c, h, HALF - 8:HALF, :][:, 0:1]
        for r in (6, 7):
            for q in range(8):
                ch, col = q // 4, (q % 4) * 256
                v = tok[x, c, ch, (h + 1) * HALF - 16:(h + 1) * HALF, col:col + 256].astype(F32)
                tails.append(v[r + 8:r + 9] * f[r:r + 1])
    hal[tp] = jnp.concatenate(tails, axis=0).astype(BF16)
    for k in range(1, 8):
        rcopy(hal.at[tp], hal.at[tp], h_s, h_r, (tp + k) % 8).start()

    ph("gu_far")
    gu.far()
    ph("tokA0")
    tok_wait(True, 0, xl, 0, 0)
    send_tok(xl, 0, 0, True, 2)
    pass_on(2, xl, 0, 0)
    tok_wait(False, 0, xr, 1, 0)
    send_tok(xr, 1, 0, False, 2)
    pass_on(3, xr, 1, 0)
    ph("gu_c1")
    gu.cross(1)
    ph("gu_c2")
    gu.cross(2)
    ph("gu_c3")
    gu.cross(3)
    ld_dw.wait()
    gd.start()
    ph("tokA1")
    tok_wait(True, 1, xl, 0, 1)
    send_tok(xl, 0, 1, True, 3)
    send_tok(x, 1, 0, True, 4)
    send_tok(x, 1, 1, True, 5)
    pass_on(2, xl, 0, 1)
    tok_wait(False, 1, xr, 1, 1)
    send_tok(xr, 1, 1, False, 3)
    send_tok(x, 0, 0, False, 4)
    send_tok(x, 0, 1, False, 5)
    pass_on(3, xr, 1, 1)
    pass_factor(2, xl, 0)
    pass_factor(3, xr, 1)
    ph("gu_last")
    for i in range(4):
        gu.last(i)
    ph("gd_near")
    gd.near()

    ph("xexp")
    blk = hal.at[pl.ds(0, 7)]
    rcopy(blk, blk, h_s, h_r, mate).wait_recv()
    hv = hal[...].reshape(256, 256).astype(F32)
    rid = lax.broadcasted_iota(jnp.int32, (256, 256), 0) % 8
    for q in range(8):
        mx[0:256, q * 256:(q + 1) * 256] = jnp.where(rid == q, hv, 0.0).astype(BF16)

    ph("gd_c0")
    gd.cross(0)
    ph("hu")

    @pl.loop(0, 6)
    def _(i):
        w = ug[:, :, :, pl.ds(pl.multiple_of(i * 256, 256), 128)].reshape(D, 128)
        r = jnp.dot(mx[0:256, :], w, preferred_element_type=F32)
        r = jnp.sum(r.reshape(32, 8, 128), axis=1)
        cols = pl.ds(pl.multiple_of(i * 128, 128), 128)
        hu[0, 0:2, cols] = jnp.zeros((2, 128), F32)
        for q in range(15):
            hu[q + 1, 0:2, cols] = r[2 * q:2 * q + 2]

    row8 = lax.broadcasted_iota(jnp.int32, (8, 128), 0)

    def hidden(xs, hs, cc, to):
        unit = [(xs[k] * 2 + cc) * 2 + hs[k] for k in range(2)]
        a = [[tok[xs[k], cc, ch, hs[k] * HALF:(hs[k] + 1) * HALF, :] for ch in range(2)]
             for k in range(2)]
        a = jnp.concatenate([jnp.concatenate(v, axis=1) for v in a], axis=0)

        def act(i, u, g):
            cols = pl.ds(i * 128, 128)
            taps = [cw[k:k + 1, cols] for k in range(4)]
            for k in range(2):
                f = rr[xs[k], cc, hs[k]]
                uk, gk = u[k * HALF:(k + 1) * HALF] * f, g[k * HALF:(k + 1) * HALF] * f
                before = hu[unit[k], :, cols]
                h0, h1 = before[0:1], before[1:2]
                u1, u2 = pltpu.roll(uk, 1, 0), pltpu.roll(uk, 2, 0)
                f1 = jnp.where(row8 == 0, h1, u1[:8])
                f2 = jnp.where(row8 == 0, h0, jnp.where(row8 == 1, h1, u2[:8]))
                u1 = jnp.concatenate([f1, u1[8:]], axis=0)
                u2 = jnp.concatenate([f2, u2[8:]], axis=0)
                s = taps[3] + taps[0] * u2 + taps[1] * u1 + taps[2] * uk
                hid[to, pl.ds(k * HALF, HALF), cols] = gated_gelu(s, gk).astype(BF16)

        for i, width in ((0, 512), (2, 512), (4, 384)):
            w = ug[:, :, :, pl.ds(i * 256, width)].reshape(D, width)
            r = jnp.dot(a, w, preferred_element_type=F32)
            act(i, r[:, :128], r[:, 128:256])
            if width == 512:
                act(i + 1, r[:, 256:384], r[:, 384:])
            else:
                act(i + 1, r[:, 256:384], pltpu.roll(r[:, 256:384], 64, 1))

    def down(frm, xs, hs, cls):
        @pl.loop(0, 4)
        def _(n):
            w = jnp.concatenate([dwn[n, k] for k in range(4)], axis=1)
            r = jnp.dot(hid[frm], w, preferred_element_type=F32).astype(BF16)
            cols = pl.ds(pl.multiple_of(n * 512, 512), 512)
            for k in range(2):
                pbuf[cls, xs[k], hs[k], :, cols] = r[k * HALF:(k + 1) * HALF]

        @pl.when(cls == 0)
        def _():
            for k in range(2):
                rcopy(pbuf.at[0, xs[k], hs[k]], precv.at[xs[k], hs[k]], p_s,
                      p_r.at[xs[k], hs[k]], mate).start()

    def core_of(cls):
        return (1 - c) * (1 - cls) + c * cls

    def group(xs, hs, slot=None, up=True, dn=True):
        @pl.loop(0, 2)
        def _(cls):
            to = cls if slot is None else slot + cls
            if up:
                hidden(xs, hs, core_of(cls), to)
            if dn:
                down(to, xs, hs, cls)

    def joined(xx, h, extra=None):
        rcopy(pbuf.at[0, xx, h], precv.at[xx, h], p_s, p_r.at[xx, h], mate).wait_recv()

        @pl.loop(0, HALF // 16)
        def _(r):
            rr = pl.ds(pl.multiple_of(r * 16, 16), 16)
            v = pbuf[1, xx, h, rr, :].astype(F32) + precv[xx, h, rr, :].astype(F32)
            if extra is not None:
                v = v + extra[rr, :].astype(F32)
            pbuf[1, xx, h, rr, :] = v.astype(BF16)

    def send_sum(xx, h, to_right, dst, k):
        side = 0 if to_right else 1
        cp = rcopy(pbuf.at[1, xx, h], dst, x_s, x_r.at[side, k],
                   (xr if to_right else xl) * 2 + c)
        cp.start()

    def wait_sum(from_left, dst, k):
        side = 0 if from_left else 1
        rcopy(dst, dst, x_s, x_r.at[side, k], mate).wait_recv()

    ph("gd_far")
    gd.far()
    ph("gd_c123")
    gd.cross(1)
    gd.cross(2)
    gd.cross(3)

    ph("tok_opp")
    tok_wait(True, 2, xo, 0, 0)
    pass_on(4, xo, 0, 0)
    tok_wait(False, 2, xo, 1, 0)
    pass_on(5, xo, 1, 0)
    tok_wait(True, 3, xo, 0, 1)
    pass_on(4, xo, 0, 1)
    pass_factor(4, xo, 0)
    tok_wait(False, 3, xo, 1, 1)
    pass_on(5, xo, 1, 1)
    pass_factor(5, xo, 1)
    ph("h_opp1")
    hidden((xo, xo), (0, 1), core_of(1), 1)
    ph("mate_opp")
    mate_wait(4, xo, 0)
    mate_wait(5, xo, 1)
    ph("h_opp0")
    hidden((xo, xo), (0, 1), core_of(0), 0)
    ph("gd_last")
    for i in range(4):
        gd.last(i)

    ph("d_opp")
    group((xo, xo), (0, 1), 0, up=False)
    ph("j_opp")
    joined(xo, 0)
    send_sum(xo, 0, True, xfwd.at[0], 0)
    joined(xo, 1)
    send_sum(xo, 1, False, xfwd.at[1], 0)
    ph("mate_near1")
    mate_wait(2, xl, 0)
    mate_wait(3, xr, 1)
    ph("g_near1")
    group((xr, xl), (1, 0))
    ph("j_near1")
    joined(xr, 1)
    send_sum(xr, 1, True, rs.at[pl.ds(HALF, HALF)], 1)
    joined(xl, 0)
    send_sum(xl, 0, False, rs.at[pl.ds(0, HALF)], 1)

    ph("tok_near2")
    tok_wait(True, 4, xl, 1, 0)
    pass_on(6, xl, 1, 0)
    tok_wait(False, 4, xr, 0, 0)
    pass_on(7, xr, 0, 0)
    tok_wait(True, 5, xl, 1, 1)
    pass_on(6, xl, 1, 1)
    pass_factor(6, xl, 1)
    tok_wait(False, 5, xr, 0, 1)
    pass_on(7, xr, 0, 1)
    pass_factor(7, xr, 0)
    mate_wait(6, xl, 1)
    mate_wait(7, xr, 0)
    ph("g_near2")
    group((xr, xl), (0, 1))
    ph("j_near2")
    wait_sum(True, xfwd.at[0], 0)
    joined(xr, 0, xfwd.at[0])
    send_sum(xr, 0, True, last.at[pl.ds(0, HALF)], 2)
    ph("j_near2b")
    wait_sum(False, xfwd.at[1], 0)
    joined(xl, 1, xfwd.at[1])
    send_sum(xl, 1, False, last.at[pl.ds(HALF, HALF)], 2)

    ph("mate_own")
    mate_wait(0, x, 0)
    mate_wait(1, x, 1)
    ph("g_own")
    group((x, x), (0, 1))
    ph("base")
    outs = []
    for h in range(2):
        rcopy(pbuf.at[0, x, h], precv.at[x, h], p_s, p_r.at[x, h], mate).wait_recv()

        @pl.loop(0, HALF // 16)
        def _(r):
            row = pl.ds(pl.multiple_of(r * 16, 16), 16)
            at = pl.ds(pl.multiple_of(h * HALF + r * 16, 16), 16)
            for ch in range(2):
                cols = pl.ds(ch * CH, CH)
                v = tok[x, c, ch, at, :].astype(F32) + pbuf[1, x, h, row, cols].astype(F32)
                base[at, cols] = v + precv[x, h, row, cols].astype(F32)

    ph("fin_w1")
    wait_sum(True, rs.at[pl.ds(HALF, HALF)], 1)
    wait_sum(False, rs.at[pl.ds(0, HALF)], 1)
    for h in range(2):
        @pl.loop(h * 12, h * 12 + 12)
        def _(r):
            at = pl.ds(pl.multiple_of(r * 16, 16), 16)
            base[at, :] = base[at, :] + rs[at, :].astype(F32)

        cp = pltpu.make_async_copy(base.at[pl.ds(h * HALF, HALF)], out.at[pl.ds(h * HALF, HALF)],
                                   lsem.at[5 + h])
        cp.start()
        outs.append(cp)
    for cp in outs:
        cp.wait()

    ph("fin_w2")
    wait_sum(True, last.at[pl.ds(0, HALF)], 2)
    wait_sum(False, last.at[pl.ds(HALF, HALF)], 2)

    ph("drain")
    @pl.when(c != half)
    def _():
        over.wait_send()

    for cp in drains:
        cp.wait_send()
    gw.drain()
    gv.drain()
    gu.drain()
    gd.drain()
    for sem, view in (
            (d_s, wm.at[0, :, :, pl.ds(0, 64)]),
            (xw_s, wm.at[1, :, :, pl.ds(0, 48)]),
            (xd_s, wm.at[1, :, :, pl.ds(0, 64)]),
            (t_s, tok.at[pl.ds(0, 3), 0]),
            (td_s, tok.at[:, 0]),
            (rd_s, rr.at[:, 0]),
            (h_s, hal.at[pl.ds(0, 7)]),
            (p_s, pbuf.at[0]),
            (x_s, precv.at[pl.ds(0, 3)])):
        rcopy(view, view, sem, lsem.at[0], mate).wait_send()
    ph("")


def body(mixed, residual, mix_weight, norm_gain, up_weight, gate_weight, conv_weight, conv_bias,
         down_weight):
    any_ = pl.BlockSpec(memory_space=pl.ANY)
    vm = pl.BlockSpec(memory_space=pltpu.VMEM)
    dma = pltpu.SemaphoreType.DMA
    part, last = pl.pallas_call(
        kernel,
        out_shape=(jax.ShapeDtypeStruct((TOK, D), F32),
                   jax.ShapeDtypeStruct((TOK, D), BF16)),
        in_specs=[any_, any_, any_, vm, any_, any_, vm, vm, any_],
        out_specs=(any_, any_),
        scratch_shapes=[
            pltpu.VMEM((2, 4, 4, 128, CH), BF16),
            pltpu.VMEM((4, 4, 128, UG), BF16),
            pltpu.VMEM((4, 4, HID, 128), BF16),
            pltpu.VMEM((2, 688, 128), BF16),
            pltpu.VMEM((8, HID), F32),
            pltpu.VMEM((4, 2, 2, TOK, CH), BF16),
            pltpu.VMEM((4, 2, 2, HALF, 128), F32),
            pltpu.VMEM((TOK, D), BF16),
            pltpu.VMEM((TOK, D), BF16),
            pltpu.VMEM((8, 32, 256), BF16),
            pltpu.VMEM((16, 8, HID), F32),
            pltpu.VMEM((2, TOK, HID), BF16),
            pltpu.VMEM((2, 4, 2, HALF, D), BF16),
            pltpu.VMEM((4, 2, HALF, D), BF16),
            pltpu.VMEM((2, HALF, D), BF16),
            pltpu.VMEM((TOK, D), F32),
            dma((8,)), dma((4,)), dma((4,)),
            dma((2, 16)), dma((4, 16)),
            dma((2, 6)), dma((8,)), dma((8,)),
            dma((4, 2)), dma((2, 3)), dma((2, 3)),
            dma((14,)),
        ],
        compiler_params=pltpu.CompilerParams(
            collective_id=0, has_side_effects=True, vmem_limit_bytes=67_043_328),
    )(mixed, residual, mix_weight, norm_gain[None], up_weight.T, gate_weight.T, conv_weight, conv_bias,
      down_weight)
    return (part + last.astype(F32)).astype(BF16)


def solution(mesh):
    rows = P(("fs", "tp"), None)
    in_specs = (rows, rows, rows, P(), P("fs", "tp"), P("fs", "tp"), P(None, "tp"), P("tp"),
                P("tp", "fs"))
    return jax.shard_map(body, mesh=mesh, in_specs=in_specs, out_specs=rows, check_vma=False)
```
